512 devices in a mesh: sp: 32 (over z, x), tp: 16 (over y, core).
Axes of the slice: x: 4, y: 8, z: 8, core: 2. Of those that a mesh axis runs over, the one named last changes fastest.
Arguments:
- queries: bfloat16 [4096, 2048], P('sp', 'tp'), may hold values from -15 to 15
- key_rows: bfloat16 [4096, 2048], P('sp', 'tp'), may hold values from -6 to 6
- value_rows: bfloat16 [4096, 2048], P('sp', 'tp'), may hold values from -6 to 6
- break_bias: bfloat16 [4096, 16], P('sp', 'tp'), may hold values from -14 to 1
- stream: bfloat16 [4096, 4096], P('sp', 'tp'), may hold values from -24 to 24
- out_proj: bfloat16 [2048, 4096], P(None, 'tp'), may hold values from -0.5 to 0.5
- norm_gain: float32 [4096], P('tp'), may hold values from 0.1 to 1.9
- expert_ids: int32 [4096, 2], P('sp'), may hold values from 0 to 63, all different within a row; in each aligned block of 128 rows (0 to 127, 128 to 255, ...) at most 8 rows name the same one
- route_weights: float32 [4096, 2], P('sp'), may hold values from 0.1 to 2.5
- gate_proj: bfloat16 [64, 4096, 384], P('sp', 'tp'), may hold values from -0.09375 to 0.09375
- up_proj: bfloat16 [64, 4096, 384], P('sp', 'tp'), may hold values from -0.09375 to 0.09375
- down_proj: bfloat16 [64, 384, 4096], P('sp', None, 'tp'), may hold values from -0.3125 to 0.3125
- shared_gate: bfloat16 [4096, 384], P('tp'), may hold values from -0.09375 to 0.09375
- shared_up: bfloat16 [4096, 384], P('tp'), may hold values from -0.09375 to 0.09375
- shared_down: bfloat16 [384, 4096], P(None, 'tp'), may hold values from -0.3125 to 0.3125
Outputs:
- result: bfloat16 [4096, 4096], P('sp', 'tp')
The draws below stay inside these ranges and needn't reach their ends.
Inputs may be any that keep to these rules, and one draw needn't show every extreme that they name: `expert_ids`: each row names 2 different experts; within the rows of one index of sp no expert is named by more than 8 rows, a bound that some block reaches of them.
All inputs are finite; a program needn't handle non-finite values.
Results may differ from the reference program's by a relative error of at most 0.022.
Values may be sent and summed in bfloat16 or wider, within the bound.
A program may use at most 64 MiB of HBM per device.

```python
import math
import jax
import jax.numpy as jnp
import numpy as np
from jax import lax

D = 4096
ATTENTION_HEADS = 16
HD = 128
FFE = 384
FFS = 384
TOPK = 2
TOK_DEV = 128
SEQUENCE_TOKENS = 4096
EXPERTS = 64
CAP = 8
N_SP = 32
N_TP = 16


score_shift = 3.125


def draw_break_bias(key, part):
    every_key_rows = jax.random.split(jax.random.fold_in(key, 11), 5)
    fast_share = 0.5
    head_draw = jax.random.uniform(every_key_rows[0], (ATTENTION_HEADS,))
    fast_heads = head_draw < fast_share
    head_level = jnp.where(fast_heads, jnp.log(1.0 / 40.0), jnp.log(1.0 / SEQUENCE_TOKENS)) - score_shift
    block_shift = jax.random.uniform(every_key_rows[1], (SEQUENCE_TOKENS // TOK_DEV, ATTENTION_HEADS), minval=-0.7, maxval=0.7)
    jitter = 0.5 * jax.random.normal(every_key_rows[2], (SEQUENCE_TOKENS, ATTENTION_HEADS))
    logarithm_break_ratio = head_level[None, :] + jnp.repeat(block_shift, TOK_DEV, axis=0) + jitter
    stick_break_mask = jax.random.uniform(every_key_rows[3], (SEQUENCE_TOKENS, ATTENTION_HEADS)) < 4.0 / SEQUENCE_TOKENS
    break_probability = jax.random.uniform(every_key_rows[4], (SEQUENCE_TOKENS, ATTENTION_HEADS), minval=0.2, maxval=0.5)
    stick_break_level = jnp.log(break_probability / (1.0 - break_probability))
    return jnp.clip(jnp.where(stick_break_mask, stick_break_level, logarithm_break_ratio), -14.0, 1.0).astype(jnp.bfloat16)


def draw_stream(key, part):
    every_key_rows = jax.random.split(jax.random.fold_in(key, 23), 3)
    column_level = jnp.linspace(jnp.log(0.3), jnp.log(3.0), D) + 0.4 * jax.random.normal(every_key_rows[0], (D,))
    row_level = jax.random.uniform(every_key_rows[1], (SEQUENCE_TOKENS, 1), minval=jnp.log(0.15), maxval=jnp.log(1.5))
    base_values = jax.random.normal(every_key_rows[2], (SEQUENCE_TOKENS, D))
    scaled = base_values * jnp.exp(column_level)[None, :] * jnp.exp(row_level)
    return jnp.clip(scaled, -24.0, 24.0).astype(jnp.bfloat16)


def levels(rng, dims, shards, low, high):
    loudness, own = 1.0, jax.random.fold_in(rng, 6)
    for axis_at, blocks in shards:
        steps = jnp.exp(jax.random.uniform(jax.random.fold_in(own, axis_at), (blocks,), jnp.float32, low / len(shards), high / len(shards)))
        loudness = loudness * jnp.repeat(steps, dims[axis_at] // blocks).reshape([-1 if axis == axis_at else 1 for axis in range(len(dims))])
    return loudness


def deal_out(key, own, number, rows, amount, top, reach, lean):
    order = jax.random.permutation(key, amount)
    heavy_load, usual = shares(amount, rows * top, reach, lean, True), shares(amount, rows * top, reach, lean, False)
    places = jnp.arange(amount)

    def named(tallies, turn):
        used = int((tallies > 0).sum())
        fixed = max(1, used // 4)
        shifted = fixed + (places - fixed + turn * (used - fixed)) % max(1, amount - fixed)
        return jnp.zeros((amount,), jnp.int32).at[order[jnp.where(places < fixed, places, shifted)]].set(jnp.asarray(tallies, jnp.int32))

    tallies = jnp.where(number % 4 == 0, named(heavy_load, number // 4), named(usual, number - number // 4 - 1))
    mixed = jax.random.permutation(jax.random.fold_in(own, 3), amount)
    donor, receiver = mixed[0:amount // 2 * 2:2], mixed[1:amount // 2 * 2:2]
    room = jnp.minimum(tallies[donor] - 1, reach - tallies[receiver]) // 2
    room = jnp.where((donor == order[0]) | (receiver == order[0]) | (tallies[receiver] == 0), 0, jnp.maximum(room, 0))
    shifted = jax.random.randint(jax.random.fold_in(own, 4), (amount // 2,), 0, 1 << 20) % (room + 1)
    tallies = tallies.at[donor].add(-shifted).at[receiver].add(shifted)
    members = jnp.searchsorted(jnp.cumsum(tallies), jnp.arange(rows * top), side="right").astype(jnp.int32)
    table = members.reshape(top, rows).T
    table = table[jax.random.permutation(jax.random.fold_in(own, 1), rows)]
    turn = jax.random.randint(jax.random.fold_in(own, 2), (rows, 1), 0, top)
    return jnp.take_along_axis(table, (jnp.arange(top)[None, :] + turn) % top, axis=1)


def shares(number_of, total, bound, slope, full):
    portions = [(1 << 20) // math.isqrt(grade ** slope) + 1 for grade in range(1, number_of + 1)]
    largest = bound if full else min(bound, max(-(-total // number_of), total * portions[0] // sum(portions)))
    least = 1 if total - largest >= number_of - 1 else 0
    given, spare = [largest] + [least] * (number_of - 1), total - largest - least * (number_of - 1)
    while spare > 0:
        candidates = [i for i in range(1, number_of) if given[i] < largest] or [i for i in range(1, number_of) if given[i] < bound]
        pool, remaining = sum([portions[i] for i in candidates]), spare
        for i in candidates:
            more = min(bound - given[i], max(1, remaining * portions[i] // pool), spare)
            given[i] = given[i] + more
            spare = spare - more
    return np.array(given)


def normal_values(key, extent, deviation, bound, shards=(), held_as=jnp.bfloat16):
    loudness = levels(key, extent, shards, -0.22, 0.18) if shards else 1.0
    drawn = jax.random.normal(key, extent, jnp.float32) * deviation * loudness
    return jnp.minimum(jnp.maximum(drawn, -bound), bound).astype(held_as)


def setup_inputs(seed: int = 0) -> dict:
    streams_of = jax.random.split(jax.random.key(seed), 16)
    queries = normal_values(streams_of[0], (SEQUENCE_TOKENS, ATTENTION_HEADS * HD), 2.5, 15.0, ((0, 32), (1, 16)))
    key_rows = normal_values(streams_of[1], (SEQUENCE_TOKENS, ATTENTION_HEADS * HD), 1.0, 6.0, ((0, 32), (1, 16)))
    value_rows = normal_values(streams_of[2], (SEQUENCE_TOKENS, ATTENTION_HEADS * HD), 1.0, 6.0, ((0, 32), (1, 16)))
    break_bias = draw_break_bias(jax.random.fold_in(streams_of[15], 71), 0)
    stream = draw_stream(jax.random.fold_in(streams_of[15], 71), 0)
    out_proj = normal_values(streams_of[5], (ATTENTION_HEADS * HD, D), (ATTENTION_HEADS * HD // 16) ** -0.5, 0.5, ((1, 16),))
    norm_gain = jnp.clip(1.0 + 0.18 * jax.random.normal(streams_of[6], (D,), jnp.float32), 0.1, 1.9)
    expert_ids_keys = jax.random.split(jax.random.fold_in(streams_of[7], 1), SEQUENCE_TOKENS // TOK_DEV)
    expert_ids_turns = jax.random.permutation(jax.random.fold_in(streams_of[7], 3), SEQUENCE_TOKENS // TOK_DEV)
    expert_ids = jax.vmap(lambda own, number: deal_out(jax.random.fold_in(streams_of[7], 2), own, number, TOK_DEV, EXPERTS, TOPK, CAP, 2))(expert_ids_keys, expert_ids_turns).reshape((SEQUENCE_TOKENS, TOPK))
    route_weights = jnp.clip(jnp.exp(math.log(2.5) - 3.218876 * jax.random.uniform(streams_of[8], (SEQUENCE_TOKENS, TOPK), jnp.float32) ** levels(streams_of[8], (SEQUENCE_TOKENS, TOPK), ((0, 32),), -0.2, 0.2)), 0.1, 2.5)
    gate_proj = normal_values(streams_of[9], (EXPERTS, D, FFE), D ** -0.5, 0.09375, ((0, 32), (1, 16)))
    up_proj = normal_values(streams_of[10], (EXPERTS, D, FFE), D ** -0.5, 0.09375, ((0, 32), (1, 16)))
    down_proj = normal_values(streams_of[11], (EXPERTS, FFE, D), FFE ** -0.5, 0.3125, ((0, 32), (2, 16)))
    shared_gate = normal_values(streams_of[12], (D, FFS), D ** -0.5, 0.09375, ((0, 16),))
    shared_up = normal_values(streams_of[13], (D, FFS), D ** -0.5, 0.09375, ((0, 16),))
    shared_down = normal_values(streams_of[14], (FFS, D), FFS ** -0.5, 0.3125, ((1, 16),))
    return {"queries": queries, "key_rows": key_rows, "value_rows": value_rows, "break_bias": break_bias, "stream": stream, "out_proj": out_proj, "norm_gain": norm_gain, "expert_ids": expert_ids, "route_weights": route_weights, "gate_proj": gate_proj, "up_proj": up_proj, "down_proj": down_proj, "shared_gate": shared_gate, "shared_up": shared_up, "shared_down": shared_down}


EPS = 1e-06
query_block = 128

def stick_attention(queries, key_rows, value_rows, break_bias):
    head_q = queries.astype(jnp.float32).reshape(SEQUENCE_TOKENS, ATTENTION_HEADS, HD)
    head_k = key_rows.astype(jnp.float32).reshape(SEQUENCE_TOKENS, ATTENTION_HEADS, HD)
    head_v = value_rows.astype(jnp.float32).reshape(SEQUENCE_TOKENS, ATTENTION_HEADS, HD)
    bias_heads = break_bias.astype(jnp.float32).T
    key_pos = jnp.arange(SEQUENCE_TOKENS, dtype=jnp.int32)

    def one_block(block_index):
        offset = block_index * query_block
        query_part = lax.dynamic_slice_in_dim(head_q, offset, query_block, 0)
        positions = offset + jnp.arange(query_block, dtype=jnp.int32)
        logits = jnp.einsum('thd,shd->hts', query_part, head_k) * HD ** (-0.5) + bias_heads[:, None, :]
        before = (key_pos[None, :] < positions[:, None])[None]
        log_fail = jnp.where(before, jax.nn.log_sigmoid(-logits), 0.0)
        tail_sum = lax.cumsum(log_fail, axis=2, reverse=True) - log_fail
        weights = jnp.where(before, jnp.exp(jax.nn.log_sigmoid(logits) + tail_sum), 0.0)
        return jnp.einsum('hts,shd->thd', weights, head_v)
    outputs = lax.map(one_block, jnp.arange(SEQUENCE_TOKENS // query_block, dtype=jnp.int32))
    return outputs.reshape(SEQUENCE_TOKENS, ATTENTION_HEADS * HD).astype(jnp.bfloat16)

def block_sum(row_block, weight):
    feature_cut = row_block.shape[1] // N_TP

    def add_block(running, block_index):
        part_rows = lax.dynamic_slice_in_dim(row_block, block_index * feature_cut, feature_cut, 1)
        part_weight = lax.dynamic_slice_in_dim(weight, block_index * feature_cut, feature_cut, 0)
        partial_value = jnp.dot(part_rows, part_weight, preferred_element_type=jnp.float32).astype(jnp.bfloat16)
        partial_value = lax.optimization_barrier(partial_value)
        return (running + partial_value.astype(jnp.float32), None)
    start_sum = jnp.zeros((row_block.shape[0], weight.shape[1]), jnp.float32)
    running, _ = lax.scan(add_block, start_sum, jnp.arange(N_TP, dtype=jnp.int32))
    return running

def reference(queries, key_rows, value_rows, break_bias, stream, out_proj, norm_gain, expert_ids, route_weights, gate_proj, up_proj, down_proj, shared_gate, shared_up, shared_down):
    attended = stick_attention(queries, key_rows, value_rows, break_bias)
    mixed = (stream.astype(jnp.float32) + jnp.dot(attended, out_proj, preferred_element_type=jnp.float32)).astype(jnp.bfloat16)
    mixed = lax.optimization_barrier(mixed)
    mixed_f = mixed.astype(jnp.float32)
    inv_rms = lax.rsqrt(lax.optimization_barrier(jnp.mean(mixed_f * mixed_f, axis=1, keepdims=True)) + EPS)
    normed = (mixed_f * inv_rms * norm_gain[None, :]).astype(jnp.bfloat16)
    shared_hidden = (jax.nn.silu(block_sum(normed, shared_gate)) * block_sum(normed, shared_up)).astype(jnp.bfloat16)
    shared_out = jnp.dot(shared_hidden, shared_down, preferred_element_type=jnp.float32)
    rows_max = N_SP * CAP
    padded = jnp.concatenate([normed, jnp.zeros((1, D), jnp.bfloat16)], 0)

    def one_expert(running, expert):
        matches = expert_ids == expert
        chosen = jnp.any(matches, axis=1)
        weight_row = lax.optimization_barrier(jnp.sum(jnp.where(matches, route_weights, 0.0), axis=1))
        weight_pad = jnp.concatenate([weight_row, jnp.zeros((1,), jnp.float32)], 0)
        picked = jnp.nonzero(chosen, size=rows_max, fill_value=SEQUENCE_TOKENS)[0].astype(jnp.int32)
        row_block = padded[picked]
        gate_pre = block_sum(row_block, gate_proj[expert])
        up_pre = block_sum(row_block, up_proj[expert])
        hidden = (jax.nn.silu(gate_pre) * up_pre).astype(jnp.bfloat16)
        expert_out = jnp.dot(hidden, down_proj[expert], preferred_element_type=jnp.float32).astype(jnp.bfloat16)
        scaled = weight_pad[picked][:, None] * expert_out.astype(jnp.float32)
        return (running.at[picked].add(scaled), None)
    routed, _ = lax.scan(one_expert, jnp.zeros((SEQUENCE_TOKENS + 1, D), jnp.float32), jnp.arange(EXPERTS, dtype=jnp.int32))
    return (mixed_f + shared_out + routed[:SEQUENCE_TOKENS]).astype(jnp.bfloat16)
```

```python
import functools

import jax
import jax.numpy as jnp
from jax import lax
from jax.experimental import pallas as pl
from jax.experimental.pallas import tpu as pltpu
from jax.sharding import PartitionSpec as P

EPS = 1e-06
NX = 4
MESH = pl.DeviceIdType.MESH
F32, BF16 = jnp.float32, jnp.bfloat16


def rdma(src, dst, send, recv, device):
    return pltpu.make_async_remote_copy(
        src_ref=src, dst_ref=dst, send_sem=send, recv_sem=recv, device_id=device, device_id_type=MESH
    )


def each(low, high, fn):
    def turn(i, carry):
        fn(i)
        return carry

    lax.fori_loop(low, high, turn, 0)


def offset_near(i, n):
    half = i // 2 + 1
    return jnp.where(lax.rem(i, 2) == 0, half, n - half)


def dot(a, b):
    return jnp.dot(a, b, preferred_element_type=F32)


def dot_nt(a, b):
    return lax.dot_general(a, b, (((1,), (1,)), ((), ())), preferred_element_type=F32)


def halves(value):
    high = value.astype(BF16)
    return high, (value - high.astype(F32)).astype(BF16)


def iota(shape, dim):
    return lax.broadcasted_iota(jnp.int32, shape, dim)


def layer_kernel(
    sizes,
    q_ref,
    k_ref,
    v_ref,
    b_ref,
    stream_ref,
    gain_ref,
    ids_ref,
    rw_ref,
    wo_hbm,
    wg_hbm,
    wu_hbm,
    wd_hbm,
    sg_hbm,
    su_hbm,
    sd_hbm,
    out_ref,
    wo,
    wg,
    wu,
    wd,
    sg,
    su,
    sd,
    kv,
    qbuf,
    part_out,
    part_in,
    tri,
    abuf,
    pt,
    w_hi,
    w_lo,
    mixed_ref,
    snd,
    arr,
    part,
    pre,
    red,
    rs_in,
    spart,
    spre,
    sred,
    srs_in,
    hbuf,
    shbuf,
    ret_out,
    ret_in,
    load_sem,
    kv_send,
    kv_recv,
    q_send,
    q_recv,
    p_send,
    p_recv,
    a_send,
    a_recv,
    af_send,
    af_recv,
    d_send,
    d_recv,
    pre_send,
    pre_recv,
    rs_send,
    rs_recv,
    spre_send,
    spre_recv,
    srs_send,
    srs_recv,
    h_send,
    h_recv,
    hf_send,
    hf_recv,
    sh_send,
    sh_recv,
    shf_send,
    shf_recv,
    r_send,
    r_recv,
):
    nz, nx, ny = sizes
    nsp, ntp = nz * nx, ny * 2
    tok, hd = q_ref.shape
    feat = stream_ref.shape[1]
    ffe = wg.shape[1]
    nslot = nsp * snd.shape[1]
    per_dest = snd.shape[1]
    cap = per_dest // 2
    nexp = nsp * 2
    width = feat * ntp
    sp, tp = lax.axis_index("sp"), lax.axis_index("tp")
    z, x = sp // nx, lax.rem(sp, nx)
    y, c = tp // 2, lax.rem(tp, 2)
    partner = (sp, y * 2 + 1 - c)

    def in_column(yy):
        return (sp, yy * 2 + c)

    loads = [
        pltpu.make_async_copy(src, dst, load_sem.at[i])
        for i, (src, dst) in enumerate(
            [(wo_hbm, wo), (sg_hbm, sg), (su_hbm, su), (wg_hbm, wg), (wu_hbm, wu), (sd_hbm, sd), (wd_hbm, wd)]
        )
    ]

    barrier = pltpu.get_barrier_semaphore()

    def greet_sp(i):
        pl.semaphore_signal(
            barrier, inc=1, device_id=(lax.rem(sp + i, nsp), tp), device_id_type=MESH
        )

    def greet_tp(i):
        pl.semaphore_signal(barrier, inc=1, device_id=in_column(lax.rem(y + i, ny)), device_id_type=MESH)

    each(1, nsp, greet_sp)
    each(1, ny, greet_tp)
    pl.semaphore_signal(barrier, inc=1, device_id=partner, device_id_type=MESH)
    for copy in loads:
        copy.start()

    eye = iota((tok, tok), 0) == iota((tok, tok), 1)

    def to_row(column):
        return jnp.sum(jnp.where(eye, column, 0.0), axis=0, keepdims=True)

    def to_column(row):
        return jnp.sum(jnp.where(eye, row, 0.0), axis=1, keepdims=True)

    kv[x, 0:tok, :] = k_ref[...]
    kv[x, tok : 2 * tok, :] = v_ref[...]
    bias_row = to_row(b_ref[...].astype(F32))
    kv[x, 2 * tok : 2 * tok + 16, :] = jnp.broadcast_to(bias_row, (16, tok)).astype(BF16)
    hk = (nx // 2) * tok
    tri[...] = (iota((hk, hk), 0) > iota((hk, hk), 1)).astype(BF16)

    pl.semaphore_wait(barrier, nsp - 1 + ny)

    def kv_copy(i):
        peer = lax.rem(x + i, nx)
        return rdma(kv.at[x], kv.at[x], kv_send.at[i], kv_recv.at[x], (z * nx + peer, tp))

    def q_copy(i):
        return rdma(q_ref, qbuf.at[z], q_send.at[i], q_recv.at[z], ((z - i) * nx + x, tp))

    each(1, nx, lambda i: kv_copy(i).start())
    each(1, z + 1, lambda i: q_copy(i).start())

    ids = ids_ref[...]
    rw = rw_ref[...]
    exp_lane = iota((tok, nexp), 1)
    first = ids[:, 0:1] == exp_lane
    second = ids[:, 1:2] == exp_lane
    named = jnp.where(first | second, 1.0, 0.0).astype(BF16)
    earlier = jnp.where(iota((tok, tok), 1) < iota((tok, tok), 0), 1.0, 0.0).astype(BF16)
    rank = dot(earlier, named).astype(BF16)
    spread = jnp.where(iota((nexp, nslot), 1) // cap == iota((nexp, nslot), 0), 1.0, 0.0).astype(BF16)
    weight_hi, weight_lo = halves(jnp.where(first, rw[:, 0:1], 0.0) + jnp.where(second, rw[:, 1:2], 0.0))
    slot_rank = lax.rem(iota((tok, nslot), 1), cap).astype(F32)
    taken = (dot(named, spread) > 0.5) & (dot(rank, spread) == slot_rank)
    taken_f = jnp.where(taken, 1.0, 0.0)
    pt[...] = taken_f.T.astype(BF16)
    w_hi[...] = (taken_f * dot(weight_hi, spread)).astype(BF16)
    w_lo[...] = (taken_f * dot(weight_lo, spread)).astype(BF16)

    def kv_arrive(i):
        xs = lax.rem(x + i, nx)
        rdma(kv.at[xs], kv.at[xs], kv_send.at[i], kv_recv.at[xs], (z * nx + xs, tp)).wait_recv()

    each(1, nx, kv_arrive)

    scale = hd ** (-0.5)

    def attend(q, own):
        logits, fails, parts = [], [], []
        for h in range(2):
            at = range(h * (nx // 2), (h + 1) * (nx // 2))
            keys = jnp.concatenate([kv[i, 0:tok, :] for i in at], axis=0)
            bias = jnp.concatenate([kv[i, 2 * tok : 2 * tok + 1, :] for i in at], axis=1).astype(F32)
            lg = dot_nt(q, keys) * scale + bias
            fail = -(jnp.maximum(lg, 0.0) + jnp.log(1.0 + jnp.exp(-jnp.abs(lg))))
            logits.append(lg + fail)
            if own:
                before = iota((tok, hk), 1) + h * hk < iota((tok, hk), 0) + x * tok
                fail = jnp.where(before, fail, 0.0)
            fails.append(fail)
            parts.append(halves(fail))
        stacked = jnp.concatenate([parts[0][0], parts[1][0], parts[0][1], parts[1][1]], axis=0)
        sums = dot(stacked, tri[...])
        tail0 = sums[0:tok] + sums[2 * tok : 3 * tok]
        tail1 = sums[tok : 2 * tok] + sums[3 * tok : 4 * tok]
        tail0 = tail0 + (tail1[:, 0:1] + fails[1][:, 0:1])
        total = tail0[:, 0:1] + fails[0][:, 0:1]
        acc = jnp.zeros((tok, hd), F32)
        for h, tail in enumerate((tail0, tail1)):
            at = range(h * (nx // 2), (h + 1) * (nx // 2))
            values = jnp.concatenate([kv[i, tok : 2 * tok, :] for i in at], axis=0)
            weights = jnp.exp(logits[h] + tail)
            if own:
                before = iota((tok, hk), 1) + h * hk < iota((tok, hk), 0) + x * tok
                weights = jnp.where(before, weights, 0.0)
            acc = acc + dot(weights.astype(BF16), values)
        return acc, total

    def part_copy(zq):
        return rdma(part_out.at[zq], part_in.at[z], p_send.at[zq], p_recv.at[z], (zq * nx + x, tp))

    def serve(i):
        zq = z + i
        rdma(qbuf.at[zq], qbuf.at[zq], q_send.at[i], q_recv.at[zq], (zq * nx + x, tp)).wait_recv()
        acc, total = attend(qbuf[zq], False)
        part_out[zq, 0:tok, :] = acc.astype(BF16)
        row = to_row(total)
        high, rest = row.astype(BF16), row - row.astype(BF16).astype(F32)
        mid, low = halves(rest)
        at_row = iota((16, tok), 0)
        rows = jnp.where(
            at_row == 0,
            high.astype(F32),
            jnp.where(at_row == 1, mid.astype(F32), jnp.where(at_row == 2, low.astype(F32), 0.0)),
        )
        part_out[zq, tok : tok + 16, :] = rows.astype(BF16)
        part_copy(zq).start()

    each(1, nz - z, serve)
    acc, later = attend(q_ref[...], True)

    def combine(i, carry):
        acc, later = carry
        zs = z - i
        rdma(part_in.at[zs], part_in.at[zs], p_send.at[zs], p_recv.at[zs], (zs * nx + x, tp)).wait_recv()
        summary = part_in[zs, 0:tok, :].astype(F32)
        row = jnp.sum(part_in[zs, tok : tok + 16, :].astype(F32), axis=0, keepdims=True)
        return acc + jnp.exp(later) * summary, later + to_column(row)

    acc, later = lax.fori_loop(1, z + 1, combine, (acc, later))

    def gather_start(buf, send, recv, fsend, frecv):
        mine = buf.at[y, c]

        def to_peer(i):
            off = offset_near(i, ny)
            rdma(mine, mine, send.at[i], recv.at[y], in_column(lax.rem(y + off, ny))).start()

        each(0, ny - 1, to_peer)
        rdma(mine, mine, fsend.at[y], frecv.at[y], partner).start()

    def gather_pass_on(buf, send, recv, fsend, frecv):
        def pass_on(i):
            ys = lax.rem(y + offset_near(i, ny), ny)
            here = buf.at[ys, c]
            rdma(here, here, send.at[i], recv.at[ys], in_column(ys)).wait_recv()
            rdma(here, here, fsend.at[ys], frecv.at[ys], partner).start()

        each(0, ny - 1, pass_on)

        def arrive(ys):
            there = buf.at[ys, 1 - c]
            rdma(there, there, fsend.at[ys], frecv.at[ys], partner).wait_recv()

        each(0, ny, arrive)

    def gather_drain(buf, send, recv, fsend, frecv):
        mine = buf.at[y, c]
        each(0, ny - 1, lambda i: rdma(mine, mine, send.at[i], recv.at[y], partner).wait_send())

        def forwarded(ys):
            here = buf.at[ys, c]
            rdma(here, here, fsend.at[ys], frecv.at[ys], partner).wait_send()

        each(0, ny, forwarded)

    a_args = (abuf, a_send, a_recv, af_send, af_recv)
    abuf[y, c] = acc.astype(BF16)
    gather_start(*a_args)
    gather_pass_on(*a_args)
    loads[0].wait()
    projected = jnp.zeros((tok, feat), F32)
    for i in range(ny):
        heads = jnp.concatenate([abuf[i, 0], abuf[i, 1]], axis=1)
        projected = projected + dot(heads, wo[i * 2 * hd : (i + 1) * 2 * hd, :])
    mixed = (stream_ref[...].astype(F32) + projected).astype(BF16)
    mixed_ref[...] = mixed

    snd[...] = dot(pt[...], mixed).astype(BF16).reshape(nsp, per_dest, feat)

    def dispatch(i):
        to = lax.rem(sp + i, nsp)
        return rdma(snd.at[to], arr.at[sp], d_send.at[i], d_recv.at[sp], (to, tp))

    each(1, nsp, lambda i: dispatch(i).start())
    arr[sp] = snd[sp]

    gain = gain_ref[...]

    def products(rows, lhs_of, gate_w, up_w):
        value = rows.astype(F32)
        squares = jnp.sum(value * value, axis=1, keepdims=True)
        lhs = lhs_of((value * gain).astype(BF16))
        gate = dot(lhs, gate_w).astype(BF16)
        up = dot(lhs, up_w).astype(BF16)
        return gate, up, two_lanes(squares)

    def two_lanes(column):
        high, low = halves(column)
        lane = iota((column.shape[0], 128), 1)
        return jnp.where(
            lane == 0, high.astype(F32), jnp.where(lane == 1, low.astype(F32), 0.0)
        ).astype(BF16)

    def laid(ref, lo, value):
        ref[:, :, lo : lo + value.shape[1]] = value.reshape(ref.shape[0], ref.shape[1], value.shape[1])

    def added(mine, theirs):
        both = mine.astype(F32) + theirs.astype(F32)
        squares = both[:, 2 * ffe : 2 * ffe + 1] + both[:, 2 * ffe + 1 : 2 * ffe + 2]
        return both[:, 0 : 2 * ffe].astype(BF16), two_lanes(squares)

    def activated(total):
        squares = total[:, 2 * ffe : 2 * ffe + 1] + total[:, 2 * ffe + 1 : 2 * ffe + 2]
        inv = lax.rsqrt(squares / width + EPS)
        gate, up = total[:, 0:ffe] * inv, total[:, ffe : 2 * ffe] * inv
        return (gate * jax.nn.sigmoid(gate) * up).astype(BF16)

    loads[1].wait()
    loads[2].wait()
    gate, up, squares = products(mixed, lambda a: a, sg[...], su[...])
    laid(spart, 0, gate)
    laid(spart, ffe, up)
    laid(spart, 2 * ffe, squares)
    ny2 = ny // 2

    def spre_copy(i):
        yy = 2 * i + 1 - c
        return rdma(spart.at[yy], spre.at[i], spre_send.at[i], spre_recv.at[i], partner)

    each(0, ny2, lambda i: spre_copy(i).start())

    def srs_copy(i):
        yy = 2 * i + c
        return rdma(sred.at[i], srs_in.at[y], srs_send.at[i], srs_recv.at[y], in_column(yy))

    def shared_add(i):
        yy = 2 * i + c
        rdma(spre.at[i], spre.at[i], spre_send.at[i], spre_recv.at[i], partner).wait_recv()
        sums, squares = added(spart[yy], spre[i])
        sred[i, :, 0 : 2 * ffe] = sums
        sred[i, :, 2 * ffe : 2 * ffe + 128] = squares

        @pl.when(yy != y)
        def _():
            srs_copy(i).start()

    each(0, ny2, shared_add)

    def arrive(i):
        src = lax.rem(sp + i, nsp)
        rdma(arr.at[src], arr.at[src], d_send.at[i], d_recv.at[src], (src, tp)).wait_recv()

    each(1, nsp, arrive)
    loads[3].wait()
    loads[4].wait()

    def by_expert(a):
        zero = jnp.zeros_like(a)
        mine = lax.rem(iota(a.shape, 0), per_dest) < cap
        return jnp.concatenate([jnp.where(mine, a, zero), jnp.where(mine, zero, a)], axis=1)

    gate, up, squares = products(arr[...].reshape(nslot, feat), by_expert, wg[...], wu[...])
    laid(part, 0, gate)
    laid(part, ffe, up)
    laid(part, 2 * ffe, squares)

    def pre_copy(i):
        yy = lax.rem(y + offset_near(ny - 2 - i, ny), ny)
        yy = jnp.where(i == ny - 1, y, yy)
        return rdma(part.at[yy * 2 + 1 - c], pre.at[yy], pre_send.at[i], pre_recv.at[yy], partner)

    each(0, ny, lambda i: pre_copy(i).start())

    def rs_copy(i):
        yy = lax.rem(y + offset_near(ny - 2 - i, ny), ny)
        return rdma(red.at[yy], rs_in.at[y], rs_send.at[i], rs_recv.at[y], in_column(yy))

    def pair_add(yy):
        rdma(pre.at[yy], pre.at[yy], pre_send.at[0], pre_recv.at[yy], partner).wait_recv()
        sums, squares = added(part[yy * 2 + c], pre[yy])
        red[yy, :, 0 : 2 * ffe] = sums
        red[yy, :, 2 * ffe : 2 * ffe + 128] = squares

    def pair_step(i):
        pair_add(lax.rem(y + offset_near(ny - 2 - i, ny), ny))
        rs_copy(i).start()

    each(0, ny - 1, pair_step)
    pair_add(y)

    sh_args = (shbuf, sh_send, sh_recv, shf_send, shf_recv)
    owner = lax.rem(y, 2) == c

    @pl.when(owner)
    def _():
        def add_in(i, total):
            ys = lax.rem(y + offset_near(i, ny), ny)
            rdma(srs_in.at[ys], srs_in.at[ys], srs_send.at[0], srs_recv.at[ys], partner).wait_recv()
            return total + srs_in[ys].astype(F32)

        total = lax.fori_loop(0, ny - 1, add_in, sred[y // 2].astype(F32))
        shbuf[y] = activated(total)

        def to_peer(i):
            off = offset_near(i, ny)
            rdma(
                shbuf.at[y], shbuf.at[y], sh_send.at[i], sh_recv.at[y], in_column(lax.rem(y + off, ny))
            ).start()

        each(0, ny - 1, to_peer)
        rdma(shbuf.at[y], shbuf.at[y], shf_send.at[y // 2], shf_recv.at[y], partner).start()

    def add_routed(i, total):
        ys = lax.rem(y + offset_near(i, ny), ny)
        rdma(rs_in.at[ys], rs_in.at[ys], rs_send.at[0], rs_recv.at[ys], partner).wait_recv()
        return total + rs_in[ys].astype(F32)

    total = lax.fori_loop(0, ny - 1, add_routed, red[y].astype(F32))
    hbuf[y, c] = activated(total)
    h_args = (hbuf, h_send, h_recv, hf_send, hf_recv)
    gather_start(*h_args)

    def shared_on(i):
        yy = 2 * i + c

        @pl.when(yy != y)
        def _():
            rdma(shbuf.at[yy], shbuf.at[yy], sh_send.at[0], sh_recv.at[yy], partner).wait_recv()
            rdma(shbuf.at[yy], shbuf.at[yy], shf_send.at[i], shf_recv.at[yy], partner).start()

    each(0, ny2, shared_on)
    gather_pass_on(*h_args)

    def expert_rows():
        rows = hbuf[...].reshape(nslot, ffe)
        return by_expert(rows)

    loads[6].wait()
    ret_out[...] = dot(expert_rows(), wd[...]).astype(BF16).reshape(nsp, per_dest, feat)

    def give_back(i):
        to = lax.rem(sp + i, nsp)
        return rdma(ret_out.at[to], ret_in.at[sp], r_send.at[i], r_recv.at[sp], (to, tp))

    each(1, nsp, lambda i: give_back(i).start())
    ret_in[sp] = ret_out[sp]

    def shared_arrive(i):
        yy = 2 * i + 1 - c
        rdma(shbuf.at[yy], shbuf.at[yy], shf_send.at[i], shf_recv.at[yy], partner).wait_recv()

    each(0, ny2, shared_arrive)
    loads[5].wait()
    base = mixed_ref[...].astype(F32) + dot(shbuf[...].reshape(tok, ffe), sd[...])

    each(1, nx, lambda i: kv_copy(i).wait_send())
    each(1, z + 1, lambda i: q_copy(i).wait_send())
    each(1, nz - z, lambda i: part_copy(z + i).wait_send())
    gather_drain(*a_args)
    each(1, nsp, lambda i: dispatch(i).wait_send())
    each(0, ny2, lambda i: spre_copy(i).wait_send())

    def srs_drain(i):
        @pl.when(2 * i + c != y)
        def _():
            srs_copy(i).wait_send()

    each(0, ny2, srs_drain)
    each(0, ny, lambda i: pre_copy(i).wait_send())
    each(0, ny - 1, lambda i: rs_copy(i).wait_send())
    gather_drain(*h_args)

    @pl.when(owner)
    def _():
        each(
            0,
            ny - 1,
            lambda i: rdma(shbuf.at[y], shbuf.at[y], sh_send.at[i], sh_recv.at[y], partner).wait_send(),
        )

    def shared_forwarded(i):
        yy = 2 * i + c
        rdma(shbuf.at[yy], shbuf.at[yy], shf_send.at[i], shf_recv.at[yy], partner).wait_send()

    each(0, ny2, shared_forwarded)

    def returned(i):
        src = lax.rem(sp + i, nsp)
        rdma(ret_in.at[src], ret_in.at[src], r_send.at[i], r_recv.at[src], (src, tp)).wait_recv()

    each(1, nsp, returned)
    rows = ret_in[...].reshape(nslot, feat)
    out_ref[...] = (base + (dot(w_hi[...], rows) + dot(w_lo[...], rows))).astype(BF16)
    each(1, nsp, lambda i: give_back(i).wait_send())


def body(
    nx,
    queries,
    key_rows,
    value_rows,
    break_bias,
    stream,
    out_proj,
    norm_gain,
    expert_ids,
    route_weights,
    gate_proj,
    up_proj,
    down_proj,
    shared_gate,
    shared_up,
    shared_down,
):
    nsp, ntp = lax.axis_size("sp"), lax.axis_size("tp")
    nz, ny = nsp // nx, ntp // 2
    tok, hd = queries.shape
    feat = stream.shape[1]
    experts_local, _, ffe = gate_proj.shape
    ffs = shared_gate.shape[1]
    cap = 2 * expert_ids.shape[1] * tok // (experts_local * nsp)
    per_dest = experts_local * cap
    chunk = nsp * per_dest // ntp
    srows = tok // ny
    wide = 2 * ffe + 128
    hk = (nx // 2) * tok

    def vm(*shape):
        return pltpu.VMEM(shape, BF16)

    def sems(*counts):
        return [pltpu.SemaphoreType.DMA((n,)) for n in counts]

    scratch = [
        vm(*out_proj.shape),
        vm(experts_local * feat, ffe),
        vm(experts_local * feat, ffe),
        vm(experts_local * ffe, feat),
        vm(feat, ffs),
        vm(feat, ffs),
        vm(ffs, feat),
        vm(nx, 2 * tok + 16, hd),
        vm(nz, tok, hd),
        vm(nz, tok + 16, hd),
        vm(nz, tok + 16, hd),
        vm(hk, hk),
        vm(ny, 2, tok, hd),
        vm(nsp * per_dest, tok),
        vm(tok, nsp * per_dest),
        vm(tok, nsp * per_dest),
        vm(tok, feat),
        vm(nsp, per_dest, feat),
        vm(nsp, per_dest, feat),
        vm(ntp, chunk, wide),
        vm(ny, chunk, wide),
        vm(ny, chunk, wide),
        vm(ny, chunk, wide),
        vm(ny, srows, wide),
        vm(ny // 2, srows, wide),
        vm(ny // 2, srows, wide),
        vm(ny, srows, wide),
        vm(ny, 2, chunk, ffe),
        vm(ny, srows, ffs),
        vm(nsp, per_dest, feat),
        vm(nsp, per_dest, feat),
        *sems(7, nx, nx, nz, nz, nz, nz, ny, ny, ny, ny, nsp, nsp, ny, ny, ny, ny),
        *sems(ny // 2, ny // 2, ny // 2, ny, ny, ny, ny, ny, ny, ny, ny // 2, ny, nsp, nsp),
    ]
    small = pl.BlockSpec(memory_space=pltpu.VMEM)
    large = pl.BlockSpec(memory_space=pl.ANY)
    return pl.pallas_call(
        functools.partial(layer_kernel, (nz, nx, ny)),
        out_shape=jax.ShapeDtypeStruct((tok, feat), BF16),
        in_specs=[small] * 8 + [large] * 7,
        out_specs=small,
        scratch_shapes=scratch,
        compiler_params=pltpu.CompilerParams(
            collective_id=0, has_side_effects=True, vmem_limit_bytes=60 * 1024 * 1024
        ),
    )(
        queries,
        key_rows,
        value_rows,
        break_bias,
        stream,
        norm_gain.reshape(1, feat),
        expert_ids,
        route_weights,
        out_proj,
        gate_proj.reshape(experts_local * feat, ffe),
        up_proj.reshape(experts_local * feat, ffe),
        down_proj.reshape(experts_local * ffe, feat),
        shared_gate,
        shared_up,
        shared_down,
    )


def solution(mesh, nx=NX):
    in_specs = (
        P("sp", "tp"),
        P("sp", "tp"),
        P("sp", "tp"),
        P("sp", "tp"),
        P("sp", "tp"),
        P(None, "tp"),
        P("tp"),
        P("sp", None),
        P("sp", None),
        P("sp", "tp", None),
        P("sp", "tp", None),
        P("sp", None, "tp"),
        P("tp", None),
        P("tp", None),
        P(None, "tp"),
    )
    return jax.shard_map(
        functools.partial(body, nx), mesh=mesh, in_specs=in_specs, out_specs=P("sp", "tp"), check_vma=False
    )
```

```python
import functools

import jax
import jax.numpy as jnp
from jax import lax
from jax.experimental import pallas as pl
from jax.experimental.pallas import tpu as pltpu
from jax.sharding import PartitionSpec as P

EPS = 1e-06
NX = 4
MESH = pl.DeviceIdType.MESH
F32, BF16 = jnp.float32, jnp.bfloat16


def rdma(src, dst, send, recv, device):
    return pltpu.make_async_remote_copy(
        src_ref=src, dst_ref=dst, send_sem=send, recv_sem=recv, device_id=device, device_id_type=MESH
    )


def each(low, high, fn):
    def turn(i, carry):
        fn(i)
        return carry

    lax.fori_loop(low, high, turn, 0)


def offset_near(i, n):
    half = i // 2 + 1
    return jnp.where(lax.rem(i, 2) == 0, half, n - half)


def dot(a, b):
    return jnp.dot(a, b, preferred_element_type=F32)


def dot_nt(a, b):
    return lax.dot_general(a, b, (((1,), (1,)), ((), ())), preferred_element_type=F32)


def halves(value):
    high = value.astype(BF16)
    return high, (value - high.astype(F32)).astype(BF16)


def iota(shape, dim):
    return lax.broadcasted_iota(jnp.int32, shape, dim)


def layer_kernel(
    sizes,
    q_hbm,
    k_hbm,
    v_hbm,
    bias_hbm,
    stream_hbm,
    gain_hbm,
    ids_hbm,
    rw_hbm,
    wo_hbm,
    wg_hbm,
    wu_hbm,
    wd_hbm,
    sg_hbm,
    su_hbm,
    sd_hbm,
    out_ref,
    q_ref,
    bias_ref,
    stream_ref,
    gain_ref,
    ids_ref,
    rw_ref,
    wo,
    wg,
    wu,
    wd,
    sg,
    su,
    sd,
    kv,
    qbuf,
    part_out,
    part_in,
    tri,
    abuf,
    pt,
    w_hi,
    w_lo,
    mixed_ref,
    snd,
    arr,
    part,
    pre,
    red,
    hub_in,
    hub_out,
    own_in,
    spart,
    spre,
    sred,
    srs_in,
    hbuf,
    shbuf,
    ret_out,
    ret_in,
    load_sem,
    kv_send,
    kv_recv,
    q_send,
    q_recv,
    p_send,
    p_recv,
    a_send,
    a_recv,
    af_send,
    af_recv,
    d_send,
    d_recv,
    pre_send,
    pre_recv,
    l1_send,
    l1_recv,
    l2_send,
    l2_recv,
    spre_send,
    spre_recv,
    srs_send,
    srs_recv,
    h_send,
    h_recv,
    hf_send,
    hf_recv,
    sh_send,
    sh_recv,
    shf_send,
    shf_recv,
    r_send,
    r_recv,
):
    nz, nx, ny = sizes
    nsp, ntp = nz * nx, ny * 2
    tok, hd = q_ref.shape
    feat = stream_ref.shape[1]
    ffe = wg.shape[1]
    nslot = nsp * snd.shape[1]
    per_dest = snd.shape[1]
    cap = per_dest // 2
    nexp = nsp * 2
    width = feat * ntp
    sp, tp = lax.axis_index("sp"), lax.axis_index("tp")
    z, x = sp // nx, lax.rem(sp, nx)
    y, c = tp // 2, lax.rem(tp, 2)
    partner = (sp, y * 2 + 1 - c)

    def in_column(yy):
        return (sp, yy * 2 + c)

    def load(i, src, dst):
        return pltpu.make_async_copy(src, dst, load_sem.at[i])

    barrier = pltpu.get_barrier_semaphore()

    def greet_sp(i):
        pl.semaphore_signal(
            barrier, inc=1, device_id=(lax.rem(sp + i, nsp), tp), device_id_type=MESH
        )

    def greet_tp(i):
        pl.semaphore_signal(barrier, inc=1, device_id=in_column(lax.rem(y + i, ny)), device_id_type=MESH)

    each(1, nsp, greet_sp)
    each(1, ny, greet_tp)
    pl.semaphore_signal(barrier, inc=1, device_id=partner, device_id_type=MESH)
    loads = [
        load(i, src, dst)
        for i, (src, dst) in enumerate(
            [
                (bias_hbm, bias_ref),
                (k_hbm, kv.at[x, 0:tok]),
                (v_hbm, kv.at[x, tok : 2 * tok]),
                (q_hbm, q_ref),
                (ids_hbm, ids_ref),
                (rw_hbm, rw_ref),
                (stream_hbm, stream_ref),
                (gain_hbm, gain_ref),
                (wo_hbm, wo),
                (sg_hbm, sg),
                (su_hbm, su),
                (wg_hbm, wg),
                (wu_hbm, wu),
                (wd_hbm, wd),
                (sd_hbm, sd),
            ]
        )
    ]
    for copy in loads:
        copy.start()

    eye = iota((tok, tok), 0) == iota((tok, tok), 1)

    def to_row(column):
        return jnp.sum(jnp.where(eye, column, 0.0), axis=0, keepdims=True)

    def to_column(row):
        return jnp.sum(jnp.where(eye, row, 0.0), axis=1, keepdims=True)

    loads[0].wait()
    kv[x, 2 * tok : 2 * tok + 16, :] = jnp.broadcast_to(bias_ref[...].astype(F32), (16, tok)).astype(BF16)
    hk = (nx // 2) * tok
    tri[...] = (iota((hk, hk), 0) > iota((hk, hk), 1)).astype(BF16)
    for i in (1, 2, 3):
        loads[i].wait()

    pl.semaphore_wait(barrier, nsp - 1 + ny)

    def kv_copy(i):
        peer = lax.rem(x + i, nx)
        return rdma(kv.at[x], kv.at[x], kv_send.at[i], kv_recv.at[x], (z * nx + peer, tp))

    def q_copy(i):
        return rdma(q_ref, qbuf.at[z], q_send.at[i], q_recv.at[z], ((z - i) * nx + x, tp))

    each(1, nx, lambda i: kv_copy(i).start())
    each(1, z + 1, lambda i: q_copy(i).start())

    loads[4].wait()
    loads[5].wait()
    exp_lane = iota((tok, nexp), 1).astype(F32)

    def columns(ref):
        return [to_column(ref[i : i + 1, :].astype(F32)) for i in range(2)]

    ids, rw = columns(ids_ref), columns(rw_ref)
    first, second = ids[0] == exp_lane, ids[1] == exp_lane
    named = jnp.where(first | second, 1.0, 0.0).astype(BF16)
    earlier = jnp.where(iota((tok, tok), 1) < iota((tok, tok), 0), 1.0, 0.0).astype(BF16)
    rank = dot(earlier, named).astype(BF16)
    spread = jnp.where(iota((nexp, nslot), 1) // cap == iota((nexp, nslot), 0), 1.0, 0.0).astype(BF16)
    weight_hi, weight_lo = halves(jnp.where(first, rw[0], 0.0) + jnp.where(second, rw[1], 0.0))
    slot_rank = lax.rem(iota((tok, nslot), 1), cap).astype(F32)
    taken = (dot(named, spread) > 0.5) & (dot(rank, spread) == slot_rank)
    taken_f = jnp.where(taken, 1.0, 0.0)
    pt[...] = taken_f.T.astype(BF16)
    w_hi[...] = (taken_f * dot(weight_hi, spread)).astype(BF16)
    w_lo[...] = (taken_f * dot(weight_lo, spread)).astype(BF16)

    def kv_arrive(i):
        xs = lax.rem(x + i, nx)
        rdma(kv.at[xs], kv.at[xs], kv_send.at[i], kv_recv.at[xs], (z * nx + xs, tp)).wait_recv()

    each(1, nx, kv_arrive)

    scale = hd ** (-0.5)

    def attend(q, own):
        logits, fails, parts = [], [], []
        for h in range(2):
            at = range(h * (nx // 2), (h + 1) * (nx // 2))
            keys = jnp.concatenate([kv[i, 0:tok, :] for i in at], axis=0)
            bias = jnp.concatenate([kv[i, 2 * tok : 2 * tok + 1, :] for i in at], axis=1).astype(F32)
            lg = dot_nt(q, keys) * scale + bias
            fail = -(jnp.maximum(lg, 0.0) + jnp.log(1.0 + jnp.exp(-jnp.abs(lg))))
            logits.append(lg + fail)
            if own:
                before = iota((tok, hk), 1) + h * hk < iota((tok, hk), 0) + x * tok
                fail = jnp.where(before, fail, 0.0)
            fails.append(fail)
            parts.append(halves(fail))
        stacked = jnp.concatenate([parts[0][0], parts[1][0], parts[0][1], parts[1][1]], axis=0)
        sums = dot(stacked, tri[...])
        tail0 = sums[0:tok] + sums[2 * tok : 3 * tok]
        tail1 = sums[tok : 2 * tok] + sums[3 * tok : 4 * tok]
        tail0 = tail0 + (tail1[:, 0:1] + fails[1][:, 0:1])
        total = tail0[:, 0:1] + fails[0][:, 0:1]
        acc = jnp.zeros((tok, hd), F32)
        for h, tail in enumerate((tail0, tail1)):
            at = range(h * (nx // 2), (h + 1) * (nx // 2))
            values = jnp.concatenate([kv[i, tok : 2 * tok, :] for i in at], axis=0)
            weights = jnp.exp(logits[h] + tail)
            if own:
                before = iota((tok, hk), 1) + h * hk < iota((tok, hk), 0) + x * tok
                weights = jnp.where(before, weights, 0.0)
            acc = acc + dot(weights.astype(BF16), values)
        return acc, total

    def part_copy(zq):
        return rdma(part_out.at[zq], part_in.at[z], p_send.at[zq], p_recv.at[z], (zq * nx + x, tp))

    def serve_far_first(i):
        off = offset_near(nz - 2 - i, nz)

        @pl.when(z + off < nz)
        def _():
            serve(off)

    def serve(i):
        zq = z + i
        rdma(qbuf.at[zq], qbuf.at[zq], q_send.at[i], q_recv.at[zq], (zq * nx + x, tp)).wait_recv()
        acc, total = attend(qbuf[zq], False)
        part_out[zq, 0:tok, :] = acc.astype(BF16)
        row = to_row(total)
        high, rest = row.astype(BF16), row - row.astype(BF16).astype(F32)
        mid, low = halves(rest)
        at_row = iota((16, tok), 0)
        rows = jnp.where(
            at_row == 0,
            high.astype(F32),
            jnp.where(at_row == 1, mid.astype(F32), jnp.where(at_row == 2, low.astype(F32), 0.0)),
        )
        part_out[zq, tok : tok + 16, :] = rows.astype(BF16)
        part_copy(zq).start()

    each(0, nz - 1, serve_far_first)
    acc, later = attend(q_ref[...], True)

    def combine(i, carry):
        acc, later = carry
        zs = z - i
        rdma(part_in.at[zs], part_in.at[zs], p_send.at[zs], p_recv.at[zs], (zs * nx + x, tp)).wait_recv()
        summary = part_in[zs, 0:tok, :].astype(F32)
        row = jnp.sum(part_in[zs, tok : tok + 16, :].astype(F32), axis=0, keepdims=True)
        return acc + jnp.exp(later) * summary, later + to_column(row)

    acc, later = lax.fori_loop(1, z + 1, combine, (acc, later))

    far_first = (4, 3, 5, 2, 6, 1, 7)

    def gather(buf, send, recv, fsend, frecv):
        def block_copy(k, block, off):
            here = buf.at[c, block]
            return rdma(here, here, send.at[k], recv.at[block], in_column(lax.rem(y + off, ny)))

        def across(block):
            here = buf.at[c, block]
            return rdma(here, here, fsend.at[block], frecv.at[block], partner)

        def start():
            for k, off in enumerate(far_first):
                block_copy(k, y, off).start()
            across(y).start()

        def pass_on():
            for k, off in enumerate(far_first):
                block = lax.rem(y + ny - off, ny)
                block_copy(k, block, off).wait_recv()
                across(block).start()

        def finish():
            def arrive(block):
                there = buf.at[1 - c, block]
                rdma(there, there, fsend.at[block], frecv.at[block], partner).wait_recv()

            each(0, ny, arrive)

        def drain():
            for k, off in enumerate(far_first):
                block_copy(k, y, off).wait_send()
            each(0, ny, lambda block: across(block).wait_send())

        return start, pass_on, finish, drain

    abuf[c, y] = acc.astype(BF16)
    a_start, a_pass, a_finish, a_drain = gather(abuf, a_send, a_recv, af_send, af_recv)
    a_start()
    a_pass()
    a_finish()
    loads[8].wait()
    loads[6].wait()
    projected = jnp.zeros((tok, feat), F32)
    for i in range(ny):
        heads = jnp.concatenate([abuf[0, i], abuf[1, i]], axis=1)
        projected = projected + dot(heads, wo[i * 2 * hd : (i + 1) * 2 * hd, :])
    mixed = (stream_ref[...].astype(F32) + projected).astype(BF16)
    mixed_ref[...] = mixed

    snd[...] = dot(pt[...], mixed).astype(BF16).reshape(nsp, per_dest, feat)

    def block_at(i, sign):
        rank = i // nx
        dz = jnp.where(rank == 0, 0, offset_near(rank - 1, nz))
        dx = lax.rem(i, nx)
        return lax.rem(z + sign * dz + nz, nz) * nx + lax.rem(x + sign * dx + nx, nx)

    def dispatch(i):
        to = block_at(i, -1)
        return rdma(snd.at[to], arr.at[i], d_send.at[i], d_recv.at[i], (to, tp))

    each(1, nsp, lambda i: dispatch(i).start())
    arr[0] = snd[sp]

    loads[7].wait()
    gain = gain_ref[...]

    def products(rows, lhs_of, gate_w, up_w):
        value = rows.astype(F32)
        squares = jnp.sum(value * value, axis=1, keepdims=True)
        lhs = lhs_of((value * gain).astype(BF16))
        gate = dot(lhs, gate_w).astype(BF16)
        up = dot(lhs, up_w).astype(BF16)
        return gate, up, two_lanes(squares)

    def two_lanes(column):
        high, low = halves(column)
        lane = iota((column.shape[0], 128), 1)
        return jnp.where(
            lane == 0, high.astype(F32), jnp.where(lane == 1, low.astype(F32), 0.0)
        ).astype(BF16)

    def laid(ref, lo, value):
        ref[:, :, lo : lo + value.shape[1]] = value.reshape(ref.shape[0], ref.shape[1], value.shape[1])

    def packed(total):
        squares = total[:, 2 * ffe : 2 * ffe + 1] + total[:, 2 * ffe + 1 : 2 * ffe + 2]
        return total[:, 0 : 2 * ffe].astype(BF16), two_lanes(squares)

    def activated(total):
        squares = total[:, 2 * ffe : 2 * ffe + 1] + total[:, 2 * ffe + 1 : 2 * ffe + 2]
        inv = lax.rsqrt(squares / width + EPS)
        gate, up = total[:, 0:ffe] * inv, total[:, ffe : 2 * ffe] * inv
        return (gate * jax.nn.sigmoid(gate) * up).astype(BF16)

    loads[9].wait()
    loads[10].wait()
    gate, up, squares = products(mixed, lambda a: a, sg[...], su[...])
    laid(spart, 0, gate)
    laid(spart, ffe, up)
    laid(spart, 2 * ffe, squares)
    ny2 = ny // 2

    def spre_copy(i):
        yy = 2 * i + 1 - c
        return rdma(spart.at[yy], spre.at[i], spre_send.at[i], spre_recv.at[i], partner)

    each(0, ny2, lambda i: spre_copy(i).start())

    def srs_copy(i):
        yy = 2 * i + c
        return rdma(sred.at[i], srs_in.at[y], srs_send.at[i], srs_recv.at[y], in_column(yy))

    def shared_add(i):
        yy = 2 * i + c
        rdma(spre.at[i], spre.at[i], spre_send.at[i], spre_recv.at[i], partner).wait_recv()
        sums, squares = packed(spart[yy].astype(F32) + spre[i].astype(F32))
        sred[i, :, 0 : 2 * ffe] = sums
        sred[i, :, 2 * ffe : 2 * ffe + 128] = squares

        @pl.when(yy != y)
        def _():
            srs_copy(i).start()

    each(0, ny2, shared_add)

    npos, rows_g, chunk = nsp // 2, nslot // 2, part.shape[3]

    def by_expert(a):
        zero = jnp.zeros_like(a)
        mine = lax.rem(iota(a.shape, 0), per_dest) < cap
        return jnp.concatenate([jnp.where(mine, a, zero), jnp.where(mine, zero, a)], axis=1)

    def pre_copy(g):
        return rdma(part.at[g, 1 - c], pre.at[g], pre_send.at[g], pre_recv.at[g], partner)

    def arrivals(g):
        def arrive(i):
            rdma(arr.at[i], arr.at[i], d_send.at[i], d_recv.at[i], partner).wait_recv()

        each(max(1, g * npos), (g + 1) * npos, arrive)

    def experts(g):
        rows = arr[g * npos : (g + 1) * npos].reshape(rows_g, feat)
        gate, up, squares = products(rows, by_expert, wg[...], wu[...])
        for lo, value in ((0, gate), (ffe, up), (2 * ffe, squares)):
            part[g, :, :, :, lo : lo + value.shape[1]] = value.reshape(2, ny, chunk, value.shape[1])
        pre_copy(g).start()

    def l1_copy(g, r):
        if r == 4:
            side = lax.rem(y, 2)
            hub, k = jnp.where(side == 0, 3, 5), 2
        else:
            side = 0 if r < 4 else 1
            hub, k = (r - 1, r - 2) if r < 4 else (r + 1, ny - r - 2)
        return rdma(
            red.at[g, lax.rem(y + r, ny)],
            hub_in.at[g, side, k],
            l1_send.at[g, r],
            l1_recv.at[g, side, k],
            in_column(lax.rem(y + hub, ny)),
        )

    def pair_add(g):
        pre_copy(g).wait_recv()
        both = part[g, c].astype(F32) + pre[g].astype(F32)
        sums, squares = packed(both.reshape(ny * chunk, both.shape[-1]))
        red[g, :, :, 0 : 2 * ffe] = sums.reshape(ny, chunk, 2 * ffe)
        red[g, :, :, 2 * ffe : 2 * ffe + 128] = squares.reshape(ny, chunk, 128)
        for r in (4, 3, 5, 2, 6):
            l1_copy(g, r).start()

    def l2_copy(g, side):
        to = lax.rem(y + (1 if side == 0 else ny - 1), ny)
        return rdma(hub_out.at[g, side], own_in.at[g, side], l2_send.at[g, side], l2_recv.at[g, side], in_column(to))

    def hub(g):
        for side in range(2):
            def add_in(k, total):
                here = hub_in.at[g, side, k]
                rdma(here, here, l1_send.at[g, 2], l1_recv.at[g, side, k], partner).wait_recv()
                return total + hub_in[g, side, k].astype(F32)

            odd = lax.rem(y, 2)
            mine = red[g, lax.rem(y + (1 if side == 0 else ny - 1), ny)].astype(F32)
            total = lax.fori_loop(0, 2 + odd if side == 0 else 3 - odd, add_in, mine)
            sums, squares = packed(total)
            hub_out[g, side, :, 0 : 2 * ffe] = sums
            hub_out[g, side, :, 2 * ffe : 2 * ffe + 128] = squares
            l2_copy(g, side).start()

    gathers = [gather(hbuf.at[g], h_send.at[g], h_recv.at[g], hf_send.at[g], hf_recv.at[g]) for g in range(2)]

    def own(g):
        total = red[g, y].astype(F32)
        for side in range(2):
            here = own_in.at[g, side]
            rdma(here, here, l2_send.at[g, side], l2_recv.at[g, side], partner).wait_recv()
            total = total + own_in[g, side].astype(F32)
        hbuf[g, c, y] = activated(total)
        gathers[g][0]()

    def give_back(i):
        to = block_at(i, 1)
        return rdma(ret_out.at[i], ret_in.at[sp], r_send.at[i], r_recv.at[i], (to, tp))

    def down(g):
        rows = by_expert(hbuf[g].reshape(rows_g, ffe))
        ret_out[g * npos : (g + 1) * npos] = dot(rows, wd[...]).astype(BF16).reshape(npos, per_dest, feat)
        each(max(1, g * npos), (g + 1) * npos, lambda i: give_back(i).start())
        if g == 0:
            ret_in[sp] = ret_out[0]

    owner = lax.rem(y, 2) == c

    arrivals(0)
    loads[11].wait()
    loads[12].wait()
    experts(0)
    pair_add(0)

    @pl.when(owner)
    def _():
        def add_in(i, total):
            ys = lax.rem(y + offset_near(i, ny), ny)
            rdma(srs_in.at[ys], srs_in.at[ys], srs_send.at[0], srs_recv.at[ys], partner).wait_recv()
            return total + srs_in[ys].astype(F32)

        total = lax.fori_loop(0, ny - 1, add_in, sred[y // 2].astype(F32))
        shbuf[y] = activated(total)

        def to_peer(i):
            off = offset_near(i, ny)
            rdma(
                shbuf.at[y], shbuf.at[y], sh_send.at[i], sh_recv.at[y], in_column(lax.rem(y + off, ny))
            ).start()

        each(0, ny - 1, to_peer)
        rdma(shbuf.at[y], shbuf.at[y], shf_send.at[y // 2], shf_recv.at[y], partner).start()

    arrivals(1)
    experts(1)
    pair_add(1)
    hub(0)
    hub(1)
    own(0)
    own(1)
    gathers[0][1]()
    def shared_on(i):
        yy = 2 * i + c

        @pl.when(yy != y)
        def _():
            rdma(shbuf.at[yy], shbuf.at[yy], sh_send.at[0], sh_recv.at[yy], partner).wait_recv()
            rdma(shbuf.at[yy], shbuf.at[yy], shf_send.at[i], shf_recv.at[yy], partner).start()

    each(0, ny2, shared_on)
    gathers[1][1]()
    gathers[0][2]()
    loads[13].wait()
    down(0)
    gathers[1][2]()
    down(1)

    def shared_arrive(i):
        yy = 2 * i + 1 - c
        rdma(shbuf.at[yy], shbuf.at[yy], shf_send.at[i], shf_recv.at[yy], partner).wait_recv()

    each(0, ny2, shared_arrive)
    loads[14].wait()
    base = mixed_ref[...].astype(F32) + dot(shbuf[...].reshape(tok, ffe), sd[...])

    each(1, nx, lambda i: kv_copy(i).wait_send())
    each(1, z + 1, lambda i: q_copy(i).wait_send())
    each(1, nz - z, lambda i: part_copy(z + i).wait_send())
    a_drain()
    each(1, nsp, lambda i: dispatch(i).wait_send())
    each(0, ny2, lambda i: spre_copy(i).wait_send())

    def srs_drain(i):
        @pl.when(2 * i + c != y)
        def _():
            srs_copy(i).wait_send()

    each(0, ny2, srs_drain)
    for g in range(2):
        pre_copy(g).wait_send()
        for r in (4, 3, 5, 2, 6):
            l1_copy(g, r).wait_send()
        for side in range(2):
            l2_copy(g, side).wait_send()
        gathers[g][3]()

    @pl.when(owner)
    def _():
        each(
            0,
            ny - 1,
            lambda i: rdma(shbuf.at[y], shbuf.at[y], sh_send.at[i], sh_recv.at[y], partner).wait_send(),
        )

    def shared_forwarded(i):
        yy = 2 * i + c
        rdma(shbuf.at[yy], shbuf.at[yy], shf_send.at[i], shf_recv.at[yy], partner).wait_send()

    each(0, ny2, shared_forwarded)

    def returned(i):
        src = block_at(i, -1)
        rdma(ret_in.at[src], ret_in.at[src], r_send.at[i], r_recv.at[i], (src, tp)).wait_recv()

    each(1, nsp, returned)
    rows = ret_in[...].reshape(nslot, feat)
    out_ref[...] = (base + (dot(w_hi[...], rows) + dot(w_lo[...], rows))).astype(BF16)
    each(1, nsp, lambda i: give_back(i).wait_send())


def body(
    nx,
    queries,
    key_rows,
    value_rows,
    break_bias,
    stream,
    out_proj,
    norm_gain,
    expert_ids,
    route_weights,
    gate_proj,
    up_proj,
    down_proj,
    shared_gate,
    shared_up,
    shared_down,
):
    nsp, ntp = lax.axis_size("sp"), lax.axis_size("tp")
    nz, ny = nsp // nx, ntp // 2
    tok, hd = queries.shape
    feat = stream.shape[1]
    experts_local, _, ffe = gate_proj.shape
    ffs = shared_gate.shape[1]
    cap = 2 * expert_ids.shape[1] * tok // (experts_local * nsp)
    per_dest = experts_local * cap
    chunk = nsp * per_dest // ntp // 2
    srows = tok // ny
    wide = 2 * ffe + 128
    hk = (nx // 2) * tok

    def vm(*shape):
        return pltpu.VMEM(shape, BF16)

    def sems(*counts):
        return [pltpu.SemaphoreType.DMA(n if isinstance(n, tuple) else (n,)) for n in counts]

    scratch = [
        vm(tok, hd),
        vm(1, tok),
        vm(tok, feat),
        pltpu.VMEM((1, feat), F32),
        pltpu.VMEM((2, tok), jnp.int32),
        pltpu.VMEM((2, tok), F32),
        vm(*out_proj.shape),
        vm(experts_local * feat, ffe),
        vm(experts_local * feat, ffe),
        vm(experts_local * ffe, feat),
        vm(feat, ffs),
        vm(feat, ffs),
        vm(ffs, feat),
        vm(nx, 2 * tok + 16, hd),
        vm(nz, tok, hd),
        vm(nz, tok + 16, hd),
        vm(nz, tok + 16, hd),
        vm(hk, hk),
        vm(2, ny, tok, hd),
        vm(nsp * per_dest, tok),
        vm(tok, nsp * per_dest),
        vm(tok, nsp * per_dest),
        vm(tok, feat),
        vm(nsp, per_dest, feat),
        vm(nsp, per_dest, feat),
        vm(2, 2, ny, chunk, wide),
        vm(2, ny, chunk, wide),
        vm(2, ny, chunk, wide),
        vm(2, 2, 3, chunk, wide),
        vm(2, 2, chunk, wide),
        vm(2, 2, chunk, wide),
        vm(ny, srows, wide),
        vm(ny // 2, srows, wide),
        vm(ny // 2, srows, wide),
        vm(ny, srows, wide),
        vm(2, 2, ny, chunk, ffe),
        vm(ny, srows, ffs),
        vm(nsp, per_dest, feat),
        vm(nsp, per_dest, feat),
        *sems(15, nx, nx, nz, nz, nz, nz, 7, ny, ny, ny, nsp, nsp, 2, 2, (2, ny), (2, 2, 3), (2, 2), (2, 2)),
        *sems(ny // 2, ny // 2, ny // 2, ny, (2, 7), (2, ny), (2, ny), (2, ny), ny, ny, ny // 2, ny, nsp, nsp),
    ]
    large = pl.BlockSpec(memory_space=pl.ANY)
    return pl.pallas_call(
        functools.partial(layer_kernel, (nz, nx, ny)),
        out_shape=jax.ShapeDtypeStruct((tok, feat), BF16),
        in_specs=[large] * 15,
        out_specs=pl.BlockSpec(memory_space=pltpu.VMEM),
        scratch_shapes=scratch,
        compiler_params=pltpu.CompilerParams(
            collective_id=0, has_side_effects=True, vmem_limit_bytes=60 * 1024 * 1024
        ),
    )(
        queries,
        key_rows,
        value_rows,
        break_bias.T,
        stream,
        norm_gain.reshape(1, feat),
        expert_ids.T,
        route_weights.T,
        out_proj,
        gate_proj.reshape(experts_local * feat, ffe),
        up_proj.reshape(experts_local * feat, ffe),
        down_proj.reshape(experts_local * ffe, feat),
        shared_gate,
        shared_up,
        shared_down,
    )


def solution(mesh, nx=NX):
    in_specs = (
        P("sp", "tp"),
        P("sp", "tp"),
        P("sp", "tp"),
        P("sp", "tp"),
        P("sp", "tp"),
        P(None, "tp"),
        P("tp"),
        P("sp", None),
        P("sp", None),
        P("sp", "tp", None),
        P("sp", "tp", None),
        P("sp", None, "tp"),
        P("tp", None),
        P("tp", None),
        P(None, "tp"),
    )
    return jax.shard_map(
        functools.partial(body, nx), mesh=mesh, in_specs=in_specs, out_specs=P("sp", "tp"), check_vma=False
    )
```

```python
import functools

import jax
import jax.numpy as jnp
from jax import lax
from jax.experimental import pallas as pl
from jax.experimental.pallas import tpu as pltpu
from jax.sharding import PartitionSpec as P

EPS = 1e-06
NX = 4
MESH = pl.DeviceIdType.MESH
F32, BF16 = jnp.float32, jnp.bfloat16


def rdma(src, dst, send, recv, device):
    return pltpu.make_async_remote_copy(
        src_ref=src, dst_ref=dst, send_sem=send, recv_sem=recv, device_id=device, device_id_type=MESH
    )


def each(low, high, fn):
    def turn(i, carry):
        fn(i)
        return carry

    lax.fori_loop(low, high, turn, 0)


def offset_near(i, n):
    half = lax.div(i, 2) + 1
    return jnp.where(lax.rem(i, 2) == 0, half, n - half)


def dot(a, b):
    return jnp.dot(a, b, preferred_element_type=F32)


def dot_nt(a, b):
    return lax.dot_general(a, b, (((1,), (1,)), ((), ())), preferred_element_type=F32)


def halves(value):
    high = value.astype(BF16)
    return high, (value - high.astype(F32)).astype(BF16)


def iota(shape, dim):
    return lax.broadcasted_iota(jnp.int32, shape, dim)


def layer_kernel(
    sizes,
    q_hbm,
    k_hbm,
    v_hbm,
    bias_hbm,
    stream_hbm,
    gain_hbm,
    ids_hbm,
    rw_hbm,
    wo_hbm,
    wg_hbm,
    wu_hbm,
    wd_hbm,
    sg_hbm,
    su_hbm,
    sd_hbm,
    out_ref,
    q_ref,
    bias_ref,
    stream_ref,
    gain_ref,
    ids_ref,
    rw_ref,
    wo,
    wg,
    wu,
    wd,
    sg,
    su,
    sd,
    kv,
    qbuf,
    part_out,
    part_in,
    tri,
    abuf,
    pt,
    w_hi,
    w_lo,
    mixed_ref,
    snd,
    arr,
    red,
    hub_in,
    hub_out,
    own_in,
    spart,
    spre,
    sred,
    srs_in,
    hbuf,
    shbuf,
    ret_out,
    ret_in,
    load_sem,
    kv_send,
    kv_recv,
    q_send,
    q_recv,
    p_send,
    p_recv,
    a_send,
    a_recv,
    af_send,
    af_recv,
    d_send,
    d_recv,
    w_send,
    w_recv,
    l1_send,
    l1_recv,
    l2_send,
    l2_recv,
    spre_send,
    spre_recv,
    srs_send,
    srs_recv,
    h_send,
    h_recv,
    sh_send,
    sh_recv,
    shf_send,
    shf_recv,
    r_send,
    r_recv,
):
    nz, nx, ny = sizes
    nsp, ntp = nz * nx, ny * 2
    tok, hd = q_ref.shape
    feat = stream_ref.shape[1]
    ffe = wg.shape[3]
    nslot = nsp * snd.shape[1]
    per_dest = snd.shape[1]
    cap = per_dest // 2
    nexp = nsp * 2
    width = feat * ntp
    sp, tp = lax.axis_index("sp"), lax.axis_index("tp")
    z, x = sp // nx, lax.rem(sp, nx)
    y, c = tp // 2, lax.rem(tp, 2)
    partner = (sp, y * 2 + 1 - c)

    def in_column(yy):
        return (sp, yy * 2 + c)

    def load(i, src, dst):
        return pltpu.make_async_copy(src, dst, load_sem.at[i])

    barrier = pltpu.get_barrier_semaphore()

    def greet_sp(i):
        pl.semaphore_signal(
            barrier, inc=1, device_id=(lax.rem(sp + i, nsp), tp), device_id_type=MESH
        )

    def greet_tp(i):
        pl.semaphore_signal(barrier, inc=1, device_id=in_column(lax.rem(y + i, ny)), device_id_type=MESH)

    each(1, nsp, greet_sp)
    each(1, ny, greet_tp)
    pl.semaphore_signal(barrier, inc=1, device_id=partner, device_id_type=MESH)
    loads = [
        load(i, src, dst)
        for i, (src, dst) in enumerate(
            [
                (bias_hbm, bias_ref),
                (k_hbm, kv.at[x, 0:tok]),
                (v_hbm, kv.at[x, tok : 2 * tok]),
                (q_hbm, q_ref),
                (ids_hbm, ids_ref),
                (rw_hbm, rw_ref),
                (stream_hbm, stream_ref),
                (gain_hbm, gain_ref.at[c]),
                (wo_hbm, wo),
                (sg_hbm, sg),
                (su_hbm, su),
                (wg_hbm, wg.at[:, c]),
                (wu_hbm, wu.at[:, c]),
                (wd_hbm, wd.at[c]),
                (sd_hbm, sd),
            ]
        )
    ]
    for copy in loads:
        copy.start()

    eye = iota((tok, tok), 0) == iota((tok, tok), 1)

    def to_row(column):
        return jnp.sum(jnp.where(eye, column, 0.0), axis=0, keepdims=True)

    def to_column(row):
        return jnp.sum(jnp.where(eye, row, 0.0), axis=1, keepdims=True)

    loads[0].wait()
    kv[x, 2 * tok : 2 * tok + 16, :] = jnp.broadcast_to(bias_ref[...].astype(F32), (16, tok)).astype(BF16)
    hk = (nx // 2) * tok
    tri[...] = (iota((hk, hk), 0) > iota((hk, hk), 1)).astype(BF16)
    for i in (1, 2, 3):
        loads[i].wait()

    pl.semaphore_wait(barrier, nsp - 1 + ny)

    def kv_copy(i):
        peer = lax.rem(x + i, nx)
        return rdma(kv.at[x], kv.at[x], kv_send.at[i], kv_recv.at[x], (z * nx + peer, tp))

    def q_copy(i):
        return rdma(q_ref, qbuf.at[z], q_send.at[i], q_recv.at[z], ((z - i) * nx + x, tp))

    each(1, nx, lambda i: kv_copy(i).start())
    each(1, z + 1, lambda i: q_copy(i).start())

    swapped = [
        rdma(mine, mine, w_send.at[i], w_recv.at[i], partner)
        for i, mine in enumerate((wg.at[:, c], wu.at[:, c], wd.at[c], gain_ref.at[c]))
    ]
    for i, copy in zip((11, 12, 13, 7), swapped):
        loads[i].wait()
        copy.start()

    loads[4].wait()
    loads[5].wait()
    exp_lane = iota((tok, nexp), 1).astype(F32)

    def columns(ref):
        return [to_column(ref[i : i + 1, :].astype(F32)) for i in range(2)]

    ids, rw = columns(ids_ref), columns(rw_ref)
    first, second = ids[0] == exp_lane, ids[1] == exp_lane
    named = jnp.where(first | second, 1.0, 0.0).astype(BF16)
    earlier = jnp.where(iota((tok, tok), 1) < iota((tok, tok), 0), 1.0, 0.0).astype(BF16)
    rank = dot(earlier, named).astype(BF16)
    spread = jnp.where(iota((nexp, nslot), 1) // cap == iota((nexp, nslot), 0), 1.0, 0.0).astype(BF16)
    weight_hi, weight_lo = halves(jnp.where(first, rw[0], 0.0) + jnp.where(second, rw[1], 0.0))
    slot_rank = lax.rem(iota((tok, nslot), 1), cap).astype(F32)
    taken = (dot(named, spread) > 0.5) & (dot(rank, spread) == slot_rank)
    taken_f = jnp.where(taken, 1.0, 0.0)
    pt[...] = taken_f.T.astype(BF16)
    w_hi[...] = (taken_f * dot(weight_hi, spread)).astype(BF16)
    w_lo[...] = (taken_f * dot(weight_lo, spread)).astype(BF16)

    def kv_arrive(i):
        xs = lax.rem(x + i, nx)
        rdma(kv.at[xs], kv.at[xs], kv_send.at[i], kv_recv.at[xs], (z * nx + xs, tp)).wait_recv()

    each(1, nx, kv_arrive)

    scale = hd ** (-0.5)

    def attend(q, own):
        logits, fails, parts = [], [], []
        for h in range(2):
            at = range(h * (nx // 2), (h + 1) * (nx // 2))
            keys = jnp.concatenate([kv[i, 0:tok, :] for i in at], axis=0)
            bias = jnp.concatenate([kv[i, 2 * tok : 2 * tok + 1, :] for i in at], axis=1).astype(F32)
            lg = dot_nt(q, keys) * scale + bias
            fail = -(jnp.maximum(lg, 0.0) + jnp.log(1.0 + jnp.exp(-jnp.abs(lg))))
            logits.append(lg + fail)
            if own:
                before = iota((tok, hk), 1) + h * hk < iota((tok, hk), 0) + x * tok
                fail = jnp.where(before, fail, 0.0)
            fails.append(fail)
            parts.append(halves(fail))
        stacked = jnp.concatenate([parts[0][0], parts[1][0], parts[0][1], parts[1][1]], axis=0)
        sums = dot(stacked, tri[...])
        tail0 = sums[0:tok] + sums[2 * tok : 3 * tok]
        tail1 = sums[tok : 2 * tok] + sums[3 * tok : 4 * tok]
        tail0 = tail0 + (tail1[:, 0:1] + fails[1][:, 0:1])
        total = tail0[:, 0:1] + fails[0][:, 0:1]
        acc = jnp.zeros((tok, hd), F32)
        for h, tail in enumerate((tail0, tail1)):
            at = range(h * (nx // 2), (h + 1) * (nx // 2))
            values = jnp.concatenate([kv[i, tok : 2 * tok, :] for i in at], axis=0)
            weights = jnp.exp(logits[h] + tail)
            if own:
                before = iota((tok, hk), 1) + h * hk < iota((tok, hk), 0) + x * tok
                weights = jnp.where(before, weights, 0.0)
            acc = acc + dot(weights.astype(BF16), values)
        return acc, total

    def part_copy(zq):
        return rdma(part_out.at[zq], part_in.at[z], p_send.at[zq], p_recv.at[z], (zq * nx + x, tp))

    def serve_far_first(i):
        off = offset_near(nz - 2 - i, nz)

        @pl.when(z + off < nz)
        def _():
            serve(off)

    def serve(i):
        zq = z + i
        rdma(qbuf.at[zq], qbuf.at[zq], q_send.at[i], q_recv.at[zq], (zq * nx + x, tp)).wait_recv()
        acc, total = attend(qbuf[zq], False)
        part_out[zq, 0:tok, :] = acc.astype(BF16)
        row = to_row(total)
        high, rest = row.astype(BF16), row - row.astype(BF16).astype(F32)
        mid, low = halves(rest)
        at_row = iota((16, tok), 0)
        rows = jnp.where(
            at_row == 0,
            high.astype(F32),
            jnp.where(at_row == 1, mid.astype(F32), jnp.where(at_row == 2, low.astype(F32), 0.0)),
        )
        part_out[zq, tok : tok + 16, :] = rows.astype(BF16)
        part_copy(zq).start()

    each(0, nz - 1, serve_far_first)
    acc, later = attend(q_ref[...], True)

    def combine(i, carry):
        acc, later = carry
        zs = z - i
        rdma(part_in.at[zs], part_in.at[zs], p_send.at[zs], p_recv.at[zs], (zs * nx + x, tp)).wait_recv()
        summary = part_in[zs, 0:tok, :].astype(F32)
        row = jnp.sum(part_in[zs, tok : tok + 16, :].astype(F32), axis=0, keepdims=True)
        return acc + jnp.exp(later) * summary, later + to_column(row)

    acc, later = lax.fori_loop(1, z + 1, combine, (acc, later))

    far_first = (4, 3, 5, 2, 6, 1, 7)

    def gather(buf, send, recv, fsend=None, frecv=None):
        def block_copy(k, block, off):
            here = buf.at[c, block] if fsend is not None else buf.at[block]
            return rdma(here, here, send.at[k], recv.at[block], in_column(lax.rem(y + off, ny)))

        def across(block):
            here = buf.at[c, block]
            return rdma(here, here, fsend.at[block], frecv.at[block], partner)

        def start():
            for k, off in enumerate(far_first):
                block_copy(k, y, off).start()
            if fsend is not None:
                across(y).start()

        def pass_on():
            for k, off in enumerate(far_first):
                block = lax.rem(y + ny - off, ny)
                block_copy(k, block, off).wait_recv()
                if fsend is not None:
                    across(block).start()

        def finish():
            def arrive(block):
                there = buf.at[1 - c, block]
                rdma(there, there, fsend.at[block], frecv.at[block], partner).wait_recv()

            each(0, ny, arrive)

        def drain():
            for k, off in enumerate(far_first):
                block_copy(k, y, off).wait_send()
            if fsend is not None:
                each(0, ny, lambda block: across(block).wait_send())

        return start, pass_on, finish, drain

    abuf[c, y] = acc.astype(BF16)
    a_start, a_pass, a_finish, a_drain = gather(abuf, a_send, a_recv, af_send, af_recv)
    a_start()
    a_pass()
    a_finish()
    loads[8].wait()
    loads[6].wait()
    projected = jnp.zeros((tok, feat), F32)
    for i in range(ny):
        heads = jnp.concatenate([abuf[0, i], abuf[1, i]], axis=1)
        projected = projected + dot(heads, wo[i * 2 * hd : (i + 1) * 2 * hd, :])
    mixed = (stream_ref[...].astype(F32) + projected).astype(BF16)
    mixed_ref[...] = mixed

    snd[...] = dot(pt[...], mixed).astype(BF16).reshape(nsp, per_dest, feat)

    def block_at(i, sign):
        rank = lax.div(i, nx)
        dz = jnp.where(rank == 0, 0, offset_near(rank - 1, nz))
        dx = lax.rem(i, nx)
        return lax.rem(z + sign * dz + nz, nz) * nx + lax.rem(x + sign * dx + nx, nx)

    def dispatch(i):
        to = block_at(i, -1)
        at, core = lax.div(i, 2), lax.rem(i, 2)
        return rdma(snd.at[to], arr.at[at, c], d_send.at[i], d_recv.at[at, c], (to, y * 2 + core))

    def dispatch_own():
        return rdma(snd.at[sp], arr.at[0, c], d_send.at[0], d_recv.at[0, c], partner)

    each(1, nsp, lambda i: dispatch(i).start())

    @pl.when(c == 0)
    def _():
        arr[0, 0] = snd[sp]

    @pl.when(c == 1)
    def _():
        dispatch_own().start()


    def products(rows, gain, lhs_of, gate_w, up_w):
        value = rows.astype(F32)
        squares = jnp.sum(value * value, axis=1, keepdims=True)
        lhs = lhs_of((value * gain).astype(BF16))
        gate = dot(lhs, gate_w).astype(BF16)
        up = dot(lhs, up_w).astype(BF16)
        return gate, up, two_lanes(squares)

    def two_lanes(column):
        high, low = halves(column)
        lane = iota((column.shape[0], 128), 1)
        return jnp.where(
            lane == 0, high.astype(F32), jnp.where(lane == 1, low.astype(F32), 0.0)
        ).astype(BF16)

    def laid(ref, lo, value):
        ref[:, :, lo : lo + value.shape[1]] = value.reshape(ref.shape[0], ref.shape[1], value.shape[1])

    def packed(total):
        squares = total[:, 2 * ffe : 2 * ffe + 1] + total[:, 2 * ffe + 1 : 2 * ffe + 2]
        return total[:, 0 : 2 * ffe].astype(BF16), two_lanes(squares)

    def activated(total):
        squares = total[:, 2 * ffe : 2 * ffe + 1] + total[:, 2 * ffe + 1 : 2 * ffe + 2]
        inv = lax.rsqrt(squares / width + EPS)
        gate, up = total[:, 0:ffe] * inv, total[:, ffe : 2 * ffe] * inv
        return (gate * jax.nn.sigmoid(gate) * up).astype(BF16)

    loads[9].wait()
    loads[10].wait()
    gate, up, squares = products(mixed, gain_ref[c], lambda a: a, sg[...], su[...])
    laid(spart, 0, gate)
    laid(spart, ffe, up)
    laid(spart, 2 * ffe, squares)
    ny2 = ny // 2

    def spre_copy(i):
        yy = 2 * i + 1 - c
        return rdma(spart.at[yy], spre.at[i], spre_send.at[i], spre_recv.at[i], partner)

    each(0, ny2, lambda i: spre_copy(i).start())

    def srs_copy(i):
        yy = 2 * i + c
        return rdma(sred.at[i], srs_in.at[y], srs_send.at[i], srs_recv.at[y], in_column(yy))

    def shared_add(i):
        yy = 2 * i + c
        rdma(spre.at[i], spre.at[i], spre_send.at[i], spre_recv.at[i], partner).wait_recv()
        sums, squares = packed(spart[yy].astype(F32) + spre[i].astype(F32))
        sred[i, :, 0 : 2 * ffe] = sums
        sred[i, :, 2 * ffe : 2 * ffe + 128] = squares

        @pl.when(yy != y)
        def _():
            srs_copy(i).start()

    each(0, ny2, shared_add)

    npos, chunk = nsp // 4, red.shape[2]
    rows_g = npos * per_dest

    def by_expert(a):
        zero = jnp.zeros_like(a)
        mine = lax.rem(iota(a.shape, 0), per_dest) < cap
        return jnp.concatenate([jnp.where(mine, a, zero), jnp.where(mine, zero, a)], axis=1)

    def arrivals(g):
        def arrive(at):
            for core in range(2):
                here = arr.at[at, core]
                rdma(here, here, d_send.at[1], d_recv.at[at, core], partner).wait_recv()

        each(max(1, g * npos), (g + 1) * npos, arrive)
        if g == 0:
            here = arr.at[0, 1]
            rdma(here, here, d_send.at[1], d_recv.at[0, 1], partner).wait_recv()

            @pl.when(c == 1)
            def _():
                here = arr.at[0, 0]
                rdma(here, here, d_send.at[1], d_recv.at[0, 0], partner).wait_recv()

    def experts(g):
        at = slice(g * npos, (g + 1) * npos)
        rows = jnp.concatenate([arr[at, core].reshape(rows_g, feat) for core in range(2)], axis=1)
        gain = jnp.concatenate([gain_ref[0], gain_ref[1]], axis=1)
        gate, up, squares = products(
            rows, gain, by_expert, wg[...].reshape(4 * feat, ffe), wu[...].reshape(4 * feat, ffe)
        )
        for lo, value in ((0, gate), (ffe, up), (2 * ffe, squares)):
            red[g, :, :, lo : lo + value.shape[1]] = value.reshape(ny, chunk, value.shape[1])
        for r in (4, 3, 5, 2, 6):
            l1_copy(g, r).start()

    def l1_copy(g, r):
        if r == 4:
            side = lax.rem(y, 2)
            hub, k = jnp.where(side == 0, 3, 5), 2
        else:
            side = 0 if r < 4 else 1
            hub, k = (r - 1, r - 2) if r < 4 else (r + 1, ny - r - 2)
        return rdma(
            red.at[g, lax.rem(y + r, ny)],
            hub_in.at[g, side, k],
            l1_send.at[g, r],
            l1_recv.at[g, side, k],
            in_column(lax.rem(y + hub, ny)),
        )

    def l2_copy(g, side):
        to = lax.rem(y + (1 if side == 0 else ny - 1), ny)
        return rdma(hub_out.at[g, side], own_in.at[g, side], l2_send.at[g, side], l2_recv.at[g, side], in_column(to))

    def hub(g):
        for side in range(2):
            def add_in(k, total):
                here = hub_in.at[g, side, k]
                rdma(here, here, l1_send.at[g, 2], l1_recv.at[g, side, k], partner).wait_recv()
                return total + hub_in[g, side, k].astype(F32)

            odd = lax.rem(y, 2)
            mine = red[g, lax.rem(y + (1 if side == 0 else ny - 1), ny)].astype(F32)
            total = lax.fori_loop(0, 2 + odd if side == 0 else 3 - odd, add_in, mine)
            sums, squares = packed(total)
            hub_out[g, side, :, 0 : 2 * ffe] = sums
            hub_out[g, side, :, 2 * ffe : 2 * ffe + 128] = squares
            l2_copy(g, side).start()

    gathers = [gather(hbuf.at[g], h_send.at[g], h_recv.at[g]) for g in range(2)]

    def own(g):
        total = red[g, y].astype(F32)
        for side in range(2):
            here = own_in.at[g, side]
            rdma(here, here, l2_send.at[g, side], l2_recv.at[g, side], partner).wait_recv()
            total = total + own_in[g, side].astype(F32)
        hbuf[g, y] = activated(total)
        gathers[g][0]()

    def give_back(at, core):
        i = 2 * at + c
        to = block_at(i, 1)
        return rdma(ret_out.at[at, core], ret_in.at[sp], r_send.at[at, core], r_recv.at[i], (to, y * 2 + core))

    def down(g):
        rows = by_expert(hbuf[g].reshape(rows_g, ffe))
        at = slice(g * npos, (g + 1) * npos)
        for core in range(2):
            ret_out[at, core] = dot(rows, wd[core]).astype(BF16).reshape(npos, per_dest, feat)

        def back(at):
            for core in range(2):
                give_back(at, core).start()

        each(max(1, g * npos), (g + 1) * npos, back)
        if g == 0:
            give_back(0, 1).start()

            @pl.when(c == 1)
            def _():
                give_back(0, 0).start()

            @pl.when(c == 0)
            def _():
                ret_in[sp] = ret_out[0, 0]

    owner = lax.rem(y, 2) == c

    arrivals(0)
    for i in (0, 1, 3):
        swapped[i].wait_recv()
    experts(0)

    @pl.when(owner)
    def _():
        def add_in(i, total):
            ys = lax.rem(y + offset_near(i, ny), ny)
            rdma(srs_in.at[ys], srs_in.at[ys], srs_send.at[0], srs_recv.at[ys], partner).wait_recv()
            return total + srs_in[ys].astype(F32)

        total = lax.fori_loop(0, ny - 1, add_in, sred[y // 2].astype(F32))
        shbuf[y] = activated(total)

        def to_peer(i):
            off = offset_near(i, ny)
            rdma(
                shbuf.at[y], shbuf.at[y], sh_send.at[i], sh_recv.at[y], in_column(lax.rem(y + off, ny))
            ).start()

        each(0, ny - 1, to_peer)
        rdma(shbuf.at[y], shbuf.at[y], shf_send.at[y // 2], shf_recv.at[y], partner).start()

    arrivals(1)
    experts(1)
    hub(0)
    hub(1)
    own(0)
    own(1)
    gathers[0][1]()
    def shared_on(i):
        yy = 2 * i + c

        @pl.when(yy != y)
        def _():
            rdma(shbuf.at[yy], shbuf.at[yy], sh_send.at[0], sh_recv.at[yy], partner).wait_recv()
            rdma(shbuf.at[yy], shbuf.at[yy], shf_send.at[i], shf_recv.at[yy], partner).start()

    each(0, ny2, shared_on)
    swapped[2].wait_recv()
    down(0)
    gathers[1][1]()
    down(1)

    def shared_arrive(i):
        yy = 2 * i + 1 - c
        rdma(shbuf.at[yy], shbuf.at[yy], shf_send.at[i], shf_recv.at[yy], partner).wait_recv()

    each(0, ny2, shared_arrive)
    loads[14].wait()
    base = mixed_ref[...].astype(F32) + dot(shbuf[...].reshape(tok, ffe), sd[...])

    each(1, nx, lambda i: kv_copy(i).wait_send())
    each(1, z + 1, lambda i: q_copy(i).wait_send())
    each(1, nz - z, lambda i: part_copy(z + i).wait_send())
    a_drain()
    each(1, nsp, lambda i: dispatch(i).wait_send())

    @pl.when(c == 1)
    def _():
        dispatch_own().wait_send()

    for copy in swapped:
        copy.wait_send()
    each(0, ny2, lambda i: spre_copy(i).wait_send())

    def srs_drain(i):
        @pl.when(2 * i + c != y)
        def _():
            srs_copy(i).wait_send()

    each(0, ny2, srs_drain)
    for g in range(2):
        for r in (4, 3, 5, 2, 6):
            l1_copy(g, r).wait_send()
        for side in range(2):
            l2_copy(g, side).wait_send()
        gathers[g][3]()

    @pl.when(owner)
    def _():
        each(
            0,
            ny - 1,
            lambda i: rdma(shbuf.at[y], shbuf.at[y], sh_send.at[i], sh_recv.at[y], partner).wait_send(),
        )

    def shared_forwarded(i):
        yy = 2 * i + c
        rdma(shbuf.at[yy], shbuf.at[yy], shf_send.at[i], shf_recv.at[yy], partner).wait_send()

    each(0, ny2, shared_forwarded)

    def returned(i):
        src = block_at(i, -1)
        rdma(ret_in.at[src], ret_in.at[src], r_send.at[i], r_recv.at[i], (src, tp)).wait_recv()

    each(1, nsp, returned)

    @pl.when(c == 1)
    def _():
        returned(0)

    rows = ret_in[...].reshape(nslot, feat)
    out_ref[...] = (base + (dot(w_hi[...], rows) + dot(w_lo[...], rows))).astype(BF16)

    def given(at):
        for core in range(2):
            give_back(at, core).wait_send()

    each(1, nsp // 2, given)
    give_back(0, 1).wait_send()

    @pl.when(c == 1)
    def _():
        give_back(0, 0).wait_send()


def body(
    nx,
    queries,
    key_rows,
    value_rows,
    break_bias,
    stream,
    out_proj,
    norm_gain,
    expert_ids,
    route_weights,
    gate_proj,
    up_proj,
    down_proj,
    shared_gate,
    shared_up,
    shared_down,
):
    nsp, ntp = lax.axis_size("sp"), lax.axis_size("tp")
    nz, ny = nsp // nx, ntp // 2
    tok, hd = queries.shape
    feat = stream.shape[1]
    experts_local, _, ffe = gate_proj.shape
    ffs = shared_gate.shape[1]
    cap = 2 * expert_ids.shape[1] * tok // (experts_local * nsp)
    per_dest = experts_local * cap
    chunk = nsp * per_dest // ntp // 2
    srows = tok // ny
    wide = 2 * ffe + 128
    hk = (nx // 2) * tok

    def vm(*shape):
        return pltpu.VMEM(shape, BF16)

    def sems(*counts):
        return [pltpu.SemaphoreType.DMA(n if isinstance(n, tuple) else (n,)) for n in counts]

    scratch = [
        vm(tok, hd),
        vm(1, tok),
        vm(tok, feat),
        pltpu.VMEM((2, 1, feat), F32),
        pltpu.VMEM((2, tok), jnp.int32),
        pltpu.VMEM((2, tok), F32),
        vm(*out_proj.shape),
        vm(experts_local, 2, feat, ffe),
        vm(experts_local, 2, feat, ffe),
        vm(2, experts_local * ffe, feat),
        vm(feat, ffs),
        vm(feat, ffs),
        vm(ffs, feat),
        vm(nx, 2 * tok + 16, hd),
        vm(nz, tok, hd),
        vm(nz, tok + 16, hd),
        vm(nz, tok + 16, hd),
        vm(hk, hk),
        vm(2, ny, tok, hd),
        vm(nsp * per_dest, tok),
        vm(tok, nsp * per_dest),
        vm(tok, nsp * per_dest),
        vm(tok, feat),
        vm(nsp, per_dest, feat),
        vm(nsp // 2, 2, per_dest, feat),
        vm(2, ny, chunk, wide),
        vm(2, 2, 3, chunk, wide),
        vm(2, 2, chunk, wide),
        vm(2, 2, chunk, wide),
        vm(ny, srows, wide),
        vm(ny // 2, srows, wide),
        vm(ny // 2, srows, wide),
        vm(ny, srows, wide),
        vm(2, ny, chunk, ffe),
        vm(ny, srows, ffs),
        vm(nsp // 2, 2, per_dest, feat),
        vm(nsp, per_dest, feat),
        *sems(15, nx, nx, nz, nz, nz, nz, 7, ny, ny, ny, nsp, (nsp // 2, 2), 4, 4, (2, ny), (2, 2, 3), (2, 2), (2, 2)),
        *sems(ny // 2, ny // 2, ny // 2, ny, (2, 7), (2, ny), ny, ny, ny // 2, ny, (nsp // 2, 2), nsp),
    ]
    large = pl.BlockSpec(memory_space=pl.ANY)
    return pl.pallas_call(
        functools.partial(layer_kernel, (nz, nx, ny)),
        out_shape=jax.ShapeDtypeStruct((tok, feat), BF16),
        in_specs=[large] * 15,
        out_specs=pl.BlockSpec(memory_space=pltpu.VMEM),
        scratch_shapes=scratch,
        compiler_params=pltpu.CompilerParams(
            collective_id=0, has_side_effects=True, vmem_limit_bytes=60 * 1024 * 1024
        ),
    )(
        queries,
        key_rows,
        value_rows,
        break_bias.T,
        stream,
        norm_gain.reshape(1, feat),
        expert_ids.T,
        route_weights.T,
        out_proj,
        gate_proj,
        up_proj,
        down_proj.reshape(experts_local * ffe, feat),
        shared_gate,
        shared_up,
        shared_down,
    )


def solution(mesh, nx=NX):
    in_specs = (
        P("sp", "tp"),
        P("sp", "tp"),
        P("sp", "tp"),
        P("sp", "tp"),
        P("sp", "tp"),
        P(None, "tp"),
        P("tp"),
        P("sp", None),
        P("sp", None),
        P("sp", "tp", None),
        P("sp", "tp", None),
        P("sp", None, "tp"),
        P("tp", None),
        P("tp", None),
        P(None, "tp"),
    )
    return jax.shard_map(
        functools.partial(body, nx), mesh=mesh, in_specs=in_specs, out_specs=P("sp", "tp"), check_vma=False
    )
```

```python
import functools

import jax
import jax.numpy as jnp
from jax import lax
from jax.experimental import pallas as pl
from jax.experimental.pallas import tpu as pltpu
from jax.sharding import PartitionSpec as P

EPS = 1e-06
NX = 4
MESH = pl.DeviceIdType.MESH
F32, BF16 = jnp.float32, jnp.bfloat16


def rdma(src, dst, send, recv, device):
    return pltpu.make_async_remote_copy(
        src_ref=src, dst_ref=dst, send_sem=send, recv_sem=recv, device_id=device, device_id_type=MESH
    )


def each(low, high, fn):
    def turn(i, carry):
        fn(i)
        return carry

    lax.fori_loop(low, high, turn, 0)


def offset_near(i, n):
    half = lax.div(i, 2) + 1
    return jnp.where(lax.rem(i, 2) == 0, half, n - half)


def dot(a, b):
    return jnp.dot(a, b, preferred_element_type=F32)


def dot_nt(a, b):
    return lax.dot_general(a, b, (((1,), (1,)), ((), ())), preferred_element_type=F32)


def halves(value):
    high = value.astype(BF16)
    return high, (value - high.astype(F32)).astype(BF16)


def iota(shape, dim):
    return lax.broadcasted_iota(jnp.int32, shape, dim)


def layer_kernel(
    sizes,
    q_hbm,
    k_hbm,
    v_hbm,
    bias_hbm,
    stream_hbm,
    gain_hbm,
    ids_hbm,
    rw_hbm,
    wo_hbm,
    wg_hbm,
    wu_hbm,
    wd_hbm,
    sg_hbm,
    su_hbm,
    sd_hbm,
    out_ref,
    q_ref,
    bias_ref,
    stream_ref,
    gain_ref,
    ids_ref,
    rw_ref,
    wo,
    wg,
    wu,
    wd,
    sg,
    su,
    sd,
    kv,
    qbuf,
    part_out,
    part_in,
    tri,
    abuf,
    pt,
    w_hi,
    w_lo,
    mixed_ref,
    snd,
    arr,
    red,
    hub_in,
    hub_out,
    own_in,
    spart,
    spre,
    sred,
    srs_in,
    hbuf,
    shbuf,
    ret_out,
    ret_in,
    load_sem,
    kv_send,
    kv_recv,
    q_send,
    q_recv,
    p_send,
    p_recv,
    a_send,
    a_recv,
    af_send,
    af_recv,
    d_send,
    d_recv,
    w_send,
    w_recv,
    l1_send,
    l1_recv,
    l2_send,
    l2_recv,
    spre_send,
    spre_recv,
    srs_send,
    srs_recv,
    h_send,
    h_recv,
    sh_send,
    sh_recv,
    shf_send,
    shf_recv,
    r_send,
    r_recv,
):
    nz, nx, ny = sizes
    nsp, ntp = nz * nx, ny * 2
    tok, hd = q_ref.shape
    feat = stream_ref.shape[1]
    ffe = wg.shape[3]
    nslot = nsp * snd.shape[1]
    per_dest = snd.shape[1]
    cap = per_dest // 2
    nexp = nsp * 2
    width = feat * ntp
    sp, tp = lax.axis_index("sp"), lax.axis_index("tp")
    z, x = sp // nx, lax.rem(sp, nx)
    y, c = tp // 2, lax.rem(tp, 2)
    partner = (sp, y * 2 + 1 - c)

    def in_column(yy):
        return (sp, yy * 2 + c)

    def load(i, src, dst):
        return pltpu.make_async_copy(src, dst, load_sem.at[i])

    barrier = pltpu.get_barrier_semaphore()

    def greet_row(i):
        to = z * nx + lax.rem(x + i, nx)
        pl.semaphore_signal(barrier, inc=1, device_id=(to, tp), device_id_type=MESH)

    def greet_later(zz):
        pl.semaphore_signal(barrier, inc=1, device_id=(zz * nx + x, tp), device_id_type=MESH)

    def greet_tp(i):
        pl.semaphore_signal(barrier, inc=1, device_id=in_column(lax.rem(y + i, ny)), device_id_type=MESH)

    each(1, ny, greet_tp)
    each(z + 1, nz, greet_later)
    each(1, nx, greet_row)
    pl.semaphore_signal(barrier, inc=1, device_id=partner, device_id_type=MESH)
    loads = [
        load(i, src, dst)
        for i, (src, dst) in enumerate(
            [
                (bias_hbm, bias_ref),
                (k_hbm, kv.at[x, 0:tok]),
                (v_hbm, kv.at[x, tok : 2 * tok]),
                (q_hbm, q_ref),
                (ids_hbm, ids_ref),
                (rw_hbm, rw_ref),
                (stream_hbm, stream_ref),
                (gain_hbm, gain_ref.at[c]),
                (wo_hbm, wo),
                (sg_hbm, sg),
                (su_hbm, su),
                (wg_hbm, wg.at[:, c]),
                (wu_hbm, wu.at[:, c]),
                (wd_hbm, wd.at[c]),
                (sd_hbm, sd),
            ]
        )
    ]
    for copy in loads:
        copy.start()

    eye = iota((tok, tok), 0) == iota((tok, tok), 1)

    def to_row(column):
        return jnp.sum(jnp.where(eye, column, 0.0), axis=0, keepdims=True)

    def to_column(row):
        return jnp.sum(jnp.where(eye, row, 0.0), axis=1, keepdims=True)

    loads[0].wait()
    kv[x, 2 * tok : 2 * tok + 16, :] = jnp.broadcast_to(bias_ref[...].astype(F32), (16, tok)).astype(BF16)
    hk = (nx // 2) * tok
    tri[...] = (iota((hk, hk), 0) > iota((hk, hk), 1)).astype(BF16)
    for i in (1, 2, 3):
        loads[i].wait()

    pl.semaphore_wait(barrier, nx - 1 + ny + z)

    def kv_copy(i):
        peer = lax.rem(x + i, nx)
        return rdma(kv.at[x], kv.at[x], kv_send.at[i], kv_recv.at[x], (z * nx + peer, tp))

    def q_copy(i):
        return rdma(q_ref, qbuf.at[z], q_send.at[i], q_recv.at[z], ((z - i) * nx + x, tp))

    each(1, nx, lambda i: kv_copy(i).start())
    each(1, z + 1, lambda i: q_copy(i).start())

    swapped = [
        rdma(mine, mine, w_send.at[i], w_recv.at[i], partner)
        for i, mine in enumerate((wg.at[:, c], wu.at[:, c], wd.at[c], gain_ref.at[c]))
    ]
    for i, copy in zip((11, 12, 13, 7), swapped):
        loads[i].wait()
        copy.start()

    loads[4].wait()
    loads[5].wait()
    exp_lane = iota((tok, nexp), 1).astype(F32)

    def columns(ref):
        return [to_column(ref[i : i + 1, :].astype(F32)) for i in range(2)]

    ids, rw = columns(ids_ref), columns(rw_ref)
    first, second = ids[0] == exp_lane, ids[1] == exp_lane
    named = jnp.where(first | second, 1.0, 0.0).astype(BF16)
    earlier = jnp.where(iota((tok, tok), 1) < iota((tok, tok), 0), 1.0, 0.0).astype(BF16)
    rank = dot(earlier, named).astype(BF16)
    spread = jnp.where(iota((nexp, nslot), 1) // cap == iota((nexp, nslot), 0), 1.0, 0.0).astype(BF16)
    weight_hi, weight_lo = halves(jnp.where(first, rw[0], 0.0) + jnp.where(second, rw[1], 0.0))
    slot_rank = lax.rem(iota((tok, nslot), 1), cap).astype(F32)
    taken = (dot(named, spread) > 0.5) & (dot(rank, spread) == slot_rank)
    taken_f = jnp.where(taken, 1.0, 0.0)
    pt[...] = taken_f.T.astype(BF16)
    w_hi[...] = (taken_f * dot(weight_hi, spread)).astype(BF16)
    w_lo[...] = (taken_f * dot(weight_lo, spread)).astype(BF16)

    def kv_arrive(i):
        xs = lax.rem(x + i, nx)
        rdma(kv.at[xs], kv.at[xs], kv_send.at[i], kv_recv.at[xs], (z * nx + xs, tp)).wait_recv()

    each(1, nx, kv_arrive)

    scale = hd ** (-0.5)

    def attend(q, own):
        logits, fails, parts = [], [], []
        for h in range(2):
            at = range(h * (nx // 2), (h + 1) * (nx // 2))
            keys = jnp.concatenate([kv[i, 0:tok, :] for i in at], axis=0)
            bias = jnp.concatenate([kv[i, 2 * tok : 2 * tok + 1, :] for i in at], axis=1).astype(F32)
            lg = dot_nt(q, keys) * scale + bias
            fail = -(jnp.maximum(lg, 0.0) + jnp.log(1.0 + jnp.exp(-jnp.abs(lg))))
            logits.append(lg + fail)
            if own:
                before = iota((tok, hk), 1) + h * hk < iota((tok, hk), 0) + x * tok
                fail = jnp.where(before, fail, 0.0)
            fails.append(fail)
            parts.append(halves(fail))
        stacked = jnp.concatenate([parts[0][0], parts[1][0], parts[0][1], parts[1][1]], axis=0)
        sums = dot(stacked, tri[...])
        tail0 = sums[0:tok] + sums[2 * tok : 3 * tok]
        tail1 = sums[tok : 2 * tok] + sums[3 * tok : 4 * tok]
        tail0 = tail0 + (tail1[:, 0:1] + fails[1][:, 0:1])
        total = tail0[:, 0:1] + fails[0][:, 0:1]
        acc = jnp.zeros((tok, hd), F32)
        for h, tail in enumerate((tail0, tail1)):
            at = range(h * (nx // 2), (h + 1) * (nx // 2))
            values = jnp.concatenate([kv[i, tok : 2 * tok, :] for i in at], axis=0)
            weights = jnp.exp(logits[h] + tail)
            if own:
                before = iota((tok, hk), 1) + h * hk < iota((tok, hk), 0) + x * tok
                weights = jnp.where(before, weights, 0.0)
            acc = acc + dot(weights.astype(BF16), values)
        return acc, total

    def part_copy(zq):
        return rdma(part_out.at[zq], part_in.at[z], p_send.at[zq], p_recv.at[z], (zq * nx + x, tp))

    def serve(i):
        zq = z + i
        rdma(qbuf.at[zq], qbuf.at[zq], q_send.at[i], q_recv.at[zq], (zq * nx + x, tp)).wait_recv()
        acc, total = attend(qbuf[zq], False)
        part_out[zq, 0:tok, :] = acc.astype(BF16)
        row = to_row(total)
        high, rest = row.astype(BF16), row - row.astype(BF16).astype(F32)
        mid, low = halves(rest)
        at_row = iota((16, tok), 0)
        rows = jnp.where(
            at_row == 0,
            high.astype(F32),
            jnp.where(at_row == 1, mid.astype(F32), jnp.where(at_row == 2, low.astype(F32), 0.0)),
        )
        part_out[zq, tok : tok + 16, :] = rows.astype(BF16)
        part_copy(zq).start()

    each(1, nz - z, serve)
    acc, later = attend(q_ref[...], True)

    def combine(i, carry):
        acc, later = carry
        zs = z - i
        rdma(part_in.at[zs], part_in.at[zs], p_send.at[zs], p_recv.at[zs], (zs * nx + x, tp)).wait_recv()
        summary = part_in[zs, 0:tok, :].astype(F32)
        row = jnp.sum(part_in[zs, tok : tok + 16, :].astype(F32), axis=0, keepdims=True)
        return acc + jnp.exp(later) * summary, later + to_column(row)

    acc, later = lax.fori_loop(1, z + 1, combine, (acc, later))

    far_first = (4, 3, 5, 2, 6, 1, 7)

    def gather(buf, send, recv, fsend=None, frecv=None):
        def block_copy(k, block, off):
            here = buf.at[c, block] if fsend is not None else buf.at[block]
            return rdma(here, here, send.at[k], recv.at[block], in_column(lax.rem(y + off, ny)))

        def across(block):
            here = buf.at[c, block]
            return rdma(here, here, fsend.at[block], frecv.at[block], partner)

        def start():
            for k, off in enumerate(far_first):
                block_copy(k, y, off).start()
            if fsend is not None:
                across(y).start()

        def pass_on():
            for k, off in enumerate(far_first):
                block = lax.rem(y + ny - off, ny)
                block_copy(k, block, off).wait_recv()
                if fsend is not None:
                    across(block).start()

        def finish():
            def arrive(block):
                there = buf.at[1 - c, block]
                rdma(there, there, fsend.at[block], frecv.at[block], partner).wait_recv()

            each(0, ny, arrive)

        def drain():
            for k, off in enumerate(far_first):
                block_copy(k, y, off).wait_send()
            if fsend is not None:
                each(0, ny, lambda block: across(block).wait_send())

        return start, pass_on, finish, drain

    abuf[c, y] = acc.astype(BF16)
    a_start, a_pass, a_finish, a_drain = gather(abuf, a_send, a_recv, af_send, af_recv)
    a_start()
    a_pass()
    a_finish()
    loads[8].wait()
    loads[6].wait()
    projected = jnp.zeros((tok, feat), F32)
    for i in range(ny):
        heads = jnp.concatenate([abuf[0, i], abuf[1, i]], axis=1)
        projected = projected + dot(heads, wo[i * 2 * hd : (i + 1) * 2 * hd, :])
    mixed = (stream_ref[...].astype(F32) + projected).astype(BF16)
    mixed_ref[...] = mixed

    snd[...] = dot(pt[...], mixed).astype(BF16).reshape(nsp, per_dest, feat)

    def block_at(i, sign):
        rank = lax.div(i, nx)
        dz = jnp.where(rank == 0, 0, offset_near(rank - 1, nz))
        dx = lax.rem(i, nx)
        return lax.rem(z + sign * dz + nz, nz) * nx + lax.rem(x + sign * dx + nx, nx)

    def dispatch(i):
        to = block_at(i, -1)
        at, core = lax.div(i, 2), lax.rem(i, 2)
        return rdma(snd.at[to], arr.at[at, c], d_send.at[i], d_recv.at[at, c], (to, y * 2 + core))

    def dispatch_own():
        return rdma(snd.at[sp], arr.at[0, c], d_send.at[0], d_recv.at[0, c], partner)

    each(1, nsp, lambda i: dispatch(i).start())

    @pl.when(c == 0)
    def _():
        arr[0, 0] = snd[sp]

    @pl.when(c == 1)
    def _():
        dispatch_own().start()


    def products(rows, gain, lhs_of, gate_w, up_w):
        value = rows.astype(F32)
        squares = jnp.sum(value * value, axis=1, keepdims=True)
        lhs = lhs_of((value * gain).astype(BF16))
        gate = dot(lhs, gate_w).astype(BF16)
        up = dot(lhs, up_w).astype(BF16)
        return gate, up, two_lanes(squares)

    def two_lanes(column):
        high, low = halves(column)
        lane = iota((column.shape[0], 128), 1)
        return jnp.where(
            lane == 0, high.astype(F32), jnp.where(lane == 1, low.astype(F32), 0.0)
        ).astype(BF16)

    def laid(ref, lo, value):
        ref[:, :, lo : lo + value.shape[1]] = value.reshape(ref.shape[0], ref.shape[1], value.shape[1])

    def packed(total):
        squares = total[:, 2 * ffe : 2 * ffe + 1] + total[:, 2 * ffe + 1 : 2 * ffe + 2]
        return total[:, 0 : 2 * ffe].astype(BF16), two_lanes(squares)

    def activated(total):
        squares = total[:, 2 * ffe : 2 * ffe + 1] + total[:, 2 * ffe + 1 : 2 * ffe + 2]
        inv = lax.rsqrt(squares / width + EPS)
        gate, up = total[:, 0:ffe] * inv, total[:, ffe : 2 * ffe] * inv
        return (gate * jax.nn.sigmoid(gate) * up).astype(BF16)

    loads[9].wait()
    loads[10].wait()
    gate, up, squares = products(mixed, gain_ref[c], lambda a: a, sg[...], su[...])
    laid(spart, 0, gate)
    laid(spart, ffe, up)
    laid(spart, 2 * ffe, squares)
    ny2 = ny // 2

    def spre_copy(i):
        yy = 2 * i + 1 - c
        return rdma(spart.at[yy], spre.at[i], spre_send.at[i], spre_recv.at[i], partner)

    each(0, ny2, lambda i: spre_copy(i).start())

    def srs_copy(i):
        yy = 2 * i + c
        return rdma(sred.at[i], srs_in.at[y], srs_send.at[i], srs_recv.at[y], in_column(yy))

    def shared_add(i):
        yy = 2 * i + c
        rdma(spre.at[i], spre.at[i], spre_send.at[i], spre_recv.at[i], partner).wait_recv()
        sums, squares = packed(spart[yy].astype(F32) + spre[i].astype(F32))
        sred[i, :, 0 : 2 * ffe] = sums
        sred[i, :, 2 * ffe : 2 * ffe + 128] = squares

        @pl.when(yy != y)
        def _():
            srs_copy(i).start()

    each(0, ny2, shared_add)

    npos, chunk = nsp // 4, red.shape[2]
    rows_g = npos * per_dest

    def by_expert(a):
        zero = jnp.zeros_like(a)
        mine = lax.rem(iota(a.shape, 0), per_dest) < cap
        return jnp.concatenate([jnp.where(mine, a, zero), jnp.where(mine, zero, a)], axis=1)

    def arrivals(g):
        def arrive(at):
            for core in range(2):
                here = arr.at[at, core]
                rdma(here, here, d_send.at[1], d_recv.at[at, core], partner).wait_recv()

        each(max(1, g * npos), (g + 1) * npos, arrive)
        if g == 0:
            here = arr.at[0, 1]
            rdma(here, here, d_send.at[1], d_recv.at[0, 1], partner).wait_recv()

            @pl.when(c == 1)
            def _():
                here = arr.at[0, 0]
                rdma(here, here, d_send.at[1], d_recv.at[0, 0], partner).wait_recv()

    def experts(g):
        at = slice(g * npos, (g + 1) * npos)
        rows = jnp.concatenate([arr[at, core].reshape(rows_g, feat) for core in range(2)], axis=1)
        gain = jnp.concatenate([gain_ref[0], gain_ref[1]], axis=1)
        gate, up, squares = products(
            rows, gain, by_expert, wg[...].reshape(4 * feat, ffe), wu[...].reshape(4 * feat, ffe)
        )
        for lo, value in ((0, gate), (ffe, up), (2 * ffe, squares)):
            red[g, :, :, lo : lo + value.shape[1]] = value.reshape(ny, chunk, value.shape[1])
        for r in (4, 3, 5, 2, 6):
            l1_copy(g, r).start()

    def l1_copy(g, r):
        if r == 4:
            side = lax.rem(y, 2)
            hub, k = jnp.where(side == 0, 3, 5), 2
        else:
            side = 0 if r < 4 else 1
            hub, k = (r - 1, r - 2) if r < 4 else (r + 1, ny - r - 2)
        return rdma(
            red.at[g, lax.rem(y + r, ny)],
            hub_in.at[g, side, k],
            l1_send.at[g, r],
            l1_recv.at[g, side, k],
            in_column(lax.rem(y + hub, ny)),
        )

    def l2_copy(g, side):
        to = lax.rem(y + (1 if side == 0 else ny - 1), ny)
        return rdma(hub_out.at[g, side], own_in.at[g, side], l2_send.at[g, side], l2_recv.at[g, side], in_column(to))

    def hub(g):
        for side in range(2):
            def add_in(k, total):
                here = hub_in.at[g, side, k]
                rdma(here, here, l1_send.at[g, 2], l1_recv.at[g, side, k], partner).wait_recv()
                return total + hub_in[g, side, k].astype(F32)

            odd = lax.rem(y, 2)
            mine = red[g, lax.rem(y + (1 if side == 0 else ny - 1), ny)].astype(F32)
            total = lax.fori_loop(0, 2 + odd if side == 0 else 3 - odd, add_in, mine)
            sums, squares = packed(total)
            hub_out[g, side, :, 0 : 2 * ffe] = sums
            hub_out[g, side, :, 2 * ffe : 2 * ffe + 128] = squares
            l2_copy(g, side).start()

    gathers = [gather(hbuf.at[g], h_send.at[g], h_recv.at[g]) for g in range(2)]

    def own(g):
        total = red[g, y].astype(F32)
        for side in range(2):
            here = own_in.at[g, side]
            rdma(here, here, l2_send.at[g, side], l2_recv.at[g, side], partner).wait_recv()
            total = total + own_in[g, side].astype(F32)
        hbuf[g, y] = activated(total)
        gathers[g][0]()

    def give_back(at, core):
        i = 2 * at + c
        to = block_at(i, 1)
        return rdma(ret_out.at[at, core], ret_in.at[sp], r_send.at[at, core], r_recv.at[i], (to, y * 2 + core))

    def down(g):
        rows = by_expert(hbuf[g].reshape(rows_g, ffe))
        at = slice(g * npos, (g + 1) * npos)
        for core in range(2):
            ret_out[at, core] = dot(rows, wd[core]).astype(BF16).reshape(npos, per_dest, feat)

        def back(at):
            for core in range(2):
                give_back(at, core).start()

        each(max(1, g * npos), (g + 1) * npos, back)
        if g == 0:
            give_back(0, 1).start()

            @pl.when(c == 1)
            def _():
                give_back(0, 0).start()

            @pl.when(c == 0)
            def _():
                ret_in[sp] = ret_out[0, 0]

    owner = lax.rem(y, 2) == c

    arrivals(0)
    for i in (0, 1, 3):
        swapped[i].wait_recv()
    experts(0)

    @pl.when(owner)
    def _():
        def add_in(i, total):
            ys = lax.rem(y + offset_near(i, ny), ny)
            rdma(srs_in.at[ys], srs_in.at[ys], srs_send.at[0], srs_recv.at[ys], partner).wait_recv()
            return total + srs_in[ys].astype(F32)

        total = lax.fori_loop(0, ny - 1, add_in, sred[y // 2].astype(F32))
        shbuf[y] = activated(total)

        def to_peer(i):
            off = offset_near(i, ny)
            rdma(
                shbuf.at[y], shbuf.at[y], sh_send.at[i], sh_recv.at[y], in_column(lax.rem(y + off, ny))
            ).start()

        each(0, ny - 1, to_peer)
        rdma(shbuf.at[y], shbuf.at[y], shf_send.at[y // 2], shf_recv.at[y], partner).start()

    arrivals(1)
    experts(1)
    hub(0)
    hub(1)
    own(0)
    own(1)
    gathers[0][1]()
    def shared_on(i):
        yy = 2 * i + c

        @pl.when(yy != y)
        def _():
            rdma(shbuf.at[yy], shbuf.at[yy], sh_send.at[0], sh_recv.at[yy], partner).wait_recv()
            rdma(shbuf.at[yy], shbuf.at[yy], shf_send.at[i], shf_recv.at[yy], partner).start()

    each(0, ny2, shared_on)
    swapped[2].wait_recv()
    down(0)
    gathers[1][1]()
    down(1)

    def shared_arrive(i):
        yy = 2 * i + 1 - c
        rdma(shbuf.at[yy], shbuf.at[yy], shf_send.at[i], shf_recv.at[yy], partner).wait_recv()

    each(0, ny2, shared_arrive)
    loads[14].wait()
    base = mixed_ref[...].astype(F32) + dot(shbuf[...].reshape(tok, ffe), sd[...])

    each(1, nx, lambda i: kv_copy(i).wait_send())
    each(1, z + 1, lambda i: q_copy(i).wait_send())
    each(1, nz - z, lambda i: part_copy(z + i).wait_send())
    a_drain()
    each(1, nsp, lambda i: dispatch(i).wait_send())

    @pl.when(c == 1)
    def _():
        dispatch_own().wait_send()

    for copy in swapped:
        copy.wait_send()
    each(0, ny2, lambda i: spre_copy(i).wait_send())

    def srs_drain(i):
        @pl.when(2 * i + c != y)
        def _():
            srs_copy(i).wait_send()

    each(0, ny2, srs_drain)
    for g in range(2):
        for r in (4, 3, 5, 2, 6):
            l1_copy(g, r).wait_send()
        for side in range(2):
            l2_copy(g, side).wait_send()
        gathers[g][3]()

    @pl.when(owner)
    def _():
        each(
            0,
            ny - 1,
            lambda i: rdma(shbuf.at[y], shbuf.at[y], sh_send.at[i], sh_recv.at[y], partner).wait_send(),
        )

    def shared_forwarded(i):
        yy = 2 * i + c
        rdma(shbuf.at[yy], shbuf.at[yy], shf_send.at[i], shf_recv.at[yy], partner).wait_send()

    each(0, ny2, shared_forwarded)

    def returned(i):
        src = block_at(i, -1)
        rdma(ret_in.at[src], ret_in.at[src], r_send.at[i], r_recv.at[i], (src, tp)).wait_recv()

    each(1, nsp, returned)

    @pl.when(c == 1)
    def _():
        returned(0)

    rows = ret_in[...].reshape(nslot, feat)
    out_ref[...] = (base + (dot(w_hi[...], rows) + dot(w_lo[...], rows))).astype(BF16)

    def given(at):
        for core in range(2):
            give_back(at, core).wait_send()

    each(1, nsp // 2, given)
    give_back(0, 1).wait_send()

    @pl.when(c == 1)
    def _():
        give_back(0, 0).wait_send()


def body(
    nx,
    queries,
    key_rows,
    value_rows,
    break_bias,
    stream,
    out_proj,
    norm_gain,
    expert_ids,
    route_weights,
    gate_proj,
    up_proj,
    down_proj,
    shared_gate,
    shared_up,
    shared_down,
):
    nsp, ntp = lax.axis_size("sp"), lax.axis_size("tp")
    nz, ny = nsp // nx, ntp // 2
    tok, hd = queries.shape
    feat = stream.shape[1]
    experts_local, _, ffe = gate_proj.shape
    ffs = shared_gate.shape[1]
    cap = 2 * expert_ids.shape[1] * tok // (experts_local * nsp)
    per_dest = experts_local * cap
    chunk = nsp * per_dest // ntp // 2
    srows = tok // ny
    wide = 2 * ffe + 128
    hk = (nx // 2) * tok

    def vm(*shape):
        return pltpu.VMEM(shape, BF16)

    def sems(*counts):
        return [pltpu.SemaphoreType.DMA(n if isinstance(n, tuple) else (n,)) for n in counts]

    scratch = [
        vm(tok, hd),
        vm(1, tok),
        vm(tok, feat),
        pltpu.VMEM((2, 1, feat), F32),
        pltpu.VMEM((2, tok), jnp.int32),
        pltpu.VMEM((2, tok), F32),
        vm(*out_proj.shape),
        vm(experts_local, 2, feat, ffe),
        vm(experts_local, 2, feat, ffe),
        vm(2, experts_local * ffe, feat),
        vm(feat, ffs),
        vm(feat, ffs),
        vm(ffs, feat),
        vm(nx, 2 * tok + 16, hd),
        vm(nz, tok, hd),
        vm(nz, tok + 16, hd),
        vm(nz, tok + 16, hd),
        vm(hk, hk),
        vm(2, ny, tok, hd),
        vm(nsp * per_dest, tok),
        vm(tok, nsp * per_dest),
        vm(tok, nsp * per_dest),
        vm(tok, feat),
        vm(nsp, per_dest, feat),
        vm(nsp // 2, 2, per_dest, feat),
        vm(2, ny, chunk, wide),
        vm(2, 2, 3, chunk, wide),
        vm(2, 2, chunk, wide),
        vm(2, 2, chunk, wide),
        vm(ny, srows, wide),
        vm(ny // 2, srows, wide),
        vm(ny // 2, srows, wide),
        vm(ny, srows, wide),
        vm(2, ny, chunk, ffe),
        vm(ny, srows, ffs),
        vm(nsp // 2, 2, per_dest, feat),
        vm(nsp, per_dest, feat),
        *sems(15, nx, nx, nz, nz, nz, nz, 7, ny, ny, ny, nsp, (nsp // 2, 2), 4, 4, (2, ny), (2, 2, 3), (2, 2), (2, 2)),
        *sems(ny // 2, ny // 2, ny // 2, ny, (2, 7), (2, ny), ny, ny, ny // 2, ny, (nsp // 2, 2), nsp),
    ]
    large = pl.BlockSpec(memory_space=pl.ANY)
    return pl.pallas_call(
        functools.partial(layer_kernel, (nz, nx, ny)),
        out_shape=jax.ShapeDtypeStruct((tok, feat), BF16),
        in_specs=[large] * 15,
        out_specs=pl.BlockSpec(memory_space=pltpu.VMEM),
        scratch_shapes=scratch,
        compiler_params=pltpu.CompilerParams(
            collective_id=0, has_side_effects=True, vmem_limit_bytes=60 * 1024 * 1024
        ),
    )(
        queries,
        key_rows,
        value_rows,
        break_bias.T,
        stream,
        norm_gain.reshape(1, feat),
        expert_ids.T,
        route_weights.T,
        out_proj,
        gate_proj,
        up_proj,
        down_proj.reshape(experts_local * ffe, feat),
        shared_gate,
        shared_up,
        shared_down,
    )


def solution(mesh, nx=NX):
    in_specs = (
        P("sp", "tp"),
        P("sp", "tp"),
        P("sp", "tp"),
        P("sp", "tp"),
        P("sp", "tp"),
        P(None, "tp"),
        P("tp"),
        P("sp", None),
        P("sp", None),
        P("sp", "tp", None),
        P("sp", "tp", None),
        P("sp", None, "tp"),
        P("tp", None),
        P("tp", None),
        P(None, "tp"),
    )
    return jax.shard_map(
        functools.partial(body, nx), mesh=mesh, in_specs=in_specs, out_specs=P("sp", "tp"), check_vma=False
    )
```

```python
import functools

import jax
import jax.numpy as jnp
from jax import lax
from jax.experimental import pallas as pl
from jax.experimental.pallas import tpu as pltpu
from jax.sharding import PartitionSpec as P

EPS = 1e-06
NX = 4
MESH = pl.DeviceIdType.MESH
F32, BF16 = jnp.float32, jnp.bfloat16


def rdma(src, dst, send, recv, device):
    return pltpu.make_async_remote_copy(
        src_ref=src, dst_ref=dst, send_sem=send, recv_sem=recv, device_id=device, device_id_type=MESH
    )


def each(low, high, fn):
    def turn(i, carry):
        fn(i)
        return carry

    lax.fori_loop(low, high, turn, 0)


def offset_near(i, n):
    half = lax.div(i, 2) + 1
    return jnp.where(lax.rem(i, 2) == 0, half, n - half)


def dot(a, b):
    return jnp.dot(a, b, preferred_element_type=F32)


def dot_nt(a, b):
    return lax.dot_general(a, b, (((1,), (1,)), ((), ())), preferred_element_type=F32)


def halves(value):
    high = value.astype(BF16)
    return high, (value - high.astype(F32)).astype(BF16)


def iota(shape, dim):
    return lax.broadcasted_iota(jnp.int32, shape, dim)


def layer_kernel(
    sizes,
    q_hbm,
    k_hbm,
    v_hbm,
    bias_hbm,
    stream_hbm,
    gain_hbm,
    ids_hbm,
    rw_hbm,
    wo_hbm,
    wg_hbm,
    wu_hbm,
    wd_hbm,
    sg_hbm,
    su_hbm,
    sd_hbm,
    out_ref,
    q_ref,
    bias_ref,
    stream_ref,
    gain_ref,
    ids_ref,
    rw_ref,
    wo,
    wg,
    wu,
    wd,
    sg,
    su,
    sd,
    kv,
    qbuf,
    part_out,
    part_in,
    tri,
    abuf,
    pt,
    w_hi,
    w_lo,
    mixed_ref,
    snd,
    arr,
    red,
    hub_in,
    hub_out,
    own_in,
    square_rows,
    inverse,
    spart,
    spre,
    sred,
    srs_in,
    hbuf,
    shbuf,
    ret_out,
    ret_in,
    load_sem,
    kv_send,
    kv_recv,
    q_send,
    q_recv,
    p_send,
    p_recv,
    a_send,
    a_recv,
    af_send,
    af_recv,
    d_send,
    d_recv,
    w_send,
    w_recv,
    l1_send,
    l1_recv,
    l2_send,
    l2_recv,
    n_send,
    n_recv,
    spre_send,
    spre_recv,
    srs_send,
    srs_recv,
    h_send,
    h_recv,
    sh_send,
    sh_recv,
    shf_send,
    shf_recv,
    r_send,
    r_recv,
):
    nz, nx, ny = sizes
    nsp, ntp = nz * nx, ny * 2
    tok, hd = q_ref.shape
    feat = stream_ref.shape[1]
    ffe = wg.shape[3]
    nslot = nsp * snd.shape[1]
    per_dest = snd.shape[1]
    cap = per_dest // 2
    nexp = nsp * 2
    width = feat * ntp
    sp, tp = lax.axis_index("sp"), lax.axis_index("tp")
    z, x = sp // nx, lax.rem(sp, nx)
    y, c = tp // 2, lax.rem(tp, 2)
    partner = (sp, y * 2 + 1 - c)

    def in_column(yy):
        return (sp, yy * 2 + c)

    def load(i, src, dst):
        return pltpu.make_async_copy(src, dst, load_sem.at[i])

    barrier = pltpu.get_barrier_semaphore()

    def greet_row(i):
        to = z * nx + lax.rem(x + i, nx)
        pl.semaphore_signal(barrier, inc=1, device_id=(to, tp), device_id_type=MESH)

    def greet_later(zz):
        pl.semaphore_signal(barrier, inc=1, device_id=(zz * nx + x, tp), device_id_type=MESH)

    def greet_tp(i):
        pl.semaphore_signal(barrier, inc=1, device_id=in_column(lax.rem(y + i, ny)), device_id_type=MESH)

    each(1, ny, greet_tp)
    each(z + 1, nz, greet_later)
    each(1, nx, greet_row)
    pl.semaphore_signal(barrier, inc=1, device_id=partner, device_id_type=MESH)
    loads = [
        load(i, src, dst)
        for i, (src, dst) in enumerate(
            [
                (bias_hbm, bias_ref),
                (k_hbm, kv.at[x, 0:tok]),
                (v_hbm, kv.at[x, tok : 2 * tok]),
                (q_hbm, q_ref),
                (ids_hbm, ids_ref),
                (rw_hbm, rw_ref),
                (stream_hbm, stream_ref),
                (gain_hbm, gain_ref.at[c]),
                (wo_hbm.at[:, 0], wo.at[0]),
                (sg_hbm, sg),
                (su_hbm, su),
                (wg_hbm, wg.at[:, c]),
                (wu_hbm, wu.at[:, c]),
                (wd_hbm, wd.at[c]),
                (sd_hbm, sd),
                (wo_hbm.at[:, 1], wo.at[1]),
            ]
        )
    ]
    for copy in loads:
        copy.start()

    eye = iota((tok, tok), 0) == iota((tok, tok), 1)

    def to_row(column):
        return jnp.sum(jnp.where(eye, column, 0.0), axis=0, keepdims=True)

    def to_column(row):
        return jnp.sum(jnp.where(eye, row, 0.0), axis=1, keepdims=True)

    loads[0].wait()
    kv[x, 2 * tok : 2 * tok + 16, :] = jnp.broadcast_to(bias_ref[...].astype(F32), (16, tok)).astype(BF16)
    hk = (nx // 2) * tok
    tri[...] = (iota((hk, hk), 0) > iota((hk, hk), 1)).astype(BF16)
    for i in (1, 2, 3):
        loads[i].wait()

    pl.semaphore_wait(barrier, nx - 1 + ny + z)

    def kv_copy(i):
        peer = lax.rem(x + i, nx)
        return rdma(kv.at[x], kv.at[x], kv_send.at[i], kv_recv.at[x], (z * nx + peer, tp))

    def q_copy(i):
        return rdma(q_ref, qbuf.at[z], q_send.at[i], q_recv.at[z], ((z - i) * nx + x, tp))

    each(1, nx, lambda i: kv_copy(i).start())
    each(1, z + 1, lambda i: q_copy(i).start())

    swapped = [
        rdma(mine, mine, w_send.at[i], w_recv.at[i], partner)
        for i, mine in enumerate((wg.at[:, c], wu.at[:, c], wd.at[c], gain_ref.at[c]))
    ]
    for i, copy in zip((11, 12, 13, 7), swapped):
        loads[i].wait()
        copy.start()

    loads[4].wait()
    loads[5].wait()
    exp_lane = iota((tok, nexp), 1).astype(F32)

    def columns(ref):
        return [to_column(ref[i : i + 1, :].astype(F32)) for i in range(2)]

    ids, rw = columns(ids_ref), columns(rw_ref)
    first, second = ids[0] == exp_lane, ids[1] == exp_lane
    named = jnp.where(first | second, 1.0, 0.0).astype(BF16)
    earlier = jnp.where(iota((tok, tok), 1) < iota((tok, tok), 0), 1.0, 0.0).astype(BF16)
    rank = dot(earlier, named).astype(BF16)
    spread = jnp.where(iota((nexp, nslot), 1) // cap == iota((nexp, nslot), 0), 1.0, 0.0).astype(BF16)
    weight_hi, weight_lo = halves(jnp.where(first, rw[0], 0.0) + jnp.where(second, rw[1], 0.0))
    slot_rank = lax.rem(iota((tok, nslot), 1), cap).astype(F32)
    taken = (dot(named, spread) > 0.5) & (dot(rank, spread) == slot_rank)
    taken_f = jnp.where(taken, 1.0, 0.0)
    pt[...] = taken_f.T.astype(BF16)
    w_hi[...] = (taken_f * dot(weight_hi, spread)).astype(BF16)
    w_lo[...] = (taken_f * dot(weight_lo, spread)).astype(BF16)

    def kv_arrive(i):
        xs = lax.rem(x + i, nx)
        rdma(kv.at[xs], kv.at[xs], kv_send.at[i], kv_recv.at[xs], (z * nx + xs, tp)).wait_recv()

    each(1, nx, kv_arrive)

    scale = hd ** (-0.5)

    def attend(q, own):
        logits, fails, parts = [], [], []
        for h in range(2):
            at = range(h * (nx // 2), (h + 1) * (nx // 2))
            keys = jnp.concatenate([kv[i, 0:tok, :] for i in at], axis=0)
            bias = jnp.concatenate([kv[i, 2 * tok : 2 * tok + 1, :] for i in at], axis=1).astype(F32)
            lg = dot_nt(q, keys) * scale + bias
            fail = -(jnp.maximum(lg, 0.0) + jnp.log(1.0 + jnp.exp(-jnp.abs(lg))))
            logits.append(lg + fail)
            if own:
                before = iota((tok, hk), 1) + h * hk < iota((tok, hk), 0) + x * tok
                fail = jnp.where(before, fail, 0.0)
            fails.append(fail)
            parts.append(halves(fail))
        stacked = jnp.concatenate([parts[0][0], parts[1][0], parts[0][1], parts[1][1]], axis=0)
        sums = dot(stacked, tri[...])
        tail0 = sums[0:tok] + sums[2 * tok : 3 * tok]
        tail1 = sums[tok : 2 * tok] + sums[3 * tok : 4 * tok]
        tail0 = tail0 + (tail1[:, 0:1] + fails[1][:, 0:1])
        total = tail0[:, 0:1] + fails[0][:, 0:1]
        acc = jnp.zeros((tok, hd), F32)
        for h, tail in enumerate((tail0, tail1)):
            at = range(h * (nx // 2), (h + 1) * (nx // 2))
            values = jnp.concatenate([kv[i, tok : 2 * tok, :] for i in at], axis=0)
            weights = jnp.exp(logits[h] + tail)
            if own:
                before = iota((tok, hk), 1) + h * hk < iota((tok, hk), 0) + x * tok
                weights = jnp.where(before, weights, 0.0)
            acc = acc + dot(weights.astype(BF16), values)
        return acc, total

    def part_copy(zq):
        return rdma(part_out.at[zq], part_in.at[z], p_send.at[zq], p_recv.at[z], (zq * nx + x, tp))

    def serve(i):
        zq = z + i
        rdma(qbuf.at[zq], qbuf.at[zq], q_send.at[i], q_recv.at[zq], (zq * nx + x, tp)).wait_recv()
        acc, total = attend(qbuf[zq], False)
        part_out[zq, 0:tok, :] = acc.astype(BF16)
        row = to_row(total)
        high, rest = row.astype(BF16), row - row.astype(BF16).astype(F32)
        mid, low = halves(rest)
        at_row = iota((16, tok), 0)
        rows = jnp.where(
            at_row == 0,
            high.astype(F32),
            jnp.where(at_row == 1, mid.astype(F32), jnp.where(at_row == 2, low.astype(F32), 0.0)),
        )
        part_out[zq, tok : tok + 16, :] = rows.astype(BF16)
        part_copy(zq).start()

    each(1, nz - z, serve)
    acc, later = attend(q_ref[...], True)

    def combine(i, carry):
        acc, later = carry
        zs = z - i
        rdma(part_in.at[zs], part_in.at[zs], p_send.at[zs], p_recv.at[zs], (zs * nx + x, tp)).wait_recv()
        summary = part_in[zs, 0:tok, :].astype(F32)
        row = jnp.sum(part_in[zs, tok : tok + 16, :].astype(F32), axis=0, keepdims=True)
        return acc + jnp.exp(later) * summary, later + to_column(row)

    acc, later = lax.fori_loop(1, z + 1, combine, (acc, later))

    far_first = (4, 3, 5, 2, 6, 1, 7)

    def gather(buf, send, recv, fsend=None, frecv=None):
        def block_copy(k, block, off):
            here = buf.at[c, block] if fsend is not None else buf.at[block]
            return rdma(here, here, send.at[k], recv.at[block], in_column(lax.rem(y + off, ny)))

        def across(block):
            here = buf.at[c, block]
            return rdma(here, here, fsend.at[block], frecv.at[block], partner)

        def start():
            for k, off in enumerate(far_first):
                block_copy(k, y, off).start()
            if fsend is not None:
                across(y).start()

        def pass_on():
            for k, off in enumerate(far_first):
                block = lax.rem(y + ny - off, ny)
                block_copy(k, block, off).wait_recv()
                if fsend is not None:
                    across(block).start()

        def finish():
            def arrive(block):
                there = buf.at[1 - c, block]
                rdma(there, there, fsend.at[block], frecv.at[block], partner).wait_recv()

            each(0, ny, arrive)

        def drain():
            for k, off in enumerate(far_first):
                block_copy(k, y, off).wait_send()
            if fsend is not None:
                each(0, ny, lambda block: across(block).wait_send())

        return start, pass_on, finish, drain

    abuf[c, y] = acc.astype(BF16)
    a_start, a_pass, a_finish, a_drain = gather(abuf, a_send, a_recv, af_send, af_recv)
    a_start()
    a_pass()
    loads[8].wait()
    loads[15].wait()
    loads[6].wait()

    def project(core):
        total = jnp.zeros((tok, feat), F32)
        for i in range(0, ny, 2):
            heads = jnp.concatenate([abuf[core, i], abuf[core, i + 1]], axis=1)
            total = total + dot(heads, wo[core, i : i + 2].reshape(2 * hd, feat))
        return total

    projected = stream_ref[...].astype(F32) + project(c)
    a_finish()
    projected = projected + project(1 - c)
    mixed = projected.astype(BF16)
    mixed_ref[...] = mixed

    snd[...] = dot(pt[...], mixed).astype(BF16).reshape(nsp, per_dest, feat)

    def block_at(i, sign):
        rank = lax.div(i, nx)
        dz = jnp.where(rank == nz - 1, 0, offset_near(nz - 2 - rank, nz))
        dx = lax.rem(i, nx)
        return lax.rem(z + sign * dz + nz, nz) * nx + lax.rem(x + sign * dx + nx, nx)

    own_i, own_at = (nz - 1) * nx, (nz - 1) * nx // 2

    def others(fn):
        each(0, own_i, fn)
        each(own_i + 1, nsp, fn)

    def dispatch(i):
        to = block_at(i, -1)
        at, core = lax.div(i, 2), lax.rem(i, 2)
        return rdma(snd.at[to], arr.at[at, c], d_send.at[i], d_recv.at[at, c], (to, y * 2 + core))

    def dispatch_own():
        return rdma(snd.at[sp], arr.at[own_at, c], d_send.at[own_i], d_recv.at[own_at, c], partner)

    others(lambda i: dispatch(i).start())

    @pl.when(c == 0)
    def _():
        arr[own_at, 0] = snd[sp]

    @pl.when(c == 1)
    def _():
        dispatch_own().start()


    def products(rows, gain, lhs_of, gate_w, up_w):
        value = rows.astype(F32)
        squares = jnp.sum(value * value, axis=1, keepdims=True)
        lhs = lhs_of((value * gain).astype(BF16))
        gate = dot(lhs, gate_w).astype(BF16)
        up = dot(lhs, up_w).astype(BF16)
        return gate, up, squares

    def two_lanes(column):
        high, low = halves(column)
        lane = iota((column.shape[0], 128), 1)
        return jnp.where(
            lane == 0, high.astype(F32), jnp.where(lane == 1, low.astype(F32), 0.0)
        ).astype(BF16)

    def laid(ref, lo, value):
        ref[:, :, lo : lo + value.shape[1]] = value.reshape(ref.shape[0], ref.shape[1], value.shape[1])

    def packed(total):
        squares = total[:, 2 * ffe : 2 * ffe + 1] + total[:, 2 * ffe + 1 : 2 * ffe + 2]
        return total[:, 0 : 2 * ffe].astype(BF16), two_lanes(squares)

    def activated(total):
        squares = total[:, 2 * ffe : 2 * ffe + 1] + total[:, 2 * ffe + 1 : 2 * ffe + 2]
        return scaled_hidden(total, lax.rsqrt(squares / width + EPS))

    def scaled_hidden(total, inv):
        gate, up = total[:, 0:ffe] * inv, total[:, ffe : 2 * ffe] * inv
        return (gate * jax.nn.sigmoid(gate) * up).astype(BF16)

    loads[9].wait()
    loads[10].wait()
    gate, up, squares = products(mixed, gain_ref[c], lambda a: a, sg[...], su[...])
    laid(spart, 0, gate)
    laid(spart, ffe, up)
    laid(spart, 2 * ffe, two_lanes(squares))
    ny2 = ny // 2

    def spre_copy(i):
        yy = 2 * i + 1 - c
        return rdma(spart.at[yy], spre.at[i], spre_send.at[i], spre_recv.at[i], partner)

    each(0, ny2, lambda i: spre_copy(i).start())

    def srs_copy(i):
        yy = 2 * i + c
        return rdma(sred.at[i], srs_in.at[y], srs_send.at[i], srs_recv.at[y], in_column(yy))

    def shared_add(i):
        yy = 2 * i + c
        rdma(spre.at[i], spre.at[i], spre_send.at[i], spre_recv.at[i], partner).wait_recv()
        sums, squares = packed(spart[yy].astype(F32) + spre[i].astype(F32))
        sred[i, :, 0 : 2 * ffe] = sums
        sred[i, :, 2 * ffe : 2 * ffe + 128] = squares

        @pl.when(yy != y)
        def _():
            srs_copy(i).start()

    each(0, ny2, shared_add)

    npos, chunk = nsp // 4, red.shape[2]
    rows_g = npos * per_dest

    def by_expert(a):
        zero = jnp.zeros_like(a)
        mine = lax.rem(iota(a.shape, 0), per_dest) < cap
        return jnp.concatenate([jnp.where(mine, a, zero), jnp.where(mine, zero, a)], axis=1)

    def arrivals(g):
        def arrive(at):
            for core in range(2):
                here = arr.at[at, core]
                rdma(here, here, d_send.at[1], d_recv.at[at, core], partner).wait_recv()

        if g == 0:
            each(0, npos, arrive)
        else:
            each(npos, own_at, arrive)
            each(own_at + 1, 2 * npos, arrive)
            here = arr.at[own_at, 1]
            rdma(here, here, d_send.at[1], d_recv.at[own_at, 1], partner).wait_recv()

            @pl.when(c == 1)
            def _():
                here = arr.at[own_at, 0]
                rdma(here, here, d_send.at[1], d_recv.at[own_at, 0], partner).wait_recv()

    def squares_copy(g, k):
        here = square_rows.at[g, y]
        return rdma(here, here, n_send.at[g, k], n_recv.at[g, y], in_column(lax.rem(y + k, ny)))

    def scales(g):
        def arrive(k):
            ys = lax.rem(y + k, ny)
            here = square_rows.at[g, ys]
            rdma(here, here, n_send.at[g, k], n_recv.at[g, ys], partner).wait_recv()

        each(1, ny, arrive)
        squares = square_rows[g, 0]
        for ys in range(1, ny):
            squares = squares + square_rows[g, ys]
        inv = to_column(lax.rsqrt(squares / width + EPS))
        inverse[g] = jnp.broadcast_to(inv, (rows_g, 128)).reshape(ny, chunk, 128)

    def experts(g):
        at = slice(g * npos, (g + 1) * npos)
        rows = jnp.concatenate([arr[at, core].reshape(rows_g, feat) for core in range(2)], axis=1)
        gain = jnp.concatenate([gain_ref[0], gain_ref[1]], axis=1)
        gate, up, squares = products(
            rows, gain, by_expert, wg[...].reshape(4 * feat, ffe), wu[...].reshape(4 * feat, ffe)
        )
        square_rows[g, y] = to_row(squares)
        for k in range(1, ny):
            squares_copy(g, k).start()
        red[g, :, :, 0:ffe] = gate.reshape(ny, chunk, ffe)
        red[g, :, :, ffe : 2 * ffe] = up.reshape(ny, chunk, ffe)
        for r in (4, 3, 5, 2, 6):
            l1_copy(g, r).start()

    def l1_copy(g, r):
        if r == 4:
            side = lax.rem(y, 2)
            hub, k = jnp.where(side == 0, 3, 5), 2
        else:
            side = 0 if r < 4 else 1
            hub, k = (r - 1, r - 2) if r < 4 else (r + 1, ny - r - 2)
        return rdma(
            red.at[g, lax.rem(y + r, ny)],
            hub_in.at[g, side, k],
            l1_send.at[g, r],
            l1_recv.at[g, side, k],
            in_column(lax.rem(y + hub, ny)),
        )

    def l2_copy(g, side):
        to = lax.rem(y + (1 if side == 0 else ny - 1), ny)
        return rdma(hub_out.at[g, side], own_in.at[g, side], l2_send.at[g, side], l2_recv.at[g, side], in_column(to))

    def hub(g):
        for side in range(2):
            def add_in(k, total):
                here = hub_in.at[g, side, k]
                rdma(here, here, l1_send.at[g, 2], l1_recv.at[g, side, k], partner).wait_recv()
                return total + hub_in[g, side, k].astype(F32)

            odd = lax.rem(y, 2)
            mine = red[g, lax.rem(y + (1 if side == 0 else ny - 1), ny)].astype(F32)
            total = lax.fori_loop(0, 2 + odd if side == 0 else 3 - odd, add_in, mine)
            hub_out[g, side] = total.astype(BF16)
            l2_copy(g, side).start()

    gathers = [gather(hbuf.at[g], h_send.at[g], h_recv.at[g]) for g in range(2)]

    def own(g):
        total = red[g, y].astype(F32)
        for side in range(2):
            here = own_in.at[g, side]
            rdma(here, here, l2_send.at[g, side], l2_recv.at[g, side], partner).wait_recv()
            total = total + own_in[g, side].astype(F32)
        hbuf[g, y] = scaled_hidden(total, inverse[g, y][:, 0:1])
        gathers[g][0]()

    def give_back(at, core):
        i = 2 * at + c
        to = block_at(i, 1)
        return rdma(ret_out.at[at, core], ret_in.at[sp], r_send.at[at, core], r_recv.at[i], (to, y * 2 + core))

    def down(g):
        rows = by_expert(hbuf[g].reshape(rows_g, ffe))
        at = slice(g * npos, (g + 1) * npos)
        for core in range(2):
            ret_out[at, core] = dot(rows, wd[core]).astype(BF16).reshape(npos, per_dest, feat)

        def back(at):
            for core in range(2):
                give_back(at, core).start()

        if g == 0:
            each(0, npos, back)
        else:
            each(npos, own_at, back)
            each(own_at + 1, 2 * npos, back)
            give_back(own_at, 1).start()

            @pl.when(c == 1)
            def _():
                give_back(own_at, 0).start()

            @pl.when(c == 0)
            def _():
                ret_in[sp] = ret_out[own_at, 0]

    owner = lax.rem(y, 2) == c

    arrivals(0)
    for i in (0, 1, 3):
        swapped[i].wait_recv()
    experts(0)

    @pl.when(owner)
    def _():
        def add_in(i, total):
            ys = lax.rem(y + offset_near(i, ny), ny)
            rdma(srs_in.at[ys], srs_in.at[ys], srs_send.at[0], srs_recv.at[ys], partner).wait_recv()
            return total + srs_in[ys].astype(F32)

        total = lax.fori_loop(0, ny - 1, add_in, sred[y // 2].astype(F32))
        shbuf[y] = activated(total)

        def to_peer(i):
            off = offset_near(i, ny)
            rdma(
                shbuf.at[y], shbuf.at[y], sh_send.at[i], sh_recv.at[y], in_column(lax.rem(y + off, ny))
            ).start()

        each(0, ny - 1, to_peer)
        rdma(shbuf.at[y], shbuf.at[y], shf_send.at[y // 2], shf_recv.at[y], partner).start()

    arrivals(1)
    experts(1)
    hub(0)
    scales(0)
    scales(1)
    hub(1)
    own(0)
    own(1)
    gathers[0][1]()
    def shared_on(i):
        yy = 2 * i + c

        @pl.when(yy != y)
        def _():
            rdma(shbuf.at[yy], shbuf.at[yy], sh_send.at[0], sh_recv.at[yy], partner).wait_recv()
            rdma(shbuf.at[yy], shbuf.at[yy], shf_send.at[i], shf_recv.at[yy], partner).start()

    each(0, ny2, shared_on)
    swapped[2].wait_recv()
    down(0)
    gathers[1][1]()
    down(1)

    def shared_arrive(i):
        yy = 2 * i + 1 - c
        rdma(shbuf.at[yy], shbuf.at[yy], shf_send.at[i], shf_recv.at[yy], partner).wait_recv()

    each(0, ny2, shared_arrive)
    loads[14].wait()
    base = mixed_ref[...].astype(F32) + dot(shbuf[...].reshape(tok, ffe), sd[...])

    each(1, nx, lambda i: kv_copy(i).wait_send())
    each(1, z + 1, lambda i: q_copy(i).wait_send())
    each(1, nz - z, lambda i: part_copy(z + i).wait_send())
    a_drain()
    others(lambda i: dispatch(i).wait_send())

    @pl.when(c == 1)
    def _():
        dispatch_own().wait_send()

    for copy in swapped:
        copy.wait_send()
    each(0, ny2, lambda i: spre_copy(i).wait_send())

    def srs_drain(i):
        @pl.when(2 * i + c != y)
        def _():
            srs_copy(i).wait_send()

    each(0, ny2, srs_drain)
    for g in range(2):
        for r in (4, 3, 5, 2, 6):
            l1_copy(g, r).wait_send()
        for side in range(2):
            l2_copy(g, side).wait_send()
        for k in range(1, ny):
            squares_copy(g, k).wait_send()
        gathers[g][3]()

    @pl.when(owner)
    def _():
        each(
            0,
            ny - 1,
            lambda i: rdma(shbuf.at[y], shbuf.at[y], sh_send.at[i], sh_recv.at[y], partner).wait_send(),
        )

    def shared_forwarded(i):
        yy = 2 * i + c
        rdma(shbuf.at[yy], shbuf.at[yy], shf_send.at[i], shf_recv.at[yy], partner).wait_send()

    each(0, ny2, shared_forwarded)

    def returned(i):
        src = block_at(i, -1)
        rdma(ret_in.at[src], ret_in.at[src], r_send.at[i], r_recv.at[i], (src, tp)).wait_recv()

    others(returned)

    @pl.when(c == 1)
    def _():
        returned(own_i)

    rows = ret_in[...].reshape(nslot, feat)
    out_ref[...] = (base + (dot(w_hi[...], rows) + dot(w_lo[...], rows))).astype(BF16)

    def given(at):
        for core in range(2):
            give_back(at, core).wait_send()

    each(0, own_at, given)
    each(own_at + 1, nsp // 2, given)
    give_back(own_at, 1).wait_send()

    @pl.when(c == 1)
    def _():
        give_back(own_at, 0).wait_send()


def body(
    nx,
    queries,
    key_rows,
    value_rows,
    break_bias,
    stream,
    out_proj,
    norm_gain,
    expert_ids,
    route_weights,
    gate_proj,
    up_proj,
    down_proj,
    shared_gate,
    shared_up,
    shared_down,
):
    nsp, ntp = lax.axis_size("sp"), lax.axis_size("tp")
    nz, ny = nsp // nx, ntp // 2
    tok, hd = queries.shape
    feat = stream.shape[1]
    experts_local, _, ffe = gate_proj.shape
    ffs = shared_gate.shape[1]
    cap = 2 * expert_ids.shape[1] * tok // (experts_local * nsp)
    per_dest = experts_local * cap
    chunk = nsp * per_dest // ntp // 2
    srows = tok // ny
    wide = 2 * ffe + 128
    hk = (nx // 2) * tok

    def vm(*shape):
        return pltpu.VMEM(shape, BF16)

    def sems(*counts):
        return [pltpu.SemaphoreType.DMA(n if isinstance(n, tuple) else (n,)) for n in counts]

    scratch = [
        vm(tok, hd),
        vm(1, tok),
        vm(tok, feat),
        pltpu.VMEM((2, 1, feat), F32),
        pltpu.VMEM((2, tok), jnp.int32),
        pltpu.VMEM((2, tok), F32),
        vm(2, ny, hd, feat),
        vm(experts_local, 2, feat, ffe),
        vm(experts_local, 2, feat, ffe),
        vm(2, experts_local * ffe, feat),
        vm(feat, ffs),
        vm(feat, ffs),
        vm(ffs, feat),
        vm(nx, 2 * tok + 16, hd),
        vm(nz, tok, hd),
        vm(nz, tok + 16, hd),
        vm(nz, tok + 16, hd),
        vm(hk, hk),
        vm(2, ny, tok, hd),
        vm(nsp * per_dest, tok),
        vm(tok, nsp * per_dest),
        vm(tok, nsp * per_dest),
        vm(tok, feat),
        vm(nsp, per_dest, feat),
        vm(nsp // 2, 2, per_dest, feat),
        vm(2, ny, chunk, 2 * ffe),
        vm(2, 2, 3, chunk, 2 * ffe),
        vm(2, 2, chunk, 2 * ffe),
        vm(2, 2, chunk, 2 * ffe),
        pltpu.VMEM((2, ny, 1, ny * chunk), F32),
        pltpu.VMEM((2, ny, chunk, 128), F32),
        vm(ny, srows, wide),
        vm(ny // 2, srows, wide),
        vm(ny // 2, srows, wide),
        vm(ny, srows, wide),
        vm(2, ny, chunk, ffe),
        vm(ny, srows, ffs),
        vm(nsp // 2, 2, per_dest, feat),
        vm(nsp, per_dest, feat),
        *sems(16, nx, nx, nz, nz, nz, nz, 7, ny, ny, ny, nsp, (nsp // 2, 2), 4, 4, (2, ny), (2, 2, 3), (2, 2), (2, 2), (2, ny), (2, ny)),
        *sems(ny // 2, ny // 2, ny // 2, ny, (2, 7), (2, ny), ny, ny, ny // 2, ny, (nsp // 2, 2), nsp),
    ]
    large = pl.BlockSpec(memory_space=pl.ANY)
    return pl.pallas_call(
        functools.partial(layer_kernel, (nz, nx, ny)),
        out_shape=jax.ShapeDtypeStruct((tok, feat), BF16),
        in_specs=[large] * 15,
        out_specs=pl.BlockSpec(memory_space=pltpu.VMEM),
        scratch_shapes=scratch,
        compiler_params=pltpu.CompilerParams(
            collective_id=0, has_side_effects=True, vmem_limit_bytes=60 * 1024 * 1024
        ),
    )(
        queries,
        key_rows,
        value_rows,
        break_bias.T,
        stream,
        norm_gain.reshape(1, feat),
        expert_ids.T,
        route_weights.T,
        out_proj.reshape(ny, 2, hd, feat),
        gate_proj,
        up_proj,
        down_proj.reshape(experts_local * ffe, feat),
        shared_gate,
        shared_up,
        shared_down,
    )


def solution(mesh, nx=NX):
    in_specs = (
        P("sp", "tp"),
        P("sp", "tp"),
        P("sp", "tp"),
        P("sp", "tp"),
        P("sp", "tp"),
        P(None, "tp"),
        P("tp"),
        P("sp", None),
        P("sp", None),
        P("sp", "tp", None),
        P("sp", "tp", None),
        P("sp", None, "tp"),
        P("tp", None),
        P("tp", None),
        P(None, "tp"),
    )
    return jax.shard_map(
        functools.partial(body, nx), mesh=mesh, in_specs=in_specs, out_specs=P("sp", "tp"), check_vma=False
    )
```

```python
import functools

import jax
import jax.numpy as jnp
from jax import lax
from jax.experimental import pallas as pl
from jax.experimental.pallas import tpu as pltpu
from jax.sharding import PartitionSpec as P

EPS = 1e-06
NX = 4
MESH = pl.DeviceIdType.MESH
F32, BF16 = jnp.float32, jnp.bfloat16


def rdma(src, dst, send, recv, device):
    return pltpu.make_async_remote_copy(
        src_ref=src, dst_ref=dst, send_sem=send, recv_sem=recv, device_id=device, device_id_type=MESH
    )


def each(low, high, fn):
    def turn(i, carry):
        fn(i)
        return carry

    lax.fori_loop(low, high, turn, 0)


def offset_near(i, n):
    half = lax.div(i, 2) + 1
    return jnp.where(lax.rem(i, 2) == 0, half, n - half)


def dot(a, b):
    return jnp.dot(a, b, preferred_element_type=F32)


def dot_nt(a, b):
    return lax.dot_general(a, b, (((1,), (1,)), ((), ())), preferred_element_type=F32)


def halves(value):
    high = value.astype(BF16)
    return high, (value - high.astype(F32)).astype(BF16)


def iota(shape, dim):
    return lax.broadcasted_iota(jnp.int32, shape, dim)


def layer_kernel(
    sizes,
    q_hbm,
    k_hbm,
    v_hbm,
    bias_hbm,
    stream_hbm,
    gain_hbm,
    ids_hbm,
    rw_hbm,
    wo_hbm,
    wg_hbm,
    wu_hbm,
    wd_hbm,
    sg_hbm,
    su_hbm,
    sd_hbm,
    out_ref,
    q_ref,
    bias_ref,
    stream_ref,
    gain_ref,
    ids_ref,
    rw_ref,
    wo,
    wg,
    wu,
    wd,
    sg,
    su,
    sd,
    kv,
    qbuf,
    part_out,
    part_in,
    tri,
    abuf,
    pt,
    w_hi,
    w_lo,
    mixed_ref,
    snd,
    arr,
    red,
    hub_in,
    hub_out,
    own_in,
    square_rows,
    inverse,
    spart,
    spre,
    sred,
    srs_in,
    hbuf,
    shbuf,
    ret_out,
    ret_in,
    load_sem,
    kv_send,
    kv_recv,
    q_send,
    q_recv,
    p_send,
    p_recv,
    a_send,
    a_recv,
    af_send,
    af_recv,
    d_send,
    d_recv,
    w_send,
    w_recv,
    l1_send,
    l1_recv,
    l2_send,
    l2_recv,
    n_send,
    n_recv,
    spre_send,
    spre_recv,
    srs_send,
    srs_recv,
    h_send,
    h_recv,
    sh_send,
    sh_recv,
    shf_send,
    shf_recv,
    r_send,
    r_recv,
):
    nz, nx, ny = sizes
    nsp, ntp = nz * nx, ny * 2
    tok, hd = q_ref.shape
    feat = stream_ref.shape[1]
    ffe = wg.shape[3]
    nslot = nsp * snd.shape[1]
    per_dest = snd.shape[1]
    cap = per_dest // 2
    nexp = nsp * 2
    width = feat * ntp
    sp, tp = lax.axis_index("sp"), lax.axis_index("tp")
    z, x = sp // nx, lax.rem(sp, nx)
    y, c = tp // 2, lax.rem(tp, 2)
    partner = (sp, y * 2 + 1 - c)

    def in_column(yy):
        return (sp, yy * 2 + c)

    def load(i, src, dst):
        return pltpu.make_async_copy(src, dst, load_sem.at[i])

    barrier = pltpu.get_barrier_semaphore()

    def greet_row(i):
        to = z * nx + lax.rem(x + i, nx)
        pl.semaphore_signal(barrier, inc=1, device_id=(to, tp), device_id_type=MESH)

    def greet_later(zz):
        pl.semaphore_signal(barrier, inc=1, device_id=(zz * nx + x, tp), device_id_type=MESH)

    def greet_tp(i):
        pl.semaphore_signal(barrier, inc=1, device_id=in_column(lax.rem(y + i, ny)), device_id_type=MESH)

    each(1, ny, greet_tp)
    each(z + 1, nz, greet_later)
    each(1, nx, greet_row)
    pl.semaphore_signal(barrier, inc=1, device_id=partner, device_id_type=MESH)
    loads = [
        load(i, src, dst)
        for i, (src, dst) in enumerate(
            [
                (bias_hbm, bias_ref),
                (k_hbm, kv.at[x, 0:tok]),
                (v_hbm, kv.at[x, tok : 2 * tok]),
                (q_hbm, q_ref),
                (ids_hbm, ids_ref),
                (rw_hbm, rw_ref),
                (stream_hbm, stream_ref),
                (gain_hbm, gain_ref.at[c]),
                (wo_hbm.at[:, 0], wo.at[0]),
                (sg_hbm, sg),
                (su_hbm, su),
                (wg_hbm, wg.at[:, c]),
                (wu_hbm, wu.at[:, c]),
                (wd_hbm, wd.at[c]),
                (sd_hbm, sd),
                (wo_hbm.at[:, 1], wo.at[1]),
            ]
        )
    ]
    for copy in loads:
        copy.start()

    eye = iota((tok, tok), 0) == iota((tok, tok), 1)

    def to_row(column):
        return jnp.sum(jnp.where(eye, column, 0.0), axis=0, keepdims=True)

    def to_column(row):
        return jnp.sum(jnp.where(eye, row, 0.0), axis=1, keepdims=True)

    loads[0].wait()
    kv[x, 2 * tok : 2 * tok + 16, :] = jnp.broadcast_to(bias_ref[...].astype(F32), (16, tok)).astype(BF16)
    hk = (nx // 2) * tok
    tri[...] = (iota((hk, hk), 0) > iota((hk, hk), 1)).astype(BF16)
    for i in (1, 2, 3):
        loads[i].wait()

    def no_part(zs):
        part_in[zs] = jnp.zeros((tok + 16, hd), BF16)

    each(z + 1, nz, no_part)

    pl.semaphore_wait(barrier, nx - 1 + ny + z)

    def kv_copy(i):
        peer = lax.rem(x + i, nx)
        return rdma(kv.at[x], kv.at[x], kv_send.at[i], kv_recv.at[x], (z * nx + peer, tp))

    def q_copy(i):
        return rdma(q_ref, qbuf.at[z], q_send.at[i], q_recv.at[z], ((z - i) * nx + x, tp))

    each(1, nx, lambda i: kv_copy(i).start())
    each(1, z + 1, lambda i: q_copy(i).start())

    swapped = [
        rdma(mine, mine, w_send.at[i], w_recv.at[i], partner)
        for i, mine in enumerate((wg.at[:, c], wu.at[:, c], wd.at[c], gain_ref.at[c]))
    ]
    for i, copy in zip((11, 12, 13, 7), swapped):
        loads[i].wait()
        copy.start()

    loads[4].wait()
    loads[5].wait()
    exp_lane = iota((tok, nexp), 1).astype(F32)

    def columns(ref):
        return [to_column(ref[i : i + 1, :].astype(F32)) for i in range(2)]

    ids, rw = columns(ids_ref), columns(rw_ref)
    first, second = ids[0] == exp_lane, ids[1] == exp_lane
    named = jnp.where(first | second, 1.0, 0.0).astype(BF16)
    earlier = jnp.where(iota((tok, tok), 1) < iota((tok, tok), 0), 1.0, 0.0).astype(BF16)
    rank = dot(earlier, named).astype(BF16)
    spread = jnp.where(iota((nexp, nslot), 1) // cap == iota((nexp, nslot), 0), 1.0, 0.0).astype(BF16)
    weight_hi, weight_lo = halves(jnp.where(first, rw[0], 0.0) + jnp.where(second, rw[1], 0.0))
    slot_rank = lax.rem(iota((tok, nslot), 1), cap).astype(F32)
    taken = (dot(named, spread) > 0.5) & (dot(rank, spread) == slot_rank)
    taken_f = jnp.where(taken, 1.0, 0.0)
    pt[...] = taken_f.T.astype(BF16)
    w_hi[...] = (taken_f * dot(weight_hi, spread)).astype(BF16)
    w_lo[...] = (taken_f * dot(weight_lo, spread)).astype(BF16)

    def kv_arrive(i):
        xs = lax.rem(x + i, nx)
        rdma(kv.at[xs], kv.at[xs], kv_send.at[i], kv_recv.at[xs], (z * nx + xs, tp)).wait_recv()

    each(1, nx, kv_arrive)

    scale = hd ** (-0.5)

    def attend(q, own):
        logits, fails, parts = [], [], []
        for h in range(2):
            at = range(h * (nx // 2), (h + 1) * (nx // 2))
            keys = jnp.concatenate([kv[i, 0:tok, :] for i in at], axis=0)
            bias = jnp.concatenate([kv[i, 2 * tok : 2 * tok + 1, :] for i in at], axis=1).astype(F32)
            lg = dot_nt(q, keys) * scale + bias
            fail = -(jnp.maximum(lg, 0.0) + jnp.log(1.0 + jnp.exp(-jnp.abs(lg))))
            logits.append(lg + fail)
            if own:
                before = iota((tok, hk), 1) + h * hk < iota((tok, hk), 0) + x * tok
                fail = jnp.where(before, fail, 0.0)
            fails.append(fail)
            parts.append(halves(fail))
        stacked = jnp.concatenate([parts[0][0], parts[1][0], parts[0][1], parts[1][1]], axis=0)
        sums = dot(stacked, tri[...])
        tail0 = sums[0:tok] + sums[2 * tok : 3 * tok]
        tail1 = sums[tok : 2 * tok] + sums[3 * tok : 4 * tok]
        tail0 = tail0 + (tail1[:, 0:1] + fails[1][:, 0:1])
        total = tail0[:, 0:1] + fails[0][:, 0:1]
        acc = jnp.zeros((tok, hd), F32)
        for h, tail in enumerate((tail0, tail1)):
            at = range(h * (nx // 2), (h + 1) * (nx // 2))
            values = jnp.concatenate([kv[i, tok : 2 * tok, :] for i in at], axis=0)
            weights = jnp.exp(logits[h] + tail)
            if own:
                before = iota((tok, hk), 1) + h * hk < iota((tok, hk), 0) + x * tok
                weights = jnp.where(before, weights, 0.0)
            acc = acc + dot(weights.astype(BF16), values)
        return acc, total

    def part_copy(zq):
        return rdma(part_out.at[zq], part_in.at[z], p_send.at[zq], p_recv.at[z], (zq * nx + x, tp))

    def serve(i):
        zq = z + i
        rdma(qbuf.at[zq], qbuf.at[zq], q_send.at[i], q_recv.at[zq], (zq * nx + x, tp)).wait_recv()
        acc, total = attend(qbuf[zq], False)
        part_out[zq, 0:tok, :] = acc.astype(BF16)
        row = to_row(total)
        high, rest = row.astype(BF16), row - row.astype(BF16).astype(F32)
        mid, low = halves(rest)
        at_row = iota((16, tok), 0)
        rows = jnp.where(
            at_row == 0,
            high.astype(F32),
            jnp.where(at_row == 1, mid.astype(F32), jnp.where(at_row == 2, low.astype(F32), 0.0)),
        )
        part_out[zq, tok : tok + 16, :] = rows.astype(BF16)
        part_copy(zq).start()

    each(1, nz - z, serve)
    acc, total = attend(q_ref[...], True)

    def part_arrive(i):
        zs = z - i
        rdma(part_in.at[zs], part_in.at[zs], p_send.at[zs], p_recv.at[zs], (zs * nx + x, tp)).wait_recv()

    each(1, z + 1, part_arrive)
    later = to_row(total)
    for i in range(1, nz):
        zs = lax.rem(z - i + nz, nz)
        acc = acc + to_column(jnp.exp(later)) * part_in[zs, 0:tok, :].astype(F32)
        later = later + jnp.sum(part_in[zs, tok : tok + 16, :].astype(F32), axis=0, keepdims=True)

    far_first = (4, 3, 5, 2, 6, 1, 7)

    def gather(buf, send, recv, fsend=None, frecv=None):
        def block_copy(k, block, off):
            here = buf.at[c, block] if fsend is not None else buf.at[block]
            return rdma(here, here, send.at[k], recv.at[block], in_column(lax.rem(y + off, ny)))

        def across(block):
            here = buf.at[c, block]
            return rdma(here, here, fsend.at[block], frecv.at[block], partner)

        def start():
            for k, off in enumerate(far_first):
                block_copy(k, y, off).start()
            if fsend is not None:
                across(y).start()

        def pass_on():
            for k, off in enumerate(far_first):
                block = lax.rem(y + ny - off, ny)
                block_copy(k, block, off).wait_recv()
                if fsend is not None:
                    across(block).start()

        def finish():
            def arrive(block):
                there = buf.at[1 - c, block]
                rdma(there, there, fsend.at[block], frecv.at[block], partner).wait_recv()

            each(0, ny, arrive)

        def drain():
            for k, off in enumerate(far_first):
                block_copy(k, y, off).wait_send()
            if fsend is not None:
                each(0, ny, lambda block: across(block).wait_send())

        return start, pass_on, finish, drain

    abuf[c, y] = acc.astype(BF16)
    a_start, a_pass, a_finish, a_drain = gather(abuf, a_send, a_recv, af_send, af_recv)
    a_start()
    a_pass()
    loads[8].wait()
    loads[15].wait()
    loads[6].wait()

    def project(core):
        total = jnp.zeros((tok, feat), F32)
        for i in range(0, ny, 2):
            heads = jnp.concatenate([abuf[core, i], abuf[core, i + 1]], axis=1)
            total = total + dot(heads, wo[core, i : i + 2].reshape(2 * hd, feat))
        return total

    projected = stream_ref[...].astype(F32) + project(c)
    a_finish()
    projected = projected + project(1 - c)
    mixed = projected.astype(BF16)
    mixed_ref[...] = mixed

    snd[...] = dot(pt[...], mixed).astype(BF16).reshape(nsp, per_dest, feat)

    def block_at(i, sign):
        rank = lax.div(i, nx)
        dz = jnp.where(rank == nz - 1, 0, offset_near(nz - 2 - rank, nz))
        dx = lax.rem(i, nx)
        return lax.rem(z + sign * dz + nz, nz) * nx + lax.rem(x + sign * dx + nx, nx)

    half = nsp // 2
    own_i = (nz - 1) * nx
    own_at = own_i % half

    def wrapped(value, n):
        return jnp.where(value >= n, value - n, value)

    def step_z(rank):
        i = nz - 2 - rank
        return 0 if rank == nz - 1 else (i // 2 + 1 if i % 2 == 0 else nz - (i // 2 + 1))

    before = [wrapped(z + (nz - step_z(rank)) % nz, nz) * nx for rank in range(nz)]
    after = [wrapped(z + step_z(rank), nz) * nx for rank in range(nz)]
    left = [wrapped(x + (nx - dx) % nx, nx) for dx in range(nx)]
    right = [wrapped(x + dx, nx) for dx in range(nx)]

    def send_out(i):
        to = before[i // nx] + left[i % nx]
        at, core = i % half, 1 - i // half
        rdma(snd.at[to], arr.at[at, c], d_send.at[i], d_recv.at[at, c], (to, y * 2 + core)).start()

    def others(fn):
        each(0, own_i, fn)
        each(own_i + 1, nsp, fn)

    def dispatch(i):
        to = block_at(i, -1)
        core = jnp.where(i < half, 1, 0)
        at = jnp.where(i < half, i, i - half)
        return rdma(snd.at[to], arr.at[at, c], d_send.at[i], d_recv.at[at, c], (to, y * 2 + core))

    def dispatch_own():
        return rdma(snd.at[sp], arr.at[own_at, c], d_send.at[own_i], d_recv.at[own_at, c], partner)

    for i in range(nsp):
        if i != own_i:
            send_out(i)

    @pl.when(c == 0)
    def _():
        arr[own_at, 0] = snd[sp]

    @pl.when(c == 1)
    def _():
        dispatch_own().start()


    def products(rows, gain, lhs_of, gate_w, up_w):
        value = rows.astype(F32)
        squares = jnp.sum(value * value, axis=1, keepdims=True)
        lhs = lhs_of((value * gain).astype(BF16))
        gate = dot(lhs, gate_w).astype(BF16)
        up = dot(lhs, up_w).astype(BF16)
        return gate, up, squares

    def two_lanes(column):
        high, low = halves(column)
        lane = iota((column.shape[0], 128), 1)
        return jnp.where(
            lane == 0, high.astype(F32), jnp.where(lane == 1, low.astype(F32), 0.0)
        ).astype(BF16)

    def laid(ref, lo, value):
        ref[:, :, lo : lo + value.shape[1]] = value.reshape(ref.shape[0], ref.shape[1], value.shape[1])

    def packed(total):
        squares = total[:, 2 * ffe : 2 * ffe + 1] + total[:, 2 * ffe + 1 : 2 * ffe + 2]
        return total[:, 0 : 2 * ffe].astype(BF16), two_lanes(squares)

    def activated(total):
        squares = total[:, 2 * ffe : 2 * ffe + 1] + total[:, 2 * ffe + 1 : 2 * ffe + 2]
        return scaled_hidden(total, lax.rsqrt(squares / width + EPS))

    def scaled_hidden(total, inv):
        gate, up = total[:, 0:ffe] * inv, total[:, ffe : 2 * ffe] * inv
        return (gate * jax.nn.sigmoid(gate) * up).astype(BF16)

    loads[9].wait()
    loads[10].wait()
    gate, up, squares = products(mixed, gain_ref[c], lambda a: a, sg[...], su[...])
    laid(spart, 0, gate)
    laid(spart, ffe, up)
    laid(spart, 2 * ffe, two_lanes(squares))
    ny2 = ny // 2

    def spre_copy(i):
        yy = 2 * i + 1 - c
        return rdma(spart.at[yy], spre.at[i], spre_send.at[i], spre_recv.at[i], partner)

    each(0, ny2, lambda i: spre_copy(i).start())

    def srs_copy(i):
        yy = 2 * i + c
        return rdma(sred.at[i], srs_in.at[y], srs_send.at[i], srs_recv.at[y], in_column(yy))

    def shared_add(i):
        yy = 2 * i + c
        rdma(spre.at[i], spre.at[i], spre_send.at[i], spre_recv.at[i], partner).wait_recv()
        sums, squares = packed(spart[yy].astype(F32) + spre[i].astype(F32))
        sred[i, :, 0 : 2 * ffe] = sums
        sred[i, :, 2 * ffe : 2 * ffe + 128] = squares

        @pl.when(yy != y)
        def _():
            srs_copy(i).start()

    each(0, ny2, shared_add)

    npos, chunk = nsp // 4, red.shape[2]
    rows_g = npos * per_dest

    def by_expert(a):
        zero = jnp.zeros_like(a)
        mine = lax.rem(iota(a.shape, 0), per_dest) < cap
        return jnp.concatenate([jnp.where(mine, a, zero), jnp.where(mine, zero, a)], axis=1)

    def arrivals(g):
        def arrive(at):
            for core in range(2):
                here = arr.at[at, core]
                rdma(here, here, d_send.at[1], d_recv.at[at, core], partner).wait_recv()

        if g != own_at // npos:
            each(g * npos, (g + 1) * npos, arrive)
        else:
            each(g * npos, own_at, arrive)
            each(own_at + 1, (g + 1) * npos, arrive)
            here = arr.at[own_at, 1]
            rdma(here, here, d_send.at[1], d_recv.at[own_at, 1], partner).wait_recv()

            @pl.when(c == 1)
            def _():
                here = arr.at[own_at, 0]
                rdma(here, here, d_send.at[1], d_recv.at[own_at, 0], partner).wait_recv()

    def squares_copy(g, k):
        here = square_rows.at[g, y]
        return rdma(here, here, n_send.at[g, k], n_recv.at[g, y], in_column(lax.rem(y + k, ny)))

    def scales(g):
        def arrive(k):
            ys = lax.rem(y + k, ny)
            here = square_rows.at[g, ys]
            rdma(here, here, n_send.at[g, k], n_recv.at[g, ys], partner).wait_recv()

        each(1, ny, arrive)
        squares = square_rows[g, 0]
        for ys in range(1, ny):
            squares = squares + square_rows[g, ys]
        inv = to_column(lax.rsqrt(squares / width + EPS))
        inverse[g] = jnp.broadcast_to(inv, (rows_g, 128)).reshape(ny, chunk, 128)

    def experts(g):
        at = slice(g * npos, (g + 1) * npos)
        rows = jnp.concatenate([arr[at, core].reshape(rows_g, feat) for core in range(2)], axis=1)
        gain = jnp.concatenate([gain_ref[0], gain_ref[1]], axis=1)
        gate, up, squares = products(
            rows, gain, by_expert, wg[...].reshape(4 * feat, ffe), wu[...].reshape(4 * feat, ffe)
        )
        square_rows[g, y] = to_row(squares)
        for k in range(1, ny):
            squares_copy(g, k).start()
        red[g, :, :, 0:ffe] = gate.reshape(ny, chunk, ffe)
        red[g, :, :, ffe : 2 * ffe] = up.reshape(ny, chunk, ffe)
        for r in (4, 3, 5, 2, 6):
            l1_copy(g, r).start()

    def l1_copy(g, r):
        if r == 4:
            side = lax.rem(y, 2)
            hub, k = jnp.where(side == 0, 3, 5), 2
        else:
            side = 0 if r < 4 else 1
            hub, k = (r - 1, r - 2) if r < 4 else (r + 1, ny - r - 2)
        return rdma(
            red.at[g, lax.rem(y + r, ny)],
            hub_in.at[g, side, k],
            l1_send.at[g, r],
            l1_recv.at[g, side, k],
            in_column(lax.rem(y + hub, ny)),
        )

    def l2_copy(g, side):
        to = lax.rem(y + (1 if side == 0 else ny - 1), ny)
        return rdma(hub_out.at[g, side], own_in.at[g, side], l2_send.at[g, side], l2_recv.at[g, side], in_column(to))

    def hub(g):
        for side in range(2):
            def add_in(k, total):
                here = hub_in.at[g, side, k]
                rdma(here, here, l1_send.at[g, 2], l1_recv.at[g, side, k], partner).wait_recv()
                return total + hub_in[g, side, k].astype(F32)

            odd = lax.rem(y, 2)
            mine = red[g, lax.rem(y + (1 if side == 0 else ny - 1), ny)].astype(F32)
            total = lax.fori_loop(0, 2 + odd if side == 0 else 3 - odd, add_in, mine)
            hub_out[g, side] = total.astype(BF16)
            l2_copy(g, side).start()

    gathers = [gather(hbuf.at[g], h_send.at[g], h_recv.at[g]) for g in range(2)]

    def own(g):
        total = red[g, y].astype(F32)
        for side in range(2):
            here = own_in.at[g, side]
            rdma(here, here, l2_send.at[g, side], l2_recv.at[g, side], partner).wait_recv()
            total = total + own_in[g, side].astype(F32)
        hbuf[g, y] = scaled_hidden(total, inverse[g, y][:, 0:1])
        gathers[g][0]()

    def give_back(at, core):
        i = at + half * (1 - c)
        to = block_at(i, 1)
        return rdma(ret_out.at[at, core], ret_in.at[sp], r_send.at[at, core], r_recv.at[i], (to, y * 2 + core))

    def down(g):
        rows = by_expert(hbuf[g].reshape(rows_g, ffe))
        at = slice(g * npos, (g + 1) * npos)
        for core in range(2):
            ret_out[at, core] = dot(rows, wd[core]).astype(BF16).reshape(npos, per_dest, feat)

        for at in range(g * npos, (g + 1) * npos):
            if at != own_at:
                near = at + half
                to = jnp.where(c == 1, after[at // nx] + right[at % nx], after[near // nx] + right[near % nx])
                for core in range(2):
                    rdma(
                        ret_out.at[at, core],
                        ret_in.at[sp],
                        r_send.at[at, core],
                        r_recv.at[at + half * (1 - c)],
                        (to, y * 2 + core),
                    ).start()
        if g == own_at // npos:
            give_back(own_at, 1).start()

            @pl.when(c == 1)
            def _():
                give_back(own_at, 0).start()

            @pl.when(c == 0)
            def _():
                ret_in[sp] = ret_out[own_at, 0]

    owner = lax.rem(y, 2) == c

    arrivals(0)
    for i in (0, 1, 3):
        swapped[i].wait_recv()
    experts(0)

    @pl.when(owner)
    def _():
        def add_in(i, total):
            ys = lax.rem(y + offset_near(i, ny), ny)
            rdma(srs_in.at[ys], srs_in.at[ys], srs_send.at[0], srs_recv.at[ys], partner).wait_recv()
            return total + srs_in[ys].astype(F32)

        total = lax.fori_loop(0, ny - 1, add_in, sred[y // 2].astype(F32))
        shbuf[y] = activated(total)

        def to_peer(i):
            off = offset_near(i, ny)
            rdma(
                shbuf.at[y], shbuf.at[y], sh_send.at[i], sh_recv.at[y], in_column(lax.rem(y + off, ny))
            ).start()

        each(0, ny - 1, to_peer)
        rdma(shbuf.at[y], shbuf.at[y], shf_send.at[y // 2], shf_recv.at[y], partner).start()

    arrivals(1)
    experts(1)
    hub(0)
    scales(0)
    scales(1)
    hub(1)
    own(0)
    own(1)
    gathers[0][1]()
    def shared_on(i):
        yy = 2 * i + c

        @pl.when(yy != y)
        def _():
            rdma(shbuf.at[yy], shbuf.at[yy], sh_send.at[0], sh_recv.at[yy], partner).wait_recv()
            rdma(shbuf.at[yy], shbuf.at[yy], shf_send.at[i], shf_recv.at[yy], partner).start()

    each(0, ny2, shared_on)
    swapped[2].wait_recv()
    down(0)
    gathers[1][1]()
    down(1)

    def shared_arrive(i):
        yy = 2 * i + 1 - c
        rdma(shbuf.at[yy], shbuf.at[yy], shf_send.at[i], shf_recv.at[yy], partner).wait_recv()

    each(0, ny2, shared_arrive)
    loads[14].wait()
    base = mixed_ref[...].astype(F32) + dot(shbuf[...].reshape(tok, ffe), sd[...])

    each(1, nx, lambda i: kv_copy(i).wait_send())
    each(1, z + 1, lambda i: q_copy(i).wait_send())
    each(1, nz - z, lambda i: part_copy(z + i).wait_send())
    a_drain()
    others(lambda i: dispatch(i).wait_send())

    @pl.when(c == 1)
    def _():
        dispatch_own().wait_send()

    for copy in swapped:
        copy.wait_send()
    each(0, ny2, lambda i: spre_copy(i).wait_send())

    def srs_drain(i):
        @pl.when(2 * i + c != y)
        def _():
            srs_copy(i).wait_send()

    each(0, ny2, srs_drain)
    for g in range(2):
        for r in (4, 3, 5, 2, 6):
            l1_copy(g, r).wait_send()
        for side in range(2):
            l2_copy(g, side).wait_send()
        for k in range(1, ny):
            squares_copy(g, k).wait_send()
        gathers[g][3]()

    @pl.when(owner)
    def _():
        each(
            0,
            ny - 1,
            lambda i: rdma(shbuf.at[y], shbuf.at[y], sh_send.at[i], sh_recv.at[y], partner).wait_send(),
        )

    def shared_forwarded(i):
        yy = 2 * i + c
        rdma(shbuf.at[yy], shbuf.at[yy], shf_send.at[i], shf_recv.at[yy], partner).wait_send()

    each(0, ny2, shared_forwarded)

    def returned(i):
        src = block_at(i, -1)
        rdma(ret_in.at[src], ret_in.at[src], r_send.at[i], r_recv.at[i], (src, tp)).wait_recv()

    others(returned)

    @pl.when(c == 1)
    def _():
        returned(own_i)

    rows = ret_in[...].reshape(nslot, feat)
    out_ref[...] = (base + (dot(w_hi[...], rows) + dot(w_lo[...], rows))).astype(BF16)

    def given(at):
        for core in range(2):
            give_back(at, core).wait_send()

    each(0, own_at, given)
    each(own_at + 1, nsp // 2, given)
    give_back(own_at, 1).wait_send()

    @pl.when(c == 1)
    def _():
        give_back(own_at, 0).wait_send()


def body(
    nx,
    queries,
    key_rows,
    value_rows,
    break_bias,
    stream,
    out_proj,
    norm_gain,
    expert_ids,
    route_weights,
    gate_proj,
    up_proj,
    down_proj,
    shared_gate,
    shared_up,
    shared_down,
):
    nsp, ntp = lax.axis_size("sp"), lax.axis_size("tp")
    nz, ny = nsp // nx, ntp // 2
    tok, hd = queries.shape
    feat = stream.shape[1]
    experts_local, _, ffe = gate_proj.shape
    ffs = shared_gate.shape[1]
    cap = 2 * expert_ids.shape[1] * tok // (experts_local * nsp)
    per_dest = experts_local * cap
    chunk = nsp * per_dest // ntp // 2
    srows = tok // ny
    wide = 2 * ffe + 128
    hk = (nx // 2) * tok

    def vm(*shape):
        return pltpu.VMEM(shape, BF16)

    def sems(*counts):
        return [pltpu.SemaphoreType.DMA(n if isinstance(n, tuple) else (n,)) for n in counts]

    scratch = [
        vm(tok, hd),
        vm(1, tok),
        vm(tok, feat),
        pltpu.VMEM((2, 1, feat), F32),
        pltpu.VMEM((2, tok), jnp.int32),
        pltpu.VMEM((2, tok), F32),
        vm(2, ny, hd, feat),
        vm(experts_local, 2, feat, ffe),
        vm(experts_local, 2, feat, ffe),
        vm(2, experts_local * ffe, feat),
        vm(feat, ffs),
        vm(feat, ffs),
        vm(ffs, feat),
        vm(nx, 2 * tok + 16, hd),
        vm(nz, tok, hd),
        vm(nz, tok + 16, hd),
        vm(nz, tok + 16, hd),
        vm(hk, hk),
        vm(2, ny, tok, hd),
        vm(nsp * per_dest, tok),
        vm(tok, nsp * per_dest),
        vm(tok, nsp * per_dest),
        vm(tok, feat),
        vm(nsp, per_dest, feat),
        vm(nsp // 2, 2, per_dest, feat),
        vm(2, ny, chunk, 2 * ffe),
        vm(2, 2, 3, chunk, 2 * ffe),
        vm(2, 2, chunk, 2 * ffe),
        vm(2, 2, chunk, 2 * ffe),
        pltpu.VMEM((2, ny, 1, ny * chunk), F32),
        pltpu.VMEM((2, ny, chunk, 128), F32),
        vm(ny, srows, wide),
        vm(ny // 2, srows, wide),
        vm(ny // 2, srows, wide),
        vm(ny, srows, wide),
        vm(2, ny, chunk, ffe),
        vm(ny, srows, ffs),
        vm(nsp // 2, 2, per_dest, feat),
        vm(nsp, per_dest, feat),
        *sems(16, nx, nx, nz, nz, nz, nz, 7, ny, ny, ny, nsp, (nsp // 2, 2), 4, 4, (2, ny), (2, 2, 3), (2, 2), (2, 2), (2, ny), (2, ny)),
        *sems(ny // 2, ny // 2, ny // 2, ny, (2, 7), (2, ny), ny, ny, ny // 2, ny, (nsp // 2, 2), nsp),
    ]
    large = pl.BlockSpec(memory_space=pl.ANY)
    return pl.pallas_call(
        functools.partial(layer_kernel, (nz, nx, ny)),
        out_shape=jax.ShapeDtypeStruct((tok, feat), BF16),
        in_specs=[large] * 15,
        out_specs=pl.BlockSpec(memory_space=pltpu.VMEM),
        scratch_shapes=scratch,
        compiler_params=pltpu.CompilerParams(
            collective_id=0, has_side_effects=True, vmem_limit_bytes=60 * 1024 * 1024
        ),
    )(
        queries,
        key_rows,
        value_rows,
        break_bias.T,
        stream,
        norm_gain.reshape(1, feat),
        expert_ids.T,
        route_weights.T,
        out_proj.reshape(ny, 2, hd, feat),
        gate_proj,
        up_proj,
        down_proj.reshape(experts_local * ffe, feat),
        shared_gate,
        shared_up,
        shared_down,
    )


def solution(mesh, nx=NX):
    in_specs = (
        P("sp", "tp"),
        P("sp", "tp"),
        P("sp", "tp"),
        P("sp", "tp"),
        P("sp", "tp"),
        P(None, "tp"),
        P("tp"),
        P("sp", None),
        P("sp", None),
        P("sp", "tp", None),
        P("sp", "tp", None),
        P("sp", None, "tp"),
        P("tp", None),
        P("tp", None),
        P(None, "tp"),
    )
    return jax.shard_map(
        functools.partial(body, nx), mesh=mesh, in_specs=in_specs, out_specs=P("sp", "tp"), check_vma=False
    )
```

```python
import functools

import jax
import jax.numpy as jnp
from jax import lax
from jax.experimental import pallas as pl
from jax.experimental.pallas import tpu as pltpu
from jax.sharding import PartitionSpec as P

EPS = 1e-06
NX = 4
MESH = pl.DeviceIdType.MESH
F32, BF16 = jnp.float32, jnp.bfloat16


def rdma(src, dst, send, recv, device):
    return pltpu.make_async_remote_copy(
        src_ref=src, dst_ref=dst, send_sem=send, recv_sem=recv, device_id=device, device_id_type=MESH
    )


def each(low, high, fn):
    def turn(i, carry):
        fn(i)
        return carry

    lax.fori_loop(low, high, turn, 0)


def offset_near(i, n):
    half = lax.div(i, 2) + 1
    return jnp.where(lax.rem(i, 2) == 0, half, n - half)


def dot(a, b):
    return jnp.dot(a, b, preferred_element_type=F32)


def dot_nt(a, b):
    return lax.dot_general(a, b, (((1,), (1,)), ((), ())), preferred_element_type=F32)


def halves(value):
    high = value.astype(BF16)
    return high, (value - high.astype(F32)).astype(BF16)


def iota(shape, dim):
    return lax.broadcasted_iota(jnp.int32, shape, dim)


def layer_kernel(
    sizes,
    q_hbm,
    k_hbm,
    v_hbm,
    bias_hbm,
    stream_hbm,
    gain_hbm,
    ids_hbm,
    rw_hbm,
    wo_hbm,
    wg_hbm,
    wu_hbm,
    wd_hbm,
    sg_hbm,
    su_hbm,
    sd_hbm,
    out_ref,
    q_ref,
    bias_ref,
    stream_ref,
    gain_ref,
    ids_ref,
    rw_ref,
    wo,
    wg,
    wu,
    wd,
    sg,
    su,
    sd,
    kv,
    qbuf,
    part_out,
    part_in,
    tri,
    abuf,
    pt,
    w_hi,
    w_lo,
    mixed_ref,
    snd,
    arr,
    red,
    hub_in,
    hub_out,
    own_in,
    square_rows,
    inverse,
    spart,
    spre,
    sred,
    srs_in,
    hbuf,
    shbuf,
    ret_out,
    ret_in,
    load_sem,
    kv_send,
    kv_recv,
    q_send,
    q_recv,
    p_send,
    p_recv,
    a_send,
    a_recv,
    af_send,
    af_recv,
    d_send,
    d_recv,
    w_send,
    w_recv,
    l1_send,
    l1_recv,
    l2_send,
    l2_recv,
    n_send,
    n_recv,
    spre_send,
    spre_recv,
    srs_send,
    srs_recv,
    h_send,
    h_recv,
    sh_send,
    sh_recv,
    shf_send,
    shf_recv,
    r_send,
    r_recv,
):
    nz, nx, ny = sizes
    nsp, ntp = nz * nx, ny * 2
    tok, hd = q_ref.shape
    feat = stream_ref.shape[1]
    ffe = wg.shape[3]
    nslot = nsp * snd.shape[1]
    per_dest = snd.shape[1]
    cap = per_dest // 2
    nexp = nsp * 2
    width = feat * ntp
    sp, tp = lax.axis_index("sp"), lax.axis_index("tp")
    z, x = sp // nx, lax.rem(sp, nx)
    y, c = tp // 2, lax.rem(tp, 2)
    partner = (sp, y * 2 + 1 - c)

    def in_column(yy):
        return (sp, yy * 2 + c)

    def load(i, src, dst):
        return pltpu.make_async_copy(src, dst, load_sem.at[i])

    barrier = pltpu.get_barrier_semaphore()

    def greet_row(i):
        to = z * nx + lax.rem(x + i, nx)
        pl.semaphore_signal(barrier, inc=1, device_id=(to, tp), device_id_type=MESH)

    def greet_later(zz):
        pl.semaphore_signal(barrier, inc=1, device_id=(zz * nx + x, tp), device_id_type=MESH)

    def greet_tp(i):
        pl.semaphore_signal(barrier, inc=1, device_id=in_column(lax.rem(y + i, ny)), device_id_type=MESH)

    each(1, ny, greet_tp)
    each(z + 1, nz, greet_later)
    each(1, nx, greet_row)
    pl.semaphore_signal(barrier, inc=1, device_id=partner, device_id_type=MESH)
    loads = [
        load(i, src, dst)
        for i, (src, dst) in enumerate(
            [
                (bias_hbm, bias_ref),
                (k_hbm, kv.at[x, 0:tok]),
                (v_hbm, kv.at[x, tok : 2 * tok]),
                (q_hbm, q_ref),
                (ids_hbm, ids_ref),
                (rw_hbm, rw_ref),
                (stream_hbm, stream_ref),
                (gain_hbm, gain_ref.at[c]),
                (wo_hbm.at[:, 0], wo.at[0]),
                (sg_hbm, sg),
                (su_hbm, su),
                (wg_hbm, wg.at[:, c]),
                (wu_hbm, wu.at[:, c]),
                (wd_hbm, wd.at[c]),
                (sd_hbm, sd),
                (wo_hbm.at[:, 1], wo.at[1]),
            ]
        )
    ]
    for copy in loads:
        copy.start()

    eye = iota((tok, tok), 0) == iota((tok, tok), 1)

    def to_row(column):
        return jnp.sum(jnp.where(eye, column, 0.0), axis=0, keepdims=True)

    def to_column(row):
        return jnp.sum(jnp.where(eye, row, 0.0), axis=1, keepdims=True)

    loads[0].wait()
    kv[x, 2 * tok : 2 * tok + 16, :] = jnp.broadcast_to(bias_ref[...].astype(F32), (16, tok)).astype(BF16)
    hk = (nx // 2) * tok
    tri[...] = (iota((hk, hk), 0) > iota((hk, hk), 1)).astype(BF16)
    for i in (1, 2, 3):
        loads[i].wait()

    def no_part(zs):
        part_in[zs] = jnp.zeros((tok + 16, hd), BF16)

    each(z + 1, nz, no_part)

    pl.semaphore_wait(barrier, nx - 1 + ny + z)

    def kv_copy(i):
        peer = lax.rem(x + i, nx)
        return rdma(kv.at[x], kv.at[x], kv_send.at[i], kv_recv.at[x], (z * nx + peer, tp))

    def q_copy(i):
        return rdma(q_ref, qbuf.at[z], q_send.at[i], q_recv.at[z], ((z - i) * nx + x, tp))

    each(1, nx, lambda i: kv_copy(i).start())
    each(1, z + 1, lambda i: q_copy(i).start())

    swapped = [
        rdma(mine, mine, w_send.at[i], w_recv.at[i], partner)
        for i, mine in enumerate((wg.at[:, c], wu.at[:, c], wd.at[c], gain_ref.at[c]))
    ]
    for i, copy in zip((11, 12, 13, 7), swapped):
        loads[i].wait()
        copy.start()

    loads[4].wait()
    loads[5].wait()
    exp_lane = iota((tok, nexp), 1).astype(F32)

    def columns(ref):
        return [to_column(ref[i : i + 1, :].astype(F32)) for i in range(2)]

    ids, rw = columns(ids_ref), columns(rw_ref)
    first, second = ids[0] == exp_lane, ids[1] == exp_lane
    named = jnp.where(first | second, 1.0, 0.0).astype(BF16)
    earlier = jnp.where(iota((tok, tok), 1) < iota((tok, tok), 0), 1.0, 0.0).astype(BF16)
    rank = dot(earlier, named).astype(BF16)
    spread = jnp.where(iota((nexp, nslot), 1) // cap == iota((nexp, nslot), 0), 1.0, 0.0).astype(BF16)
    weight_hi, weight_lo = halves(jnp.where(first, rw[0], 0.0) + jnp.where(second, rw[1], 0.0))
    slot_rank = lax.rem(iota((tok, nslot), 1), cap).astype(F32)
    taken = (dot(named, spread) > 0.5) & (dot(rank, spread) == slot_rank)
    taken_f = jnp.where(taken, 1.0, 0.0)
    pt[...] = taken_f.T.astype(BF16)
    w_hi[...] = (taken_f * dot(weight_hi, spread)).astype(BF16)
    w_lo[...] = (taken_f * dot(weight_lo, spread)).astype(BF16)

    def kv_arrive(i):
        xs = lax.rem(x + i, nx)
        rdma(kv.at[xs], kv.at[xs], kv_send.at[i], kv_recv.at[xs], (z * nx + xs, tp)).wait_recv()

    each(1, nx, kv_arrive)

    scale = hd ** (-0.5)

    def attend(q, own):
        logits, fails, parts = [], [], []
        for h in range(2):
            at = range(h * (nx // 2), (h + 1) * (nx // 2))
            keys = jnp.concatenate([kv[i, 0:tok, :] for i in at], axis=0)
            bias = jnp.concatenate([kv[i, 2 * tok : 2 * tok + 1, :] for i in at], axis=1).astype(F32)
            lg = dot_nt(q, keys) * scale + bias
            fail = -(jnp.maximum(lg, 0.0) + jnp.log(1.0 + jnp.exp(-jnp.abs(lg))))
            logits.append(lg + fail)
            if own:
                before = iota((tok, hk), 1) + h * hk < iota((tok, hk), 0) + x * tok
                fail = jnp.where(before, fail, 0.0)
            fails.append(fail)
            parts.append(halves(fail))
        stacked = jnp.concatenate([parts[0][0], parts[1][0], parts[0][1], parts[1][1]], axis=0)
        sums = dot(stacked, tri[...])
        tail0 = sums[0:tok] + sums[2 * tok : 3 * tok]
        tail1 = sums[tok : 2 * tok] + sums[3 * tok : 4 * tok]
        tail0 = tail0 + (tail1[:, 0:1] + fails[1][:, 0:1])
        total = tail0[:, 0:1] + fails[0][:, 0:1]
        acc = jnp.zeros((tok, hd), F32)
        for h, tail in enumerate((tail0, tail1)):
            at = range(h * (nx // 2), (h + 1) * (nx // 2))
            values = jnp.concatenate([kv[i, tok : 2 * tok, :] for i in at], axis=0)
            weights = jnp.exp(logits[h] + tail)
            if own:
                before = iota((tok, hk), 1) + h * hk < iota((tok, hk), 0) + x * tok
                weights = jnp.where(before, weights, 0.0)
            acc = acc + dot(weights.astype(BF16), values)
        return acc, total

    def part_copy(zq):
        return rdma(part_out.at[zq], part_in.at[z], p_send.at[zq], p_recv.at[z], (zq * nx + x, tp))

    def serve(i):
        zq = z + i
        rdma(qbuf.at[zq], qbuf.at[zq], q_send.at[i], q_recv.at[zq], (zq * nx + x, tp)).wait_recv()
        acc, total = attend(qbuf[zq], False)
        part_out[zq, 0:tok, :] = acc.astype(BF16)
        row = to_row(total)
        high, rest = row.astype(BF16), row - row.astype(BF16).astype(F32)
        mid, low = halves(rest)
        at_row = iota((16, tok), 0)
        rows = jnp.where(
            at_row == 0,
            high.astype(F32),
            jnp.where(at_row == 1, mid.astype(F32), jnp.where(at_row == 2, low.astype(F32), 0.0)),
        )
        part_out[zq, tok : tok + 16, :] = rows.astype(BF16)
        part_copy(zq).start()

    each(1, nz - z, serve)
    acc, total = attend(q_ref[...], True)

    def part_arrive(i):
        zs = z - i
        rdma(part_in.at[zs], part_in.at[zs], p_send.at[zs], p_recv.at[zs], (zs * nx + x, tp)).wait_recv()

    each(1, z + 1, part_arrive)
    later = to_row(total)
    for i in range(1, nz):
        zs = lax.rem(z - i + nz, nz)
        acc = acc + to_column(jnp.exp(later)) * part_in[zs, 0:tok, :].astype(F32)
        later = later + jnp.sum(part_in[zs, tok : tok + 16, :].astype(F32), axis=0, keepdims=True)

    far_first = (4, 3, 5, 2, 6, 1, 7)

    def gather(buf, send, recv, fsend=None, frecv=None):
        def block_copy(k, block, off):
            here = buf.at[c, block] if fsend is not None else buf.at[block]
            return rdma(here, here, send.at[k], recv.at[block], in_column(lax.rem(y + off, ny)))

        def across(block):
            here = buf.at[c, block]
            return rdma(here, here, fsend.at[block], frecv.at[block], partner)

        def start():
            for k, off in enumerate(far_first):
                block_copy(k, y, off).start()
            if fsend is not None:
                across(y).start()

        def pass_on():
            for k, off in enumerate(far_first):
                block = lax.rem(y + ny - off, ny)
                block_copy(k, block, off).wait_recv()
                if fsend is not None:
                    across(block).start()

        def finish():
            def arrive(block):
                there = buf.at[1 - c, block]
                rdma(there, there, fsend.at[block], frecv.at[block], partner).wait_recv()

            each(0, ny, arrive)

        def drain():
            for k, off in enumerate(far_first):
                block_copy(k, y, off).wait_send()
            if fsend is not None:
                each(0, ny, lambda block: across(block).wait_send())

        return start, pass_on, finish, drain

    abuf[c, y] = acc.astype(BF16)
    a_start, a_pass, a_finish, a_drain = gather(abuf, a_send, a_recv, af_send, af_recv)
    a_start()
    a_pass()
    loads[8].wait()
    loads[15].wait()
    loads[6].wait()

    def project(core):
        total = jnp.zeros((tok, feat), F32)
        for i in range(0, ny, 2):
            heads = jnp.concatenate([abuf[core, i], abuf[core, i + 1]], axis=1)
            total = total + dot(heads, wo[core, i : i + 2].reshape(2 * hd, feat))
        return total

    projected = stream_ref[...].astype(F32) + project(c)
    a_finish()
    projected = projected + project(1 - c)
    mixed = projected.astype(BF16)
    mixed_ref[...] = mixed

    snd[...] = dot(pt[...], mixed).astype(BF16).reshape(nsp, per_dest, feat)

    def block_at(i, sign):
        rank = lax.div(i, nx)
        dz = jnp.where(rank == nz - 1, 0, offset_near(nz - 2 - rank, nz))
        dx = lax.rem(i, nx)
        return lax.rem(z + sign * dz + nz, nz) * nx + lax.rem(x + sign * dx + nx, nx)

    half = nsp // 2
    own_i = (nz - 1) * nx
    own_at = own_i % half

    def wrapped(value, n):
        return jnp.where(value >= n, value - n, value)

    def step_z(rank):
        i = nz - 2 - rank
        return 0 if rank == nz - 1 else (i // 2 + 1 if i % 2 == 0 else nz - (i // 2 + 1))

    before = [wrapped(z + (nz - step_z(rank)) % nz, nz) * nx for rank in range(nz)]
    after = [wrapped(z + step_z(rank), nz) * nx for rank in range(nz)]
    left = [wrapped(x + (nx - dx) % nx, nx) for dx in range(nx)]
    right = [wrapped(x + dx, nx) for dx in range(nx)]

    def send_out(i):
        to = before[i // nx] + left[i % nx]
        at, core = i % half, 1 - i // half
        rdma(snd.at[to], arr.at[at, c], d_send.at[i], d_recv.at[at, c], (to, y * 2 + core)).start()

    def others(fn):
        each(0, own_i, fn)
        each(own_i + 1, nsp, fn)

    def dispatch(i):
        to = block_at(i, -1)
        core = jnp.where(i < half, 1, 0)
        at = jnp.where(i < half, i, i - half)
        return rdma(snd.at[to], arr.at[at, c], d_send.at[i], d_recv.at[at, c], (to, y * 2 + core))

    def dispatch_own():
        return rdma(snd.at[sp], arr.at[own_at, c], d_send.at[own_i], d_recv.at[own_at, c], partner)

    for k in range(nsp):
        i = k // 2 + half * (k % 2)
        if i != own_i:
            send_out(i)

    @pl.when(c == 0)
    def _():
        arr[own_at, 0] = snd[sp]

    @pl.when(c == 1)
    def _():
        dispatch_own().start()


    def products(rows, gain, lhs_of, gate_w, up_w):
        value = rows.astype(F32)
        squares = jnp.sum(value * value, axis=1, keepdims=True)
        lhs = lhs_of((value * gain).astype(BF16))
        gate = dot(lhs, gate_w).astype(BF16)
        up = dot(lhs, up_w).astype(BF16)
        return gate, up, squares

    def two_lanes(column):
        high, low = halves(column)
        lane = iota((column.shape[0], 128), 1)
        return jnp.where(
            lane == 0, high.astype(F32), jnp.where(lane == 1, low.astype(F32), 0.0)
        ).astype(BF16)

    def laid(ref, lo, value):
        ref[:, :, lo : lo + value.shape[1]] = value.reshape(ref.shape[0], ref.shape[1], value.shape[1])

    def packed(total):
        squares = total[:, 2 * ffe : 2 * ffe + 1] + total[:, 2 * ffe + 1 : 2 * ffe + 2]
        return total[:, 0 : 2 * ffe].astype(BF16), two_lanes(squares)

    def activated(total):
        squares = total[:, 2 * ffe : 2 * ffe + 1] + total[:, 2 * ffe + 1 : 2 * ffe + 2]
        return scaled_hidden(total, lax.rsqrt(squares / width + EPS))

    def scaled_hidden(total, inv):
        gate, up = total[:, 0:ffe] * inv, total[:, ffe : 2 * ffe] * inv
        return (gate * jax.nn.sigmoid(gate) * up).astype(BF16)

    loads[9].wait()
    loads[10].wait()
    gate, up, squares = products(mixed, gain_ref[c], lambda a: a, sg[...], su[...])
    laid(spart, 0, gate)
    laid(spart, ffe, up)
    laid(spart, 2 * ffe, two_lanes(squares))
    ny2 = ny // 2

    def spre_copy(i):
        yy = 2 * i + 1 - c
        return rdma(spart.at[yy], spre.at[i], spre_send.at[i], spre_recv.at[i], partner)

    each(0, ny2, lambda i: spre_copy(i).start())

    def srs_copy(i):
        yy = 2 * i + c
        return rdma(sred.at[i], srs_in.at[y], srs_send.at[i], srs_recv.at[y], in_column(yy))

    def shared_add(i):
        yy = 2 * i + c
        rdma(spre.at[i], spre.at[i], spre_send.at[i], spre_recv.at[i], partner).wait_recv()
        sums, squares = packed(spart[yy].astype(F32) + spre[i].astype(F32))
        sred[i, :, 0 : 2 * ffe] = sums
        sred[i, :, 2 * ffe : 2 * ffe + 128] = squares

        @pl.when(yy != y)
        def _():
            srs_copy(i).start()

    each(0, ny2, shared_add)

    npos, chunk = nsp // 4, red.shape[2]
    rows_g = npos * per_dest

    def by_expert(a):
        zero = jnp.zeros_like(a)
        mine = lax.rem(iota(a.shape, 0), per_dest) < cap
        return jnp.concatenate([jnp.where(mine, a, zero), jnp.where(mine, zero, a)], axis=1)

    def arrivals(g):
        def arrive(at):
            for core in range(2):
                here = arr.at[at, core]
                rdma(here, here, d_send.at[1], d_recv.at[at, core], partner).wait_recv()

        if g != own_at // npos:
            each(g * npos, (g + 1) * npos, arrive)
        else:
            each(g * npos, own_at, arrive)
            each(own_at + 1, (g + 1) * npos, arrive)
            here = arr.at[own_at, 1]
            rdma(here, here, d_send.at[1], d_recv.at[own_at, 1], partner).wait_recv()

            @pl.when(c == 1)
            def _():
                here = arr.at[own_at, 0]
                rdma(here, here, d_send.at[1], d_recv.at[own_at, 0], partner).wait_recv()

    def squares_copy(g, k):
        here = square_rows.at[g, y]
        return rdma(here, here, n_send.at[g, k], n_recv.at[g, y], in_column(lax.rem(y + k, ny)))

    def scales(g):
        def arrive(k):
            ys = lax.rem(y + k, ny)
            here = square_rows.at[g, ys]
            rdma(here, here, n_send.at[g, k], n_recv.at[g, ys], partner).wait_recv()

        each(1, ny, arrive)
        squares = square_rows[g, 0]
        for ys in range(1, ny):
            squares = squares + square_rows[g, ys]
        inv = to_column(lax.rsqrt(squares / width + EPS))
        inverse[g] = jnp.broadcast_to(inv, (rows_g, 128)).reshape(ny, chunk, 128)

    def experts(g):
        at = slice(g * npos, (g + 1) * npos)
        rows = jnp.concatenate([arr[at, core].reshape(rows_g, feat) for core in range(2)], axis=1)
        gain = jnp.concatenate([gain_ref[0], gain_ref[1]], axis=1)
        gate, up, squares = products(
            rows, gain, by_expert, wg[...].reshape(4 * feat, ffe), wu[...].reshape(4 * feat, ffe)
        )
        square_rows[g, y] = to_row(squares)
        for k in range(1, ny):
            squares_copy(g, k).start()
        red[g, :, :, 0:ffe] = gate.reshape(ny, chunk, ffe)
        red[g, :, :, ffe : 2 * ffe] = up.reshape(ny, chunk, ffe)
        for r in (4, 3, 5, 2, 6):
            l1_copy(g, r).start()

    def l1_copy(g, r):
        if r == 4:
            side = lax.rem(y, 2)
            hub, k = jnp.where(side == 0, 3, 5), 2
        else:
            side = 0 if r < 4 else 1
            hub, k = (r - 1, r - 2) if r < 4 else (r + 1, ny - r - 2)
        return rdma(
            red.at[g, lax.rem(y + r, ny)],
            hub_in.at[g, side, k],
            l1_send.at[g, r],
            l1_recv.at[g, side, k],
            in_column(lax.rem(y + hub, ny)),
        )

    def l2_copy(g, side):
        to = lax.rem(y + (1 if side == 0 else ny - 1), ny)
        return rdma(hub_out.at[g, side], own_in.at[g, side], l2_send.at[g, side], l2_recv.at[g, side], in_column(to))

    def hub(g):
        for side in range(2):
            def add_in(k, total):
                here = hub_in.at[g, side, k]
                rdma(here, here, l1_send.at[g, 2], l1_recv.at[g, side, k], partner).wait_recv()
                return total + hub_in[g, side, k].astype(F32)

            odd = lax.rem(y, 2)
            mine = red[g, lax.rem(y + (1 if side == 0 else ny - 1), ny)].astype(F32)
            total = lax.fori_loop(0, 2 + odd if side == 0 else 3 - odd, add_in, mine)
            hub_out[g, side] = total.astype(BF16)
            l2_copy(g, side).start()

    gathers = [gather(hbuf.at[g], h_send.at[g], h_recv.at[g]) for g in range(2)]

    def own(g):
        total = red[g, y].astype(F32)
        for side in range(2):
            here = own_in.at[g, side]
            rdma(here, here, l2_send.at[g, side], l2_recv.at[g, side], partner).wait_recv()
            total = total + own_in[g, side].astype(F32)
        hbuf[g, y] = scaled_hidden(total, inverse[g, y][:, 0:1])
        gathers[g][0]()

    def give_back(at, core):
        i = at + half * (1 - c)
        to = block_at(i, 1)
        return rdma(ret_out.at[at, core], ret_in.at[sp], r_send.at[at, core], r_recv.at[i], (to, y * 2 + core))

    def down(g):
        rows = by_expert(hbuf[g].reshape(rows_g, ffe))
        at = slice(g * npos, (g + 1) * npos)
        for core in range(2):
            ret_out[at, core] = dot(rows, wd[core]).astype(BF16).reshape(npos, per_dest, feat)

        for at in range(g * npos, (g + 1) * npos):
            if at != own_at:
                near = at + half
                to = jnp.where(c == 1, after[at // nx] + right[at % nx], after[near // nx] + right[near % nx])
                for core in range(2):
                    rdma(
                        ret_out.at[at, core],
                        ret_in.at[sp],
                        r_send.at[at, core],
                        r_recv.at[at + half * (1 - c)],
                        (to, y * 2 + core),
                    ).start()
        if g == own_at // npos:
            give_back(own_at, 1).start()

            @pl.when(c == 1)
            def _():
                give_back(own_at, 0).start()

            @pl.when(c == 0)
            def _():
                ret_in[sp] = ret_out[own_at, 0]

    owner = lax.rem(y, 2) == c

    arrivals(0)
    for i in (0, 1, 3):
        swapped[i].wait_recv()
    experts(0)

    @pl.when(owner)
    def _():
        def add_in(i, total):
            ys = lax.rem(y + offset_near(i, ny), ny)
            rdma(srs_in.at[ys], srs_in.at[ys], srs_send.at[0], srs_recv.at[ys], partner).wait_recv()
            return total + srs_in[ys].astype(F32)

        total = lax.fori_loop(0, ny - 1, add_in, sred[y // 2].astype(F32))
        shbuf[y] = activated(total)

        def to_peer(i):
            off = offset_near(i, ny)
            rdma(
                shbuf.at[y], shbuf.at[y], sh_send.at[i], sh_recv.at[y], in_column(lax.rem(y + off, ny))
            ).start()

        each(0, ny - 1, to_peer)
        rdma(shbuf.at[y], shbuf.at[y], shf_send.at[y // 2], shf_recv.at[y], partner).start()

    arrivals(1)
    experts(1)
    hub(0)
    scales(0)
    scales(1)
    hub(1)
    own(0)
    own(1)
    gathers[0][1]()
    def shared_on(i):
        yy = 2 * i + c

        @pl.when(yy != y)
        def _():
            rdma(shbuf.at[yy], shbuf.at[yy], sh_send.at[0], sh_recv.at[yy], partner).wait_recv()
            rdma(shbuf.at[yy], shbuf.at[yy], shf_send.at[i], shf_recv.at[yy], partner).start()

    each(0, ny2, shared_on)
    swapped[2].wait_recv()
    down(0)
    gathers[1][1]()
    down(1)

    def shared_arrive(i):
        yy = 2 * i + 1 - c
        rdma(shbuf.at[yy], shbuf.at[yy], shf_send.at[i], shf_recv.at[yy], partner).wait_recv()

    each(0, ny2, shared_arrive)
    loads[14].wait()
    base = mixed_ref[...].astype(F32) + dot(shbuf[...].reshape(tok, ffe), sd[...])

    each(1, nx, lambda i: kv_copy(i).wait_send())
    each(1, z + 1, lambda i: q_copy(i).wait_send())
    each(1, nz - z, lambda i: part_copy(z + i).wait_send())
    a_drain()
    others(lambda i: dispatch(i).wait_send())

    @pl.when(c == 1)
    def _():
        dispatch_own().wait_send()

    for copy in swapped:
        copy.wait_send()
    each(0, ny2, lambda i: spre_copy(i).wait_send())

    def srs_drain(i):
        @pl.when(2 * i + c != y)
        def _():
            srs_copy(i).wait_send()

    each(0, ny2, srs_drain)
    for g in range(2):
        for r in (4, 3, 5, 2, 6):
            l1_copy(g, r).wait_send()
        for side in range(2):
            l2_copy(g, side).wait_send()
        for k in range(1, ny):
            squares_copy(g, k).wait_send()
        gathers[g][3]()

    @pl.when(owner)
    def _():
        each(
            0,
            ny - 1,
            lambda i: rdma(shbuf.at[y], shbuf.at[y], sh_send.at[i], sh_recv.at[y], partner).wait_send(),
        )

    def shared_forwarded(i):
        yy = 2 * i + c
        rdma(shbuf.at[yy], shbuf.at[yy], shf_send.at[i], shf_recv.at[yy], partner).wait_send()

    each(0, ny2, shared_forwarded)

    def returned(i):
        src = block_at(i, -1)
        rdma(ret_in.at[src], ret_in.at[src], r_send.at[i], r_recv.at[i], (src, tp)).wait_recv()

    others(returned)

    @pl.when(c == 1)
    def _():
        returned(own_i)

    rows = ret_in[...].reshape(nslot, feat)
    out_ref[...] = (base + (dot(w_hi[...], rows) + dot(w_lo[...], rows))).astype(BF16)

    def given(at):
        for core in range(2):
            give_back(at, core).wait_send()

    each(0, own_at, given)
    each(own_at + 1, nsp // 2, given)
    give_back(own_at, 1).wait_send()

    @pl.when(c == 1)
    def _():
        give_back(own_at, 0).wait_send()


def body(
    nx,
    queries,
    key_rows,
    value_rows,
    break_bias,
    stream,
    out_proj,
    norm_gain,
    expert_ids,
    route_weights,
    gate_proj,
    up_proj,
    down_proj,
    shared_gate,
    shared_up,
    shared_down,
):
    nsp, ntp = lax.axis_size("sp"), lax.axis_size("tp")
    nz, ny = nsp // nx, ntp // 2
    tok, hd = queries.shape
    feat = stream.shape[1]
    experts_local, _, ffe = gate_proj.shape
    ffs = shared_gate.shape[1]
    cap = 2 * expert_ids.shape[1] * tok // (experts_local * nsp)
    per_dest = experts_local * cap
    chunk = nsp * per_dest // ntp // 2
    srows = tok // ny
    wide = 2 * ffe + 128
    hk = (nx // 2) * tok

    def vm(*shape):
        return pltpu.VMEM(shape, BF16)

    def sems(*counts):
        return [pltpu.SemaphoreType.DMA(n if isinstance(n, tuple) else (n,)) for n in counts]

    scratch = [
        vm(tok, hd),
        vm(1, tok),
        vm(tok, feat),
        pltpu.VMEM((2, 1, feat), F32),
        pltpu.VMEM((2, tok), jnp.int32),
        pltpu.VMEM((2, tok), F32),
        vm(2, ny, hd, feat),
        vm(experts_local, 2, feat, ffe),
        vm(experts_local, 2, feat, ffe),
        vm(2, experts_local * ffe, feat),
        vm(feat, ffs),
        vm(feat, ffs),
        vm(ffs, feat),
        vm(nx, 2 * tok + 16, hd),
        vm(nz, tok, hd),
        vm(nz, tok + 16, hd),
        vm(nz, tok + 16, hd),
        vm(hk, hk),
        vm(2, ny, tok, hd),
        vm(nsp * per_dest, tok),
        vm(tok, nsp * per_dest),
        vm(tok, nsp * per_dest),
        vm(tok, feat),
        vm(nsp, per_dest, feat),
        vm(nsp // 2, 2, per_dest, feat),
        vm(2, ny, chunk, 2 * ffe),
        vm(2, 2, 3, chunk, 2 * ffe),
        vm(2, 2, chunk, 2 * ffe),
        vm(2, 2, chunk, 2 * ffe),
        pltpu.VMEM((2, ny, 1, ny * chunk), F32),
        pltpu.VMEM((2, ny, chunk, 128), F32),
        vm(ny, srows, wide),
        vm(ny // 2, srows, wide),
        vm(ny // 2, srows, wide),
        vm(ny, srows, wide),
        vm(2, ny, chunk, ffe),
        vm(ny, srows, ffs),
        vm(nsp // 2, 2, per_dest, feat),
        vm(nsp, per_dest, feat),
        *sems(16, nx, nx, nz, nz, nz, nz, 7, ny, ny, ny, nsp, (nsp // 2, 2), 4, 4, (2, ny), (2, 2, 3), (2, 2), (2, 2), (2, ny), (2, ny)),
        *sems(ny // 2, ny // 2, ny // 2, ny, (2, 7), (2, ny), ny, ny, ny // 2, ny, (nsp // 2, 2), nsp),
    ]
    large = pl.BlockSpec(memory_space=pl.ANY)
    return pl.pallas_call(
        functools.partial(layer_kernel, (nz, nx, ny)),
        out_shape=jax.ShapeDtypeStruct((tok, feat), BF16),
        in_specs=[large] * 15,
        out_specs=pl.BlockSpec(memory_space=pltpu.VMEM),
        scratch_shapes=scratch,
        compiler_params=pltpu.CompilerParams(
            collective_id=0, has_side_effects=True, vmem_limit_bytes=60 * 1024 * 1024
        ),
    )(
        queries,
        key_rows,
        value_rows,
        break_bias.T,
        stream,
        norm_gain.reshape(1, feat),
        expert_ids.T,
        route_weights.T,
        out_proj.reshape(ny, 2, hd, feat),
        gate_proj,
        up_proj,
        down_proj.reshape(experts_local * ffe, feat),
        shared_gate,
        shared_up,
        shared_down,
    )


def solution(mesh, nx=NX):
    in_specs = (
        P("sp", "tp"),
        P("sp", "tp"),
        P("sp", "tp"),
        P("sp", "tp"),
        P("sp", "tp"),
        P(None, "tp"),
        P("tp"),
        P("sp", None),
        P("sp", None),
        P("sp", "tp", None),
        P("sp", "tp", None),
        P("sp", None, "tp"),
        P("tp", None),
        P("tp", None),
        P(None, "tp"),
    )
    return jax.shard_map(
        functools.partial(body, nx), mesh=mesh, in_specs=in_specs, out_specs=P("sp", "tp"), check_vma=False
    )
```
